32 devices in a mesh: grp: 2 (over y), sp: 4 (over z), tp: 4 (over x, core).
Axes of the slice: x: 2, y: 2, z: 4, core: 2. Of those that a mesh axis runs over, the one named last changes fastest.
Arguments:
- resid_in: bfloat16 [8, 256, 2048], P(('grp', 'tp'), 'sp'), parts along dimension 0, may hold values from -6 to 6
- query_one: bfloat16 [8, 256, 1024], P('grp', 'sp', 'tp'), parts along dimension 0, may hold values from -624 to 624
- key_one: bfloat16 [8, 256, 256], P('grp', 'sp', 'tp'), parts along dimension 0, may hold values from -7.78125 to 7.78125
- query_two: bfloat16 [8, 256, 1024], P('grp', 'sp', 'tp'), parts along dimension 0, may hold values from -624 to 624
- key_two: bfloat16 [8, 256, 256], P('grp', 'sp', 'tp'), parts along dimension 0, may hold values from -7.78125 to 7.78125
- value: bfloat16 [8, 256, 512], P('grp', 'sp', 'tp'), parts along dimension 0, may hold values from -6 to 6
- lam: float32 [32], P('tp'), may hold values from 0.3 to 0.8
- head_gain: float32 [64], replicated, may hold values from 0.1 to 1.9
- doc_ids: int32 [8, 256], P('grp', 'sp'), parts along dimension 0, may hold values from 0 to 3, never falling along the last dimension, each value on 1 to 128 neighbouring positions
- out_weight: bfloat16 [2048, 2048], P('tp'), may hold values from -0.125 to 0.125
- norm_gain: float32 [2048], replicated, may hold values from 0.1 to 1.9
- gate_weight: bfloat16 [2048, 5632], P('sp', 'tp'), may hold values from -0.125 to 0.125
- value_weight: bfloat16 [2048, 5632], P('sp', 'tp'), may hold values from -0.125 to 0.125
- conv_gate: float32 [3, 5632], P(None, 'tp'), may hold values from -3.5 to 3.5
- conv_value: float32 [3, 5632], P(None, 'tp'), may hold values from -3.5 to 3.5
- down_weight: bfloat16 [5632, 2048], P('tp', 'sp'), may hold values from -0.078125 to 0.078125
Outputs:
- resid_out: bfloat16 [8, 256, 2048], P(('grp', 'tp'), 'sp'), parts along dimension 0
The draws below stay inside these ranges and needn't reach their ends.
There are 2 independent parts, one for each index of `grp`. The reference program is written for one: setup_inputs(seed, part) draws one part's arguments, and reference() takes and returns one part's arrays. A program takes and returns all parts, laid end to end along the dimension named above; an argument that names none is the same for every part. Nothing has to cross between parts.
All inputs are finite; a program needn't handle non-finite values.
Results may differ from the reference program's by a relative error of at most 0.014.
Values may be sent and summed in bfloat16 or wider, within the bound.
A program may use at most 128 MiB of HBM per device.

```python
import math
import jax
import jax.numpy as jnp
import numpy as np
from jax import lax

D = 2048
HEADS = 32
KV_HEADS = 8
QK = 32
HEAD_DIM = 64
FF = 5632
SEQS = 4
SEQ_LEN = 256
N_TP = 4


def drawn_queries(key):
    base = 1.3 * jax.random.normal(jax.random.fold_in(key, 11), (SEQS, SEQ_LEN, HEADS * QK), jnp.float32)
    base = jnp.clip(base, -7.8, 7.8)
    return base.astype(jnp.bfloat16)


def draw_query_one(key, part):
    return drawn_queries(jax.random.fold_in(key, 1))


def draw_query_two(key, part):
    return drawn_queries(jax.random.fold_in(key, 2))


def block_levels(own_key, shape, cuts, least, largest):
    level = 1.0
    for axis_at, parts in cuts:
        steps = jax.random.uniform(jax.random.fold_in(jax.random.fold_in(own_key, 6), axis_at), (parts,), jnp.float32, least / len(cuts), largest / len(cuts))
        level = level * jnp.repeat(jnp.exp(steps), shape[axis_at] // parts).reshape((-1,) + (1,) * (len(shape) - 1 - axis_at))
    return level


def length_profile(number_of, total, most, lean):
    portions = [(1 << 20) // math.isqrt(rank ** lean) + 1 for rank in range(2, number_of + 1)]
    spare, holding = total - most - (number_of - 1), [1] * (number_of - 1)
    while spare > 0:
        movable = [i for i in range(number_of - 1) if holding[i] < most]
        pool, left = sum([portions[i] for i in movable]), spare
        for i in movable:
            addition = min(most - holding[i], max(1, left * portions[i] // pool), spare)
            holding[i] = holding[i] + addition
            spare = spare - addition
    return np.array([most] + holding)


def ragged(own_key, amount, total, limit, slope):
    if amount == 2:
        one = jax.random.randint(own_key, (), max(1, total - limit), min(limit, total - 1) + 1)
        return jnp.stack([one, total - one])
    lengths = jnp.asarray(length_profile(amount, total, limit, slope), jnp.int32)
    twos = (amount - 1) // 2
    giver, sink = lengths[1:1 + 2 * twos:2], lengths[2:2 + 2 * twos:2]
    margin = jnp.minimum(giver - 1, limit - sink)
    shifted = jax.random.randint(jax.random.fold_in(own_key, 1), (twos,), 0, 1 << 20) % (margin + 1)
    lengths = lengths.at[1:1 + 2 * twos:2].set(giver - shifted).at[2:2 + 2 * twos:2].set(sink + shifted)
    return lengths[jax.random.permutation(jax.random.fold_in(own_key, 2), amount)]


def noise(stream_key, extent, scale, bound, pieces=(), kind=jnp.bfloat16):
    drawn = scale * jax.random.normal(stream_key, extent, jnp.float32)
    if pieces:
        drawn = drawn * block_levels(stream_key, extent, pieces, -0.22, 0.18)
    return jnp.clip(drawn, -bound, bound).astype(kind)


def setup_inputs(seed: int = 0, part: int = 0) -> dict:
    arg_keys = jax.random.split(jax.random.key(seed), 17)
    part_keys = jax.random.split(jax.random.fold_in(arg_keys[16], part), 17)
    resid_in = noise(part_keys[0], (SEQS, SEQ_LEN, D), 1.0, 6.0, ((0, 4), (1, 4)))
    query_one = draw_query_one(jax.random.fold_in(jax.random.fold_in(arg_keys[16], part), 71), part)
    key_one = noise(part_keys[2], (SEQS, SEQ_LEN, KV_HEADS * QK), 1.3, 7.78125, ((1, 4), (2, 4)))
    query_two = draw_query_two(jax.random.fold_in(jax.random.fold_in(arg_keys[16], part), 71), part)
    key_two = noise(part_keys[4], (SEQS, SEQ_LEN, KV_HEADS * QK), 1.3, 7.78125, ((1, 4), (2, 4)))
    value = noise(part_keys[5], (SEQS, SEQ_LEN, KV_HEADS * HEAD_DIM), 1.0, 6.0, ((1, 4), (2, 4)))
    lam = jnp.clip(0.3 + 0.5 * jax.random.uniform(arg_keys[6], (HEADS,), jnp.float32) ** block_levels(arg_keys[6], (HEADS,), ((0, 4),), -0.2, 0.2), 0.3, 0.8)
    head_gain = jnp.clip(1.0 + 0.18 * jax.random.normal(arg_keys[7], (HEAD_DIM,), jnp.float32), 0.1, 1.9)
    doc_ids = jax.vmap(lambda own: jnp.searchsorted(jnp.cumsum(ragged(own, 4, SEQ_LEN, SEQ_LEN // 2, 1)), jnp.arange(SEQ_LEN), side="right"))(jax.random.split(part_keys[8], SEQS)).reshape((SEQS, SEQ_LEN)).astype(jnp.int32)
    out_weight = noise(arg_keys[9], (HEADS * HEAD_DIM, D), (HEADS * HEAD_DIM) ** -0.5, 0.125, ((0, 4),))
    norm_gain = jnp.clip(1.0 + 0.18 * jax.random.normal(arg_keys[10], (D,), jnp.float32), 0.1, 1.9)
    gate_weight = noise(arg_keys[11], (D, FF), D ** -0.5, 0.125, ((0, 4), (1, 4)))
    value_weight = noise(arg_keys[12], (D, FF), D ** -0.5, 0.125, ((0, 4), (1, 4)))
    conv_gate = noise(arg_keys[13], (3, FF), 3 ** -0.5, 3.5, ((1, 4),), jnp.float32)
    conv_value = noise(arg_keys[14], (3, FF), 3 ** -0.5, 3.5, ((1, 4),), jnp.float32)
    down_weight = noise(arg_keys[15], (FF, D), FF ** -0.5, 0.078125, ((0, 4), (1, 4)))
    return dict(resid_in=resid_in, query_one=query_one, key_one=key_one, query_two=query_two, key_two=key_two, value=value, lam=lam, head_gain=head_gain, doc_ids=doc_ids, out_weight=out_weight, norm_gain=norm_gain, gate_weight=gate_weight, value_weight=value_weight, conv_gate=conv_gate, conv_value=conv_value, down_weight=down_weight)


NEG_BIG = -1e+30
NORM_EPS = 1e-06
ROPE_BASE = 500000.0

def rotate(block, positions, heads):
    entries = block.astype(jnp.float32).reshape(block.shape[:-1] + (heads, -1))
    width = entries.shape[-1]
    half = width // 2
    freqs = ROPE_BASE ** (-jnp.arange(half, dtype=jnp.float32) * 2.0 / width)
    angles = positions.astype(jnp.float32)[:, None] * freqs[None, :]
    cosine = jnp.cos(angles)[:, None, :]
    sine = jnp.sin(angles)[:, None, :]
    first = entries[..., :half]
    second = entries[..., half:]
    turned = jnp.concatenate([first * cosine - second * sine, second * cosine + first * sine], axis=-1)
    return turned.astype(jnp.bfloat16)

def depthwise(edge, current, taps, edge_docs, docs):
    count = current.shape[0]
    extended = jnp.concatenate([edge, current], axis=0).astype(jnp.float32)
    ext_docs = jnp.concatenate([edge_docs, docs], axis=0)
    total = taps[2][None, :] * extended[2:]
    for shift_k in range(2):
        same = (ext_docs[shift_k:shift_k + count] == docs)[:, None]
        total = total + jnp.where(same, taps[shift_k][None, :] * extended[shift_k:shift_k + count], 0.0)
    return total

def head_rows(args, positions, docs, gain):
    q_one, k_one, q_two, k_two, vals, weight = args
    tokens = vals.shape[0]
    blk = math.gcd(tokens, 512)
    scale = q_one.shape[-1] ** (-0.5)

    def one_block(index):
        start = index * blk
        qpos = start + jnp.arange(blk, dtype=jnp.int32)
        qdoc = lax.dynamic_slice_in_dim(docs, start, blk, 0)
        allowed = (positions[None, :] <= qpos[:, None]) & (docs[None, :] == qdoc[:, None])

        def branch(q_all, k_all):
            qblock = lax.dynamic_slice_in_dim(q_all, start, blk, 0)
            scores = jnp.dot(qblock, k_all.T, preferred_element_type=jnp.float32) * scale
            scores = jnp.where(allowed, scores, NEG_BIG)
            peak = lax.optimization_barrier(jnp.max(scores, axis=-1, keepdims=True))
            expd = jnp.where(allowed, jnp.exp(scores - peak), 0.0)
            numer = jnp.dot(expd.astype(jnp.bfloat16), vals, preferred_element_type=jnp.float32)
            return numer / lax.optimization_barrier(jnp.sum(expd, axis=-1, keepdims=True))
        mixed = branch(q_one, k_one) - weight * branch(q_two, k_two)
        meansq = lax.optimization_barrier(jnp.mean(mixed * mixed, axis=-1, keepdims=True))
        return (mixed * lax.rsqrt(meansq + NORM_EPS) * gain[None, :]).astype(jnp.bfloat16)
    out = lax.map(one_block, jnp.arange(tokens // blk))
    return out.reshape(tokens, -1)

def grouped_product(left, right, groups):
    width = left.shape[1] // groups
    total = jnp.zeros((left.shape[0], right.shape[1]), jnp.float32)
    for group in range(groups):
        part = jnp.dot(left[:, group * width:(group + 1) * width], right[group * width:(group + 1) * width], preferred_element_type=jnp.float32).astype(jnp.bfloat16)
        part = lax.optimization_barrier(part)
        total = total + part.astype(jnp.float32)
    return total

def reference(resid_in, query_one, key_one, query_two, key_two, value, lam, head_gain, doc_ids, out_weight, norm_gain, gate_weight, value_weight, conv_gate, conv_value, down_weight):
    heads = lam.shape[0]
    key_width = query_one.shape[2] // heads
    kv_heads = key_one.shape[2] // key_width
    group = heads // kv_heads

    def by_head(block):
        return jnp.transpose(block, (1, 0, 2))

    def one_sequence(args):
        resid, q_a, k_a, q_b, k_b, vals_in, docs = args
        tokens = resid.shape[0]
        positions = jnp.arange(tokens, dtype=jnp.int32)
        q_first = by_head(rotate(q_a, positions, heads))
        k_first = jnp.repeat(by_head(rotate(k_a, positions, kv_heads)), group, axis=0)
        q_second = by_head(rotate(q_b, positions, heads))
        k_second = jnp.repeat(by_head(rotate(k_b, positions, kv_heads)), group, axis=0)
        vals = jnp.repeat(by_head(vals_in.reshape(tokens, kv_heads, -1)), group, axis=0)
        per_head = lax.map(lambda items: head_rows(items, positions, docs, head_gain), (q_first, k_first, q_second, k_second, vals, lam))
        heads_out = jnp.transpose(per_head, (1, 0, 2)).reshape(tokens, -1)
        proj = grouped_product(heads_out, out_weight, N_TP)
        mid = resid.astype(jnp.float32) + proj
        meansq = lax.optimization_barrier(jnp.mean(mid * mid, axis=-1, keepdims=True))
        normed = (mid * lax.rsqrt(meansq + NORM_EPS) * norm_gain[None, :]).astype(jnp.bfloat16)
        up_gate = jnp.dot(normed, gate_weight, preferred_element_type=jnp.float32).astype(jnp.bfloat16)
        up_value = jnp.dot(normed, value_weight, preferred_element_type=jnp.float32).astype(jnp.bfloat16)
        edge = jnp.zeros((2, up_gate.shape[1]), jnp.bfloat16)
        edge_docs = jnp.full((2,), -1, jnp.int32)
        conv_g = depthwise(edge, up_gate, conv_gate, edge_docs, docs)
        conv_v = depthwise(edge, up_value, conv_value, edge_docs, docs)
        hidden = (jax.nn.silu(conv_g) * conv_v).astype(jnp.bfloat16)
        down = grouped_product(hidden, down_weight, N_TP)
        return (mid + down).astype(jnp.bfloat16)
    return lax.map(one_sequence, (resid_in, query_one, key_one, query_two, key_two, value, doc_ids))
```

```python
import functools
import math

import jax
import jax.numpy as jnp
import numpy as np
from jax import lax
from jax.experimental import pallas as pl
from jax.experimental.pallas import tpu as pltpu
from jax.sharding import PartitionSpec as P

NEG_BIG = -1e30
NORM_EPS = 1e-06
ROPE_BASE = 500000.0


MESH = pl.DeviceIdType.MESH
VMEM = pl.BlockSpec(memory_space=pltpu.VMEM)


def greet(devices):
    barrier = pltpu.get_barrier_semaphore()
    for device in devices:
        pl.semaphore_signal(barrier, inc=1, device_id=device, device_id_type=MESH)
    pl.semaphore_wait(barrier, len(devices))


def remote(src, dst, send_sem, recv_sem, device):
    return pltpu.make_async_remote_copy(
        src_ref=src,
        dst_ref=dst,
        send_sem=send_sem,
        recv_sem=recv_sem,
        device_id=device,
        device_id_type=MESH,
    )


def partners():
    at = lax.axis_index("tp")
    return at, at + 1 - 2 * lax.rem(at, 2), lax.rem(at + 2, 4)


def spread_kernel(n, own_ref, out_ref, send_sem, recv_sem):
    me = lax.axis_index("sp")
    peers = [lax.rem(me + shift, n) for shift in range(1, n)]
    greet([{"sp": peer} for peer in peers])
    copies = []
    for k, peer in enumerate(peers):
        copy = remote(
            own_ref, out_ref.at[:, me], send_sem.at[k], recv_sem.at[k], {"sp": peer}
        )
        copy.start()
        copies.append(copy)
    out_ref[:, me] = own_ref[...]
    for copy in copies:
        copy.wait_recv()
    for copy in copies:
        copy.wait_send()


def gather_sp(own):
    n = lax.axis_size("sp")
    if n > 8:
        return lax.all_gather(own, "sp", axis=1, tiled=True)
    outer, rows, width = own.shape
    out = pl.pallas_call(
        functools.partial(spread_kernel, n),
        out_shape=jax.ShapeDtypeStruct((outer, n, rows, width), own.dtype),
        in_specs=[VMEM],
        out_specs=VMEM,
        scratch_shapes=[pltpu.SemaphoreType.DMA((n - 1,)), pltpu.SemaphoreType.DMA((n - 1,))],
        compiler_params=pltpu.CompilerParams(collective_id=1, has_side_effects=True),
        cost_estimate=pl.CostEstimate(flops=0, bytes_accessed=30_000_000, transcendentals=0),
        name="gather_sp",
    )(own)
    return out.reshape(outer, n * rows, width)


def rows_kernel(n, own_ref, out_ref, z_send, z_recv, x_send, x_recv, c_send, c_recv):
    me = lax.axis_index("sp")
    tp, near, far = partners()
    greet([{"tp": near}, {"tp": far}] + [{"sp": lax.rem(me + k, n)} for k in range(1, n)])
    sources = [lax.rem(me - k + n, n) for k in range(n)]
    z_copies = []
    for k in range(1, n):
        copy = remote(
            own_ref,
            out_ref.at[tp, me],
            z_send.at[k - 1],
            z_recv.at[k - 1],
            {"sp": lax.rem(me + k, n)},
        )
        z_copies.append(copy)

    def along(owner, k, send, recv, device):
        block = out_ref.at[owner, sources[k]]
        return remote(block, block, send, recv, device)

    x_copies = [remote(own_ref, out_ref.at[tp, me], x_send.at[0], x_recv.at[0], {"tp": far})]
    c_copies = [remote(own_ref, out_ref.at[tp, me], c_send.at[0], c_recv.at[0], {"tp": near})]
    for k in range(1, n):
        x_copies.append(along(tp, k, x_send.at[k], x_recv.at[k], {"tp": far}))
        c_copies.append(along(tp, k, c_send.at[k], c_recv.at[k], {"tp": near}))
    f_copies = [along(far, k, c_send.at[n + k], c_recv.at[n + k], {"tp": near}) for k in range(n)]
    x_copies[0].start()
    for copy in z_copies:
        copy.start()
    c_copies[0].start()
    out_ref[tp, me] = own_ref[...]
    for k in range(1, n):
        z_copies[k - 1].wait_recv()
        x_copies[k].start()
        c_copies[k].start()
    for k in range(n):
        x_copies[k].wait_recv()
        f_copies[k].start()
    for copy in c_copies + f_copies:
        copy.wait_recv()
    for copy in z_copies + x_copies + c_copies + f_copies:
        copy.wait_send()


def gather_rows(own):
    n, wide = lax.axis_size("sp"), lax.axis_size("tp")
    if n > 8 or wide != 4:
        out = lax.all_gather(own, ("tp", "sp"), axis=0)
        return out.reshape((wide, n) + own.shape)
    dma = pltpu.SemaphoreType.DMA
    return pl.pallas_call(
        functools.partial(rows_kernel, n),
        out_shape=jax.ShapeDtypeStruct((wide, n) + own.shape, own.dtype),
        in_specs=[VMEM],
        out_specs=VMEM,
        scratch_shapes=[
            dma((n - 1,)),
            dma((n - 1,)),
            dma((n,)),
            dma((n,)),
            dma((2 * n,)),
            dma((2 * n,)),
        ],
        compiler_params=pltpu.CompilerParams(collective_id=2, has_side_effects=True),
        cost_estimate=pl.CostEstimate(flops=0, bytes_accessed=90_000_000, transcendentals=0),
        name="gather_rows",
    )(own)


def reduce_kernel(
    n, chunks, part_ref, base_ref, out_ref, got_c, sum_c, got_x, sum_x, got_z,
    c_send, c_recv, x_send, x_recv, z_send, z_recv,
):
    tp, near, far = partners()
    low, high = lax.rem(tp, 2), tp // 2
    shifts = range(1, n)
    me = lax.axis_index("sp") if n > 1 else 0
    greet([{"tp": near}, {"tp": far}] + [{"sp": lax.rem(me + k, n)} for k in shifts])
    width = part_ref.shape[-1] // chunks
    cols = [pl.ds(i * width, width) for i in range(chunks)]
    c_copies, x_copies, z_copies = [], [], []
    for i in range(chunks):
        copy = remote(
            part_ref.at[:, 1 - low, :, :, cols[i]],
            got_c.at[i],
            c_send.at[i],
            c_recv.at[i],
            {"tp": near},
        )
        copy.start()
        c_copies.append(copy)
    for i in range(chunks):
        c_copies[i].wait_recv()
        mine = part_ref[:, low, :, :, cols[i]].astype(jnp.float32)
        sum_c[i] = (mine + got_c[i].astype(jnp.float32)).astype(sum_c.dtype)
        copy = remote(
            sum_c.at[i, 1 - high], got_x.at[i], x_send.at[i], x_recv.at[i], {"tp": far}
        )
        copy.start()
        x_copies.append(copy)
    for i in range(chunks):
        x_copies[i].wait_recv()
        both = sum_c[i, high].astype(jnp.float32) + got_x[i].astype(jnp.float32)
        sum_x[i] = both.astype(sum_x.dtype)
        for k in shifts:
            peer = lax.rem(me + k, n)
            copy = remote(
                sum_x.at[i, peer],
                got_z.at[i, k - 1],
                z_send.at[i, k - 1],
                z_recv.at[i, k - 1],
                {"sp": peer},
            )
            copy.start()
            z_copies.append(copy)
    for i in range(chunks):
        total = sum_x[i, me].astype(jnp.float32)
        for k in shifts:
            z_copies[i * (n - 1) + k - 1].wait_recv()
            total = total + got_z[i, k - 1].astype(jnp.float32)
        out_ref[:, cols[i]] = (base_ref[:, cols[i]] + total).astype(out_ref.dtype)
    for copy in c_copies + x_copies + z_copies:
        copy.wait_send()


def reduce_rows(part, base, dtype, over_sp):
    wide, n = part.shape[:2]
    if n > 8 or wide != 4 or part.size > 8_000_000:
        axes = ("tp", "sp") if over_sp else "tp"
        flat = part.reshape(-1, part.shape[-1])
        total = lax.psum_scatter(flat, axes, scatter_dimension=0, tiled=True)
        return (base + total.astype(jnp.float32)).astype(dtype)
    rows, columns = part.shape[2:]
    chunks = 4 if columns % 512 == 0 else 1
    width = columns // chunks
    dma = pltpu.SemaphoreType.DMA
    zs = max(n - 1, 1)
    return pl.pallas_call(
        functools.partial(reduce_kernel, n, chunks),
        out_shape=jax.ShapeDtypeStruct((rows, columns), dtype),
        in_specs=[VMEM, VMEM],
        out_specs=VMEM,
        scratch_shapes=[
            pltpu.VMEM((chunks, 2, n, rows, width), part.dtype),
            pltpu.VMEM((chunks, 2, n, rows, width), part.dtype),
            pltpu.VMEM((chunks, n, rows, width), part.dtype),
            pltpu.VMEM((chunks, n, rows, width), part.dtype),
            pltpu.VMEM((chunks, zs, rows, width), part.dtype),
            dma((chunks,)),
            dma((chunks,)),
            dma((chunks,)),
            dma((chunks,)),
            dma((chunks, zs)),
            dma((chunks, zs)),
        ],
        compiler_params=pltpu.CompilerParams(
            collective_id=3 if over_sp else 4, has_side_effects=True
        ),
        cost_estimate=pl.CostEstimate(flops=0, bytes_accessed=60_000_000, transcendentals=0),
        name="reduce_all" if over_sp else "reduce_tp",
    )(part.reshape(2, 2, n, rows, columns), base)


def rotate(block, positions, heads):
    columns = block.shape[-1]
    width = columns // heads
    half = width // 2
    at = jnp.arange(columns, dtype=jnp.int32)
    freqs = ROPE_BASE ** (-(at % half).astype(jnp.float32) * 2.0 / width)
    angles = positions.astype(jnp.float32)[:, None] * freqs[None, :]
    source = jnp.where(at % width < half, at + half, at - half)
    sign = jnp.where(at % width < half, -1.0, 1.0)
    turn = jnp.where(at[:, None] == source[None, :], sign[None, :], 0.0).astype(jnp.bfloat16)
    flat = block.reshape(-1, columns)
    other = jnp.dot(flat, turn, preferred_element_type=jnp.float32).reshape(block.shape)
    turned = block.astype(jnp.float32) * jnp.cos(angles) + other * jnp.sin(angles)
    return turned.astype(jnp.bfloat16)


def depthwise(current, taps, docs):
    shown = current.astype(jnp.float32)
    total = taps[2] * shown
    for back in (1, 2):
        moved = jnp.pad(shown, ((0, 0), (back, 0), (0, 0)))[:, : shown.shape[1]]
        moved_docs = jnp.pad(docs, ((0, 0), (back, 0)), constant_values=-1)[:, : docs.shape[1]]
        total = total + jnp.where((moved_docs == docs)[..., None], taps[2 - back] * moved, 0.0)
    return total


def cyclic(array, axis, by):
    length = lax.axis_size(axis)
    return lax.ppermute(array, axis, [(i, (i + by) % length) for i in range(length)])


def exchange(piece, whole):
    count = lax.axis_size("sp")
    copies = lax.axis_size("grp")
    me = lax.axis_index("sp")
    mine = lax.axis_index("grp")
    if count > 8:
        pieces = jnp.stack([whole(dest) for dest in range(count)], axis=0)
        return lax.all_to_all(pieces, "sp", 0, 0)
    parts = []
    for shift in range(1, count):
        part = piece(lax.rem(me + shift, count), mine)
        parts.append(cyclic(part, "sp", shift))
    got = [jnp.stack(parts, axis=0)]
    for turn in range(1, copies):
        got.append(cyclic(got[0], "grp", turn))
    got = jnp.stack(got, axis=1)
    held = whole(me)
    held = jnp.broadcast_to(held[None], (1,) + held.shape)
    order = [lax.rem(mine - share + copies, copies) for share in range(copies)]
    out = []
    for source in range(count):
        shift = lax.rem(me - source + count, count)
        there = lax.max(shift - 1, 0)
        shares = [
            lax.dynamic_slice(got, (there, at) + (0,) * (got.ndim - 2), (1, 1) + got.shape[2:])[0]
            for at in order
        ]
        out.append(jnp.where(shift == 0, held, jnp.concatenate(shares, axis=0)[None]))
    return jnp.concatenate(out, axis=0)


def online_step(state, queries, keys, vals, allowed, scale):
    peak, total, accum = state
    scores = (
        jnp.einsum("sqhgd,skhd->shgqk", queries, keys, preferred_element_type=jnp.float32) * scale
    )
    mask = allowed[:, None, None]
    scores = jnp.where(mask, scores, NEG_BIG)
    new_peak = jnp.maximum(peak, jnp.max(scores, axis=-1))
    expd = jnp.where(mask, jnp.exp(scores - new_peak[..., None]), 0.0)
    fade = jnp.exp(peak - new_peak)
    new_total = total * fade + jnp.sum(expd, axis=-1)
    update = jnp.einsum(
        "shgqk,skhd->shgqd", expd.astype(jnp.bfloat16), vals, preferred_element_type=jnp.float32
    )
    return (new_peak, new_total, accum * fade[..., None] + update)


HBM = pl.BlockSpec(memory_space=pltpu.HBM)
SMEM = pl.BlockSpec(memory_space=pltpu.SMEM)
LANES = 128


def rounded(array):
    return array.astype(jnp.bfloat16)


def wide(array):
    return array.astype(jnp.float32)


def dot(left, right):
    return jnp.dot(left, right, preferred_element_type=jnp.float32)


def layer_kernel(
    n, per, tiles, scale,
    resid, q_one, q_two, kv, docs, lam, head_gain, norm_gain, taps_gate, taps_value,
    cosine, sine, turn, spread, out_hbm, gate_hbm, value_hbm, down_hbm,
    out,
    kv_all, docs_all, docs_row, out_w, heads, part_one, got_one, sum_one, got_far, mid,
    rows_all, up_w, down_w, hidden, part_two, got_two, sum_far, got_x, sum_z, own_z, got_z,
    d_send, d_recv, k_send, k_recv, o_sem, l_sem, w_send, w_recv, y_send,
    c1_send, c1_recv, x1_send, x1_recv,
    az_send, az_recv, ax_send, ax_recv, ac_send, ac_recv,
    c2_send, c2_recv, x2_send, x2_recv, z2_send, z2_recv,
):
    z, g = lax.axis_index("sp"), lax.axis_index("grp")
    tp, near, far = partners()
    low, high = lax.rem(tp, 2), tp // 2
    diag = (1 - high) * 2 + 1 - low
    other = {"grp": 1 - g}
    spare = per * n - tiles
    rows, depth, columns = kv.shape[1], gate_hbm.shape[0], down_hbm.shape[1]
    features, total = resid.shape[1], n * rows
    peers = [lax.rem(z + k, n) for k in range(1, n)]
    greet([{"sp": peer} for peer in peers] + [{"tp": near}, {"tp": far}, other])

    def rows_at(block):
        return pl.ds(pl.multiple_of(block * rows, rows), rows)

    def doc_copy(k, source, peer):
        return remote(docs, docs_all.at[source], d_send.at[k], d_recv.at[source], {"sp": peer})

    def key_copy(k, source, peer):
        there = kv_all.at[:, rows_at(source)]
        return remote(kv, there, k_send.at[k], k_recv.at[source], {"sp": peer})

    for k, peer in enumerate(peers):
        doc_copy(k, z, peer).start()
    for k, peer in reversed(list(enumerate(peers))):

        @pl.when(peer > z)
        def _():
            key_copy(k, z, peer).start()

    out_copy = pltpu.make_async_copy(out_hbm, out_w, o_sem)
    out_copy.start()

    def tile_of(block, k):
        return per * block + k - low * spare

    def valid(block, k):
        tile = tile_of(block, k)
        return (tile >= 0) & (tile < tiles)

    def weight_from(m, tile):
        at = pl.ds(pl.multiple_of(jnp.clip(tile, 0, tiles - 1) * LANES, LANES), LANES)
        if m == 2:
            return down_hbm.at[at, :]
        return (gate_hbm, value_hbm)[m].at[:, at]

    def weight_to(m, source, k):
        if m == 2:
            across = pl.ds(pl.multiple_of(source * columns, columns), columns)
            return down_w.at[pl.ds(k * LANES, LANES), across]
        along = pl.ds(pl.multiple_of(source * depth, depth), depth)
        return up_w.at[along, pl.ds((2 * k + m) * LANES, LANES)]

    def over_z(m, k, source, dest):
        return lax.rem(k + m + source + dest, 2) == g

    def z_copy(m, k, peer):
        return remote(
            weight_from(m, tile_of(peer, k)), weight_to(m, z, k),
            w_send.at[peer, 3 * k + m], w_recv.at[z, 3 * k + m], {"sp": peer},
        )

    def y_copy(m, k, source):
        block = weight_to(m, source, k)
        at = 3 * k + m
        return remote(block, block, y_send.at[source, at], w_recv.at[source, at], other)

    def own_copy(m, k):
        return pltpu.make_async_copy(
            weight_from(m, tile_of(z, k)), weight_to(m, z, k), l_sem.at[3 * k + m]
        )

    def when_sent(m, k, act):
        for peer in peers:

            @pl.when(valid(peer, k) & over_z(m, k, z, peer))
            def _():
                act(z_copy(m, k, peer))

    def when_got(m, k, first, act):
        for source in reversed(peers):
            hop = over_z(m, k, source, z)

            @pl.when(valid(z, k) & (hop if first else jnp.logical_not(hop)))
            def _():
                act(y_copy(m, k, source))

    def send(m, k):
        when_sent(m, k, lambda copy: copy.start())

    def relay(m, k):
        def act(copy):
            copy.wait_recv()
            copy.start()

        when_got(m, k, True, act)

    def settle(m, k):
        when_got(m, k, False, lambda copy: copy.wait_recv())

        @pl.when(valid(z, k))
        def _():
            own_copy(m, k).wait()

    for k in range(per):
        for m in (0, 1):
            send(m, k)
    for k in range(per):

        @pl.when(valid(z, k))
        def _():
            for m in (0, 1, 2):
                own_copy(m, k).start()

        @pl.when(jnp.logical_not(valid(z, k)))
        def _():
            pair = pl.ds(2 * k * LANES, 2 * LANES)
            up_w[:, pair] = jnp.zeros((up_w.shape[0], 2 * LANES), up_w.dtype)
            one = pl.ds(k * LANES, LANES)
            down_w[one, :] = jnp.zeros((LANES, down_w.shape[1]), down_w.dtype)

    docs_all[z] = docs[...]
    kv_all[:, rows_at(z)] = kv[...]
    for block in range(1, n):

        @pl.when(block > z)
        def _():
            blank = jnp.zeros((kv_all.shape[0], rows, kv_all.shape[2]), kv_all.dtype)
            kv_all[:, pl.ds(block * rows, rows)] = blank

    for k, source in enumerate(peers):
        doc_copy(k, source, source).wait_recv()
    docs_row[...] = functools.reduce(lambda a, b: a + b, [docs_all[i] for i in range(n)])
    for k, source in enumerate(peers):

        @pl.when(source < z)
        def _():
            key_copy(k, source, source).wait_recv()

    def iota(height, width, axis):
        return lax.broadcasted_iota(jnp.int32, (height, width), axis)

    def attend(seq, carry):
        doc_row = docs_row[seq][0:1]
        at_query = iota(rows, total, 0) + z * rows
        at_key = iota(rows, total, 1)
        doc_query = jnp.sum(jnp.where(at_key == at_query, doc_row, 0.0), axis=1, keepdims=True)
        allowed = (at_key <= at_query) & (doc_row == doc_query)
        bias = jnp.where(allowed, 0.0, NEG_BIG)
        bias = jnp.concatenate([bias] * 4, axis=0)
        q_cos, q_sin = cosine[rows_at(z)], sine[rows_at(z)]
        packed = kv_all[seq]
        spun = dot(packed[:, :LANES], spread[...])
        vals = wide(packed[:, LANES:])
        swapped = pltpu.roll(vals, LANES // 2, 1)
        lane = iota(total, LANES, 1)
        queries, keys = [], []
        width = cosine.shape[1]
        for index, source in enumerate((q_one, q_two)):
            block = source[seq]
            turned = wide(block) * q_cos + dot(block, turn[...]) * q_sin
            queries.append(rounded(turned))
            start = 2 * index * width
            straight = spun[:, start : start + width]
            crossed = spun[:, start + width : start + 2 * width]
            keys.append(rounded(straight * cosine[...] + crossed * sine[...]))
        q_lane = iota(rows, LANES, 1) // (LANES // 4)
        row4 = iota(4 * rows, 1, 0) // rows
        half_lane = iota(2 * rows, LANES, 1) < LANES // 2
        for c in range(2):
            across = slice(c * LANES, (c + 1) * LANES)
            pair = (vals, swapped) if c == 0 else (swapped, vals)
            both = rounded(jnp.where(lane < LANES // 2, pair[0], pair[1]))
            found = []
            for query, key in zip(queries, keys):
                local = wide(query[:, across])
                stack = jnp.concatenate(
                    [rounded(jnp.where(q_lane == j, local, 0.0)) for j in (0, 2, 1, 3)], axis=0
                )
                scores = lax.dot_general(
                    stack, key[:, across], (((1,), (1,)), ((), ())),
                    preferred_element_type=jnp.float32,
                )
                scores = scores * scale + bias
                expd = jnp.exp(scores - jnp.max(scores, axis=1, keepdims=True))
                summed = jnp.sum(expd, axis=1, keepdims=True)
                found.append(dot(rounded(expd), both) / summed)
            weights = jnp.where(
                row4 == 0, lam[4 * c],
                jnp.where(
                    row4 == 1, lam[4 * c + 2],
                    jnp.where(row4 == 2, lam[4 * c + 1], lam[4 * c + 3]),
                ),
            )
            mixed = found[0] - weights * found[1]
            meansq = jnp.sum(mixed * mixed, axis=1, keepdims=True) * (1.0 / LANES)
            normed = mixed * lax.rsqrt(meansq + NORM_EPS) * head_gain[...]
            merged = rounded(jnp.where(half_lane, normed[: 2 * rows], normed[2 * rows :]))
            base = 2 * c * LANES
            heads[seq, :, base : base + LANES] = merged[:rows]
            heads[seq, :, base + LANES : base + 2 * LANES] = merged[rows:]
        return carry

    lax.fori_loop(0, kv.shape[0], attend, 0)
    relay(0, 0)
    relay(1, 0)

    out_copy.wait()
    halves = got_one.shape[0]
    width = features // halves

    def c1_copy(i):
        cols = pl.ds(i * width, width)
        return remote(
            part_one.at[:, 1 - low, :, cols], got_one.at[i], c1_send.at[i], c1_recv.at[i], {"tp": near}
        )

    def x1_copy(i):
        return remote(sum_one.at[i], got_far.at[i], x1_send.at[i], x1_recv.at[i], {"tp": far})

    flat = heads[...].reshape(4 * rows, heads.shape[2])
    for i in range(halves):
        cols = pl.ds(i * width, width)
        made = rounded(dot(flat, out_w[:, cols]))
        part_one[:, :, :, cols] = made.reshape(2, 2, rows, width)
        c1_copy(i).start()
    for i in range(halves):
        cols = pl.ds(i * width, width)
        c1_copy(i).wait_recv()
        sum_one[i] = rounded(wide(part_one[1 - high, low, :, cols]) + wide(got_one[i, 1 - high]))
        x1_copy(i).start()
        kept = wide(part_one[high, low, :, cols]) + wide(got_one[i, high])
        mid[:, cols] = wide(resid[:, cols]) + kept
    relay(0, 1)
    relay(1, 1)
    for i in range(halves):
        cols = pl.ds(i * width, width)
        x1_copy(i).wait_recv()
        mid[:, cols] = mid[:, cols] + wide(got_far[i])
    held = mid[...]
    meansq = jnp.mean(held * held, axis=1, keepdims=True)
    rows_all[tp, rows_at(z)] = rounded(held * lax.rsqrt(meansq + NORM_EPS) * norm_gain[...])

    def x_copy(owner, block):
        part = rows_all.at[owner, rows_at(block)]
        return remote(part, part, ax_send.at[block], ax_recv.at[block], {"tp": far})

    def c_copy(owner, hop, block):
        part = rows_all.at[owner, rows_at(block)]
        return remote(part, part, ac_send.at[hop, block], ac_recv.at[hop, block], {"tp": near})

    def chain_copy(way, block):
        part = rows_all.at[tp, rows_at(block)]
        peer = lax.rem(z + (1 if way == 0 else n - 1), n)
        return remote(part, part, az_send.at[way, block], az_recv.at[block], {"sp": peer})

    def pass_on(block):
        @pl.when(z >= block)
        def _():
            @pl.when(z < n - 1)
            def _():
                chain_copy(0, block).start()

        @pl.when(z <= block)
        def _():
            @pl.when(z > 0)
            def _():
                chain_copy(1, block).start()

        x_copy(tp, block).start()
        c_copy(tp, 0, block).start()

    pass_on(z)
    send(2, 0)
    for step in range(1, n):
        for block in (z - step, z + step):

            @pl.when((block >= 0) & (block < n))
            def _():
                chain_copy(0, block).wait_recv()
                pass_on(block)

        if step < per:
            send(2, step)
    for k in range(n, per):
        send(2, k)
    for k in range(2, per):
        relay(0, k)
        relay(1, k)
    relay(2, 0)
    for step in range(n):
        for block in (z - step, z + step) if step else (z,):

            @pl.when((block >= 0) & (block < n))
            def _():
                x_copy(far, block).wait_recv()
                c_copy(far, 1, block).start()

    relay(2, 1)
    for block in range(n):
        c_copy(near, 0, block).wait_recv()
        c_copy(diag, 1, block).wait_recv()
    for k in range(per):
        for m in (0, 1):
            settle(m, k)

    def lift(seq, carry):
        doc_row = docs_row[seq][0:1]
        at_row, at_col = iota(total, total, 0), iota(total, total, 1)
        doc_col = jnp.sum(jnp.where(at_row == at_col, doc_row, 0.0), axis=1, keepdims=True)
        same = jnp.where(doc_row == doc_col, 1.0, 0.0)
        back_one, back_two = [
            jnp.sum(jnp.where(at_col == at_row - back, same, 0.0), axis=1, keepdims=True)
            for back in (1, 2)
        ]

        def depthwise_of(current, taps):
            shown = wide(rounded(current))
            return (
                taps[2:3] * shown
                + taps[1:2] * (pltpu.roll(shown, 1, 0) * back_one)
                + taps[0:1] * (pltpu.roll(shown, 2, 0) * back_two)
            )

        for k in range(per):
            made = dot(rows_all[seq], up_w[:, 2 * k * LANES : (2 * k + 2) * LANES])
            tile = jnp.clip(tile_of(z, k), 0, tiles - 1)
            at = pl.ds(pl.multiple_of(tile * LANES, LANES), LANES)
            conv_g = depthwise_of(made[:, :LANES], taps_gate[:, at])
            conv_v = depthwise_of(made[:, LANES:], taps_value[:, at])
            unit = conv_g / (1.0 + jnp.exp(-conv_g)) * conv_v
            hidden[seq, :, k * LANES : (k + 1) * LANES] = rounded(unit)
        return carry

    lax.fori_loop(0, rows_all.shape[0], lift, 0)
    for k in range(2, per):
        relay(2, k)
    for k in range(per):
        settle(2, k)

    def c2_copy(i, seq):
        return remote(part_two.at[seq], got_two.at[i], c2_send.at[i], c2_recv.at[i], {"tp": near})

    chunk = 512 if features % 512 == 0 else features

    def lower(i, carry):
        seq = lax.rem(high + 1 - lax.rem(i, 2), 2) * 2 + lax.rem(low + 1 - i // 2, 2)
        for c in range(features // chunk):
            cols = slice(c * chunk, (c + 1) * chunk)
            part_two[seq, :, cols] = rounded(dot(hidden[seq], down_w[:, cols]))

        @pl.when(i < 2)
        def _():
            c2_copy(i, seq).start()

        return carry

    lax.fori_loop(0, rows_all.shape[0], lower, 0)

    def x2_copy(block):
        return remote(
            sum_far.at[block], got_x.at[block], x2_send.at[block], x2_recv.at[block], {"tp": far}
        )

    def z2_copy(k, block, source):
        return remote(
            sum_z.at[k], got_z.at[source], z2_send.at[k], z2_recv.at[source], {"sp": block}
        )

    shifts = sorted(range(n), key=lambda k: (k == 0, -min(k, n - k)))
    c2_copy(0, diag).wait_recv()
    for shift in shifts:
        block = lax.rem(z + shift, n)
        there = rows_at(block)
        sum_far[block] = rounded(wide(part_two[far, there]) + wide(got_two[0, there]))
        x2_copy(block).start()
    c2_copy(1, near).wait_recv()
    for k, shift in enumerate(shifts):
        block = lax.rem(z + shift, n)
        there = rows_at(block)
        x2_copy(block).wait_recv()
        both = wide(part_two[tp, there]) + wide(got_two[1, there]) + wide(got_x[block])
        if shift:
            sum_z[k] = rounded(both)
            z2_copy(k, block, z).start()
        else:
            own_z[...] = mid[...] + both
    answer = own_z[...]
    for k, source in enumerate(peers):
        z2_copy(k, source, source).wait_recv()
        answer = answer + wide(got_z[source])
    out[...] = answer.astype(out.dtype)

    for k, peer in enumerate(peers):
        doc_copy(k, z, peer).wait_send()

        @pl.when(peer > z)
        def _():
            key_copy(k, z, peer).wait_send()

        z2_copy(k, peer, z).wait_send()
    for k in range(per):
        for m in (0, 1, 2):
            when_sent(m, k, lambda copy: copy.wait_send())
            when_got(m, k, True, lambda copy: copy.wait_send())
    for i in range(halves):
        c1_copy(i).wait_send()
        x1_copy(i).wait_send()
    for block in range(n):

        @pl.when((z >= block) & (z < n - 1))
        def _():
            chain_copy(0, block).wait_send()

        @pl.when((z <= block) & (z > 0))
        def _():
            chain_copy(1, block).wait_send()

        x_copy(tp, block).wait_send()
        c_copy(tp, 0, block).wait_send()
        c_copy(far, 1, block).wait_send()
        x2_copy(block).wait_send()
    c2_copy(0, diag).wait_send()
    c2_copy(1, near).wait_send()


def rope_tables(total, width, copies):
    half = width // 2
    freqs = np.float32(ROPE_BASE) ** (-np.arange(half, dtype=np.float32) * np.float32(2.0) / np.float32(width))
    angles = np.arange(total, dtype=np.float32)[:, None] * freqs.astype(np.float32)[None, :]
    tile = lambda table: np.tile(table.astype(np.float32), (1, 2 * copies))
    return tile(np.cos(angles)), tile(np.sin(angles))


def turn_matrix(width):
    half = width // 2
    at = np.arange(width)
    source = np.where(at < half, at + half, at - half)
    sign = np.where(at < half, -1.0, 1.0)
    return np.where(at[:, None] == source[None, :], sign[None, :], 0.0)


def spread_matrix(width, group, kv_local):
    straight = np.kron(np.eye(kv_local), np.tile(np.eye(width), (1, group)))
    crossed = np.kron(np.eye(kv_local), np.tile(turn_matrix(width), (1, group)))
    both = np.concatenate([straight, crossed], axis=1)
    return np.kron(np.eye(2), both)


def kernel_fits(resid_in, query_one, key_one, value, lam, gate_weight):
    heads = lam.shape[0]
    width = query_one.shape[2] // heads
    kv_local = key_one.shape[2] // width
    group = heads // kv_local
    seqs, rows = query_one.shape[:2]
    return (
        lax.axis_size("tp") == 4
        and lax.axis_size("grp") == 2
        and 2 <= lax.axis_size("sp") <= 8
        and kv_local == 2
        and group == 4
        and group * width == LANES
        and value.shape[2] == LANES
        and seqs == 4
        and resid_in.shape[0] == 1
        and rows % 16 == 0
        and rows * lax.axis_size("sp") <= 256
        and gate_weight.shape[0] <= 512
        and gate_weight.shape[1] % LANES == 0
        and gate_weight.shape[1] <= 1536
        and resid_in.shape[2] <= 2048
    )


def whole_layer(
    resid_in, query_one, key_one, query_two, key_two, value, lam, head_gain, doc_ids,
    out_weight, norm_gain, gate_weight, value_weight, conv_gate, conv_value, down_weight,
):
    n = lax.axis_size("sp")
    z = lax.axis_index("sp")
    seqs, rows = query_one.shape[:2]
    heads = lam.shape[0]
    width = query_one.shape[2] // heads
    kv_local = key_one.shape[2] // width
    group = heads // kv_local
    features, total = resid_in.shape[2], n * rows
    depth, columns = gate_weight.shape[0], down_weight.shape[1]
    tiles = gate_weight.shape[1] // LANES
    per = -(-tiles // n)
    kv = jnp.concatenate([key_one, key_two, value], axis=-1)
    docs = lax.dynamic_update_slice(
        jnp.zeros((seqs, total), jnp.float32), doc_ids.astype(jnp.float32), (0, z * rows)
    )
    docs = jnp.broadcast_to(docs[:, None], (seqs, 8, total))
    cosine, sine = rope_tables(total, width, heads)
    turn = np.kron(np.eye(heads), turn_matrix(width))
    spread = spread_matrix(width, group, kv_local)
    gain = jnp.concatenate([head_gain, head_gain])[None]
    halves = 2
    bf16, f32 = jnp.bfloat16, jnp.float32
    dma = pltpu.SemaphoreType.DMA
    vmem = pltpu.VMEM
    scratch = [
        vmem((seqs, total, kv.shape[2]), bf16),
        vmem((n, seqs, 8, total), f32),
        vmem((seqs, 8, total), f32),
        vmem(out_weight.shape, bf16),
        vmem((seqs, rows, out_weight.shape[0]), bf16),
        vmem((2, 2, rows, features), bf16),
        vmem((halves, 2, rows, features // halves), bf16),
        vmem((halves, rows, features // halves), bf16),
        vmem((halves, rows, features // halves), bf16),
        vmem((rows, features), f32),
        vmem((seqs, total, features), bf16),
        vmem((n * depth, 2 * per * LANES), bf16),
        vmem((per * LANES, n * columns), bf16),
        vmem((seqs, total, per * LANES), bf16),
        vmem((seqs, total, features), bf16),
        vmem((2, total, features), bf16),
        vmem((n, rows, features), bf16),
        vmem((n, rows, features), bf16),
        vmem((n, rows, features), bf16),
        vmem((rows, features), f32),
        vmem((n, rows, features), bf16),
        dma((n,)), dma((n,)), dma((n,)), dma((n,)), dma, dma((3 * per,)),
        dma((n, 3 * per)), dma((n, 3 * per)), dma((n, 3 * per)),
        dma((halves,)), dma((halves,)), dma((halves,)), dma((halves,)),
        dma((2, n)), dma((n,)), dma((n,)), dma((n,)), dma((2, n)), dma((2, n)),
        dma((2,)), dma((2,)), dma((n,)), dma((n,)), dma((n,)), dma((n,)),
    ]
    out = pl.pallas_call(
        functools.partial(layer_kernel, n, per, tiles, width ** (-0.5)),
        out_shape=jax.ShapeDtypeStruct((rows, features), resid_in.dtype),
        in_specs=[VMEM] * 5 + [SMEM] + [VMEM] * 8 + [HBM] * 4,
        out_specs=VMEM,
        scratch_shapes=scratch,
        compiler_params=pltpu.CompilerParams(
            collective_id=5, has_side_effects=True, vmem_limit_bytes=60 * 2**20
        ),
        name="whole_layer",
    )(
        resid_in.reshape(rows, features), query_one, query_two, kv, docs, lam, gain,
        norm_gain[None], conv_gate, conv_value,
        jnp.asarray(cosine), jnp.asarray(sine), jnp.asarray(turn, bf16), jnp.asarray(spread, bf16),
        out_weight, gate_weight, value_weight, down_weight,
    )
    return out.reshape(resid_in.shape)


def per_device_apart(
    resid_in,
    query_one,
    key_one,
    query_two,
    key_two,
    value,
    lam,
    head_gain,
    doc_ids,
    out_weight,
    norm_gain,
    gate_weight,
    value_weight,
    conv_gate,
    conv_value,
    down_weight,
):
    n_sp = lax.axis_size("sp")
    me = lax.axis_index("sp")
    depth, width = gate_weight.shape
    share = width // n_sp
    copies = lax.axis_size("grp")

    def cut(weight, row, column, size):
        return lax.dynamic_slice(weight, (row, column), size)

    def up_piece(dest, part):
        size = (depth // copies, share)
        row, column = part * size[0], dest * share
        return jnp.stack([cut(gate_weight, row, column, size), cut(value_weight, row, column, size)])

    def up_whole(dest):
        return jnp.stack([up_piece(dest, part) for part in range(copies)])

    def down_piece(dest, part):
        size = (share // copies, down_weight.shape[1])
        return cut(down_weight, dest * share + part * size[0], 0, size)

    def down_whole(dest):
        return jnp.stack([down_piece(dest, part) for part in range(copies)])

    up_all = exchange(up_piece, up_whole)
    down_all = exchange(down_piece, down_whole)
    gate_all = up_all[:, :, 0].reshape(-1, share)
    value_all = up_all[:, :, 1].reshape(-1, share)
    down_full = jnp.transpose(down_all, (1, 2, 0, 3)).reshape(share, -1)
    seqs = query_one.shape[0]
    rows = query_one.shape[1]
    heads = lam.shape[0]
    key_width = query_one.shape[2] // heads
    kv_local = key_one.shape[2] // key_width
    group = heads // kv_local
    head_width = value.shape[2] // kv_local
    scale = key_width ** (-0.5)
    positions = lax.axis_index("sp") * rows + jnp.arange(rows, dtype=jnp.int32)
    q_first = rotate(query_one, positions, heads).reshape(seqs, rows, kv_local, group, key_width)
    q_second = rotate(query_two, positions, heads).reshape(seqs, rows, kv_local, group, key_width)
    k_first = rotate(key_one, positions, kv_local).reshape(seqs, rows, kv_local * key_width)
    k_second = rotate(key_two, positions, kv_local).reshape(seqs, rows, kv_local * key_width)
    start_state = (
        jnp.full((seqs, kv_local, group, rows), NEG_BIG, jnp.float32),
        jnp.zeros((seqs, kv_local, group, rows), jnp.float32),
        jnp.zeros((seqs, kv_local, group, rows, head_width), jnp.float32),
    )
    packed = jnp.concatenate(
        [k_first, k_second, value, doc_ids.astype(jnp.bfloat16)[..., None]], axis=-1
    )
    packed = gather_sp(packed)
    key_cols = k_first.shape[2]
    keys_one = packed[..., :key_cols]
    keys_two = packed[..., key_cols : 2 * key_cols]
    vals = packed[..., 2 * key_cols : -1]
    docs = packed[..., -1].astype(jnp.int32)
    count = keys_one.shape[1]
    step_len = math.gcd(count, 512)

    def inner(state, index):
        offset = index * step_len
        ka = lax.dynamic_slice_in_dim(keys_one, offset, step_len, 1).reshape(
            seqs, step_len, kv_local, key_width
        )
        kb = lax.dynamic_slice_in_dim(keys_two, offset, step_len, 1).reshape(
            seqs, step_len, kv_local, key_width
        )
        va = lax.dynamic_slice_in_dim(vals, offset, step_len, 1).reshape(
            seqs, step_len, kv_local, head_width
        )
        dpiece = lax.dynamic_slice_in_dim(docs, offset, step_len, 1)
        key_pos = offset + jnp.arange(step_len, dtype=jnp.int32)
        allowed = (key_pos[None, None, :] <= positions[None, :, None]) & (
            dpiece[:, None, :] == doc_ids[:, :, None]
        )
        first = online_step(state[0], q_first, ka, va, allowed, scale)
        second = online_step(state[1], q_second, kb, va, allowed, scale)
        return ((first, second), None)

    def run(state):
        return lax.scan(inner, state, jnp.arange(count // step_len))[0]

    first, second = lax.cond(
        jnp.int32(0) <= positions[rows - 1], run, lambda state: state, (start_state, start_state)
    )
    weights = lam.reshape(kv_local, group)[None, :, :, None, None]
    mixed = first[2] / first[1][..., None] - weights * (second[2] / second[1][..., None])
    meansq = jnp.mean(mixed * mixed, axis=-1, keepdims=True)
    normed_heads = mixed * lax.rsqrt(meansq + NORM_EPS) * head_gain
    heads_out = jnp.transpose(normed_heads, (0, 3, 1, 2, 4)).reshape(
        seqs * rows, heads * head_width
    )
    heads_out = heads_out.astype(jnp.bfloat16)
    own = resid_in.shape[0]
    features = resid_in.shape[2]
    proj = jnp.dot(heads_out, out_weight, preferred_element_type=jnp.float32).astype(jnp.bfloat16)
    mid = reduce_rows(
        proj.reshape(-1, 1, own * rows, features),
        resid_in.astype(jnp.float32).reshape(own * rows, features),
        jnp.float32,
        False,
    )
    meansq_mid = jnp.mean(mid * mid, axis=-1, keepdims=True)
    normed = (mid * lax.rsqrt(meansq_mid + NORM_EPS) * norm_gain).astype(jnp.bfloat16)
    gathered = gather_rows(normed).reshape(-1, n_sp, own, rows, features)
    full_rows = jnp.transpose(gathered, (0, 2, 1, 3, 4)).reshape(-1, features)
    total_rows = n_sp * rows
    start = me * share
    taps_gate = lax.dynamic_slice_in_dim(conv_gate, start, share, 1)
    taps_value = lax.dynamic_slice_in_dim(conv_value, start, share, 1)
    up_gate = jnp.dot(full_rows, gate_all, preferred_element_type=jnp.float32)
    up_value = jnp.dot(full_rows, value_all, preferred_element_type=jnp.float32)
    up_gate = up_gate.astype(jnp.bfloat16).reshape(seqs, total_rows, share)
    up_value = up_value.astype(jnp.bfloat16).reshape(seqs, total_rows, share)
    conv_g = depthwise(up_gate, taps_gate, docs)
    conv_v = depthwise(up_value, taps_value, docs)
    hidden = (jax.nn.silu(conv_g) * conv_v).astype(jnp.bfloat16)
    hidden = hidden.reshape(-1, own, n_sp, rows, share)
    hidden = jnp.transpose(hidden, (0, 2, 1, 3, 4)).reshape(-1, share)
    partial_down = jnp.dot(hidden, down_full, preferred_element_type=jnp.float32)
    partial_down = partial_down.astype(jnp.bfloat16).reshape(-1, n_sp, own * rows, features)
    return reduce_rows(partial_down, mid, jnp.bfloat16, True).reshape(resid_in.shape)


def per_device(*args):
    resid_in, query_one, key_one, value, lam, gate_weight = [args[i] for i in (0, 1, 2, 5, 6, 11)]
    if kernel_fits(resid_in, query_one, key_one, value, lam, gate_weight):
        return whole_layer(*args)
    return per_device_apart(*args)


def solution(mesh):
    placed = (
        P(("grp", "tp"), "sp", None),
        P("grp", "sp", "tp"),
        P("grp", "sp", "tp"),
        P("grp", "sp", "tp"),
        P("grp", "sp", "tp"),
        P("grp", "sp", "tp"),
        P("tp"),
        P(),
        P("grp", "sp"),
        P("tp", None),
        P(),
        P("sp", "tp"),
        P("sp", "tp"),
        P(None, "tp"),
        P(None, "tp"),
        P("tp", "sp"),
    )
    return jax.shard_map(
        per_device,
        mesh=mesh,
        in_specs=placed,
        out_specs=P(("grp", "tp"), "sp", None),
        check_vma=False,
    )
```

```python
import functools
import math

import jax
import jax.numpy as jnp
import numpy as np
from jax import lax
from jax.experimental import pallas as pl
from jax.experimental.pallas import tpu as pltpu
from jax.sharding import PartitionSpec as P

NEG_BIG = -1e30
NORM_EPS = 1e-06
ROPE_BASE = 500000.0


MESH = pl.DeviceIdType.MESH
VMEM = pl.BlockSpec(memory_space=pltpu.VMEM)


def greet(devices):
    barrier = pltpu.get_barrier_semaphore()
    for device in devices:
        pl.semaphore_signal(barrier, inc=1, device_id=device, device_id_type=MESH)
    pl.semaphore_wait(barrier, len(devices))


def remote(src, dst, send_sem, recv_sem, device):
    return pltpu.make_async_remote_copy(
        src_ref=src,
        dst_ref=dst,
        send_sem=send_sem,
        recv_sem=recv_sem,
        device_id=device,
        device_id_type=MESH,
    )


def partners():
    at = lax.axis_index("tp")
    return at, at + 1 - 2 * lax.rem(at, 2), lax.rem(at + 2, 4)


def spread_kernel(n, own_ref, out_ref, send_sem, recv_sem):
    me = lax.axis_index("sp")
    peers = [lax.rem(me + shift, n) for shift in range(1, n)]
    greet([{"sp": peer} for peer in peers])
    copies = []
    for k, peer in enumerate(peers):
        copy = remote(
            own_ref, out_ref.at[:, me], send_sem.at[k], recv_sem.at[k], {"sp": peer}
        )
        copy.start()
        copies.append(copy)
    out_ref[:, me] = own_ref[...]
    for copy in copies:
        copy.wait_recv()
    for copy in copies:
        copy.wait_send()


def gather_sp(own):
    n = lax.axis_size("sp")
    if n > 8:
        return lax.all_gather(own, "sp", axis=1, tiled=True)
    outer, rows, width = own.shape
    out = pl.pallas_call(
        functools.partial(spread_kernel, n),
        out_shape=jax.ShapeDtypeStruct((outer, n, rows, width), own.dtype),
        in_specs=[VMEM],
        out_specs=VMEM,
        scratch_shapes=[pltpu.SemaphoreType.DMA((n - 1,)), pltpu.SemaphoreType.DMA((n - 1,))],
        compiler_params=pltpu.CompilerParams(collective_id=1, has_side_effects=True),
        cost_estimate=pl.CostEstimate(flops=0, bytes_accessed=30_000_000, transcendentals=0),
        name="gather_sp",
    )(own)
    return out.reshape(outer, n * rows, width)


def rows_kernel(n, own_ref, out_ref, z_send, z_recv, x_send, x_recv, c_send, c_recv):
    me = lax.axis_index("sp")
    tp, near, far = partners()
    greet([{"tp": near}, {"tp": far}] + [{"sp": lax.rem(me + k, n)} for k in range(1, n)])
    sources = [lax.rem(me - k + n, n) for k in range(n)]
    z_copies = []
    for k in range(1, n):
        copy = remote(
            own_ref,
            out_ref.at[tp, me],
            z_send.at[k - 1],
            z_recv.at[k - 1],
            {"sp": lax.rem(me + k, n)},
        )
        z_copies.append(copy)

    def along(owner, k, send, recv, device):
        block = out_ref.at[owner, sources[k]]
        return remote(block, block, send, recv, device)

    x_copies = [remote(own_ref, out_ref.at[tp, me], x_send.at[0], x_recv.at[0], {"tp": far})]
    c_copies = [remote(own_ref, out_ref.at[tp, me], c_send.at[0], c_recv.at[0], {"tp": near})]
    for k in range(1, n):
        x_copies.append(along(tp, k, x_send.at[k], x_recv.at[k], {"tp": far}))
        c_copies.append(along(tp, k, c_send.at[k], c_recv.at[k], {"tp": near}))
    f_copies = [along(far, k, c_send.at[n + k], c_recv.at[n + k], {"tp": near}) for k in range(n)]
    x_copies[0].start()
    for copy in z_copies:
        copy.start()
    c_copies[0].start()
    out_ref[tp, me] = own_ref[...]
    for k in range(1, n):
        z_copies[k - 1].wait_recv()
        x_copies[k].start()
        c_copies[k].start()
    for k in range(n):
        x_copies[k].wait_recv()
        f_copies[k].start()
    for copy in c_copies + f_copies:
        copy.wait_recv()
    for copy in z_copies + x_copies + c_copies + f_copies:
        copy.wait_send()


def gather_rows(own):
    n, wide = lax.axis_size("sp"), lax.axis_size("tp")
    if n > 8 or wide != 4:
        out = lax.all_gather(own, ("tp", "sp"), axis=0)
        return out.reshape((wide, n) + own.shape)
    dma = pltpu.SemaphoreType.DMA
    return pl.pallas_call(
        functools.partial(rows_kernel, n),
        out_shape=jax.ShapeDtypeStruct((wide, n) + own.shape, own.dtype),
        in_specs=[VMEM],
        out_specs=VMEM,
        scratch_shapes=[
            dma((n - 1,)),
            dma((n - 1,)),
            dma((n,)),
            dma((n,)),
            dma((2 * n,)),
            dma((2 * n,)),
        ],
        compiler_params=pltpu.CompilerParams(collective_id=2, has_side_effects=True),
        cost_estimate=pl.CostEstimate(flops=0, bytes_accessed=90_000_000, transcendentals=0),
        name="gather_rows",
    )(own)


def reduce_kernel(
    n, chunks, part_ref, base_ref, out_ref, got_c, sum_c, got_x, sum_x, got_z,
    c_send, c_recv, x_send, x_recv, z_send, z_recv,
):
    tp, near, far = partners()
    low, high = lax.rem(tp, 2), tp // 2
    shifts = range(1, n)
    me = lax.axis_index("sp") if n > 1 else 0
    greet([{"tp": near}, {"tp": far}] + [{"sp": lax.rem(me + k, n)} for k in shifts])
    width = part_ref.shape[-1] // chunks
    cols = [pl.ds(i * width, width) for i in range(chunks)]
    c_copies, x_copies, z_copies = [], [], []
    for i in range(chunks):
        copy = remote(
            part_ref.at[:, 1 - low, :, :, cols[i]],
            got_c.at[i],
            c_send.at[i],
            c_recv.at[i],
            {"tp": near},
        )
        copy.start()
        c_copies.append(copy)
    for i in range(chunks):
        c_copies[i].wait_recv()
        mine = part_ref[:, low, :, :, cols[i]].astype(jnp.float32)
        sum_c[i] = (mine + got_c[i].astype(jnp.float32)).astype(sum_c.dtype)
        copy = remote(
            sum_c.at[i, 1 - high], got_x.at[i], x_send.at[i], x_recv.at[i], {"tp": far}
        )
        copy.start()
        x_copies.append(copy)
    for i in range(chunks):
        x_copies[i].wait_recv()
        both = sum_c[i, high].astype(jnp.float32) + got_x[i].astype(jnp.float32)
        sum_x[i] = both.astype(sum_x.dtype)
        for k in shifts:
            peer = lax.rem(me + k, n)
            copy = remote(
                sum_x.at[i, peer],
                got_z.at[i, k - 1],
                z_send.at[i, k - 1],
                z_recv.at[i, k - 1],
                {"sp": peer},
            )
            copy.start()
            z_copies.append(copy)
    for i in range(chunks):
        total = sum_x[i, me].astype(jnp.float32)
        for k in shifts:
            z_copies[i * (n - 1) + k - 1].wait_recv()
            total = total + got_z[i, k - 1].astype(jnp.float32)
        out_ref[:, cols[i]] = (base_ref[:, cols[i]] + total).astype(out_ref.dtype)
    for copy in c_copies + x_copies + z_copies:
        copy.wait_send()


def reduce_rows(part, base, dtype, over_sp):
    wide, n = part.shape[:2]
    if n > 8 or wide != 4 or part.size > 8_000_000:
        axes = ("tp", "sp") if over_sp else "tp"
        flat = part.reshape(-1, part.shape[-1])
        total = lax.psum_scatter(flat, axes, scatter_dimension=0, tiled=True)
        return (base + total.astype(jnp.float32)).astype(dtype)
    rows, columns = part.shape[2:]
    chunks = 4 if columns % 512 == 0 else 1
    width = columns // chunks
    dma = pltpu.SemaphoreType.DMA
    zs = max(n - 1, 1)
    return pl.pallas_call(
        functools.partial(reduce_kernel, n, chunks),
        out_shape=jax.ShapeDtypeStruct((rows, columns), dtype),
        in_specs=[VMEM, VMEM],
        out_specs=VMEM,
        scratch_shapes=[
            pltpu.VMEM((chunks, 2, n, rows, width), part.dtype),
            pltpu.VMEM((chunks, 2, n, rows, width), part.dtype),
            pltpu.VMEM((chunks, n, rows, width), part.dtype),
            pltpu.VMEM((chunks, n, rows, width), part.dtype),
            pltpu.VMEM((chunks, zs, rows, width), part.dtype),
            dma((chunks,)),
            dma((chunks,)),
            dma((chunks,)),
            dma((chunks,)),
            dma((chunks, zs)),
            dma((chunks, zs)),
        ],
        compiler_params=pltpu.CompilerParams(
            collective_id=3 if over_sp else 4, has_side_effects=True
        ),
        cost_estimate=pl.CostEstimate(flops=0, bytes_accessed=60_000_000, transcendentals=0),
        name="reduce_all" if over_sp else "reduce_tp",
    )(part.reshape(2, 2, n, rows, columns), base)


def rotate(block, positions, heads):
    columns = block.shape[-1]
    width = columns // heads
    half = width // 2
    at = jnp.arange(columns, dtype=jnp.int32)
    freqs = ROPE_BASE ** (-(at % half).astype(jnp.float32) * 2.0 / width)
    angles = positions.astype(jnp.float32)[:, None] * freqs[None, :]
    source = jnp.where(at % width < half, at + half, at - half)
    sign = jnp.where(at % width < half, -1.0, 1.0)
    turn = jnp.where(at[:, None] == source[None, :], sign[None, :], 0.0).astype(jnp.bfloat16)
    flat = block.reshape(-1, columns)
    other = jnp.dot(flat, turn, preferred_element_type=jnp.float32).reshape(block.shape)
    turned = block.astype(jnp.float32) * jnp.cos(angles) + other * jnp.sin(angles)
    return turned.astype(jnp.bfloat16)


def depthwise(current, taps, docs):
    shown = current.astype(jnp.float32)
    total = taps[2] * shown
    for back in (1, 2):
        moved = jnp.pad(shown, ((0, 0), (back, 0), (0, 0)))[:, : shown.shape[1]]
        moved_docs = jnp.pad(docs, ((0, 0), (back, 0)), constant_values=-1)[:, : docs.shape[1]]
        total = total + jnp.where((moved_docs == docs)[..., None], taps[2 - back] * moved, 0.0)
    return total


def cyclic(array, axis, by):
    length = lax.axis_size(axis)
    return lax.ppermute(array, axis, [(i, (i + by) % length) for i in range(length)])


def exchange(piece, whole):
    count = lax.axis_size("sp")
    copies = lax.axis_size("grp")
    me = lax.axis_index("sp")
    mine = lax.axis_index("grp")
    if count > 8:
        pieces = jnp.stack([whole(dest) for dest in range(count)], axis=0)
        return lax.all_to_all(pieces, "sp", 0, 0)
    parts = []
    for shift in range(1, count):
        part = piece(lax.rem(me + shift, count), mine)
        parts.append(cyclic(part, "sp", shift))
    got = [jnp.stack(parts, axis=0)]
    for turn in range(1, copies):
        got.append(cyclic(got[0], "grp", turn))
    got = jnp.stack(got, axis=1)
    held = whole(me)
    held = jnp.broadcast_to(held[None], (1,) + held.shape)
    order = [lax.rem(mine - share + copies, copies) for share in range(copies)]
    out = []
    for source in range(count):
        shift = lax.rem(me - source + count, count)
        there = lax.max(shift - 1, 0)
        shares = [
            lax.dynamic_slice(got, (there, at) + (0,) * (got.ndim - 2), (1, 1) + got.shape[2:])[0]
            for at in order
        ]
        out.append(jnp.where(shift == 0, held, jnp.concatenate(shares, axis=0)[None]))
    return jnp.concatenate(out, axis=0)


def online_step(state, queries, keys, vals, allowed, scale):
    peak, total, accum = state
    scores = (
        jnp.einsum("sqhgd,skhd->shgqk", queries, keys, preferred_element_type=jnp.float32) * scale
    )
    mask = allowed[:, None, None]
    scores = jnp.where(mask, scores, NEG_BIG)
    new_peak = jnp.maximum(peak, jnp.max(scores, axis=-1))
    expd = jnp.where(mask, jnp.exp(scores - new_peak[..., None]), 0.0)
    fade = jnp.exp(peak - new_peak)
    new_total = total * fade + jnp.sum(expd, axis=-1)
    update = jnp.einsum(
        "shgqk,skhd->shgqd", expd.astype(jnp.bfloat16), vals, preferred_element_type=jnp.float32
    )
    return (new_peak, new_total, accum * fade[..., None] + update)


HBM = pl.BlockSpec(memory_space=pltpu.HBM)
SMEM = pl.BlockSpec(memory_space=pltpu.SMEM)
LANES = 128


def rounded(array):
    return array.astype(jnp.bfloat16)


def wide(array):
    return array.astype(jnp.float32)


def dot(left, right):
    return jnp.dot(left, right, preferred_element_type=jnp.float32)


class Phases:
    def __init__(self):
        self.open = None

    def __call__(self, name):
        if self.open is not None:
            self.open.__exit__(None, None, None)
        self.open = jax.named_scope(name) if name else None
        if name:
            self.open.__enter__()


def layer_kernel(
    n, per, tiles, scale,
    resid, q_one, q_two, k_one, k_two, vals_own, doc_ids, lam, head_gain, norm_gain,
    taps_gate, taps_value, cosine, sine, turn, spread, join, out_hbm, gate_hbm, value_hbm, down_hbm,
    out,
    kv_all, docs_all, docs_row, out_w, heads, part_one, got_one, sum_one, got_far, mid,
    rows_all, up_w, down_w, hidden, part_two, got_two, sum_far, got_x, sum_z, own_z, got_z,
    d_send, d_recv, k_send, k_recv, o_sem, l_sem, w_send, w_recv, y_send,
    c1_send, c1_recv, x1_send, x1_recv,
    az_send, az_recv, ax_send, ax_recv, ac_send, ac_recv,
    c2_send, c2_recv, x2_send, x2_recv, z2_send, z2_recv,
):
    phase = Phases()
    z, g = lax.axis_index("sp"), lax.axis_index("grp")
    tp, near, far = partners()
    low, high = lax.rem(tp, 2), tp // 2
    diag = (1 - high) * 2 + 1 - low
    other = {"grp": 1 - g}
    spare = per * n - tiles
    seqs, rows = q_one.shape[:2]
    depth, columns = gate_hbm.shape[0], down_hbm.shape[1]
    features, total = resid.shape[1], n * rows
    peers = [lax.rem(z + k, n) for k in range(1, n)]
    phase("greet")
    greet([{"sp": peer} for peer in peers] + [{"tp": near}, {"tp": far}, other])

    def rows_at(block):
        return pl.ds(pl.multiple_of(block * rows, rows), rows)

    phase("send_kv")
    def doc_copy(k, source, peer):
        part = docs_all.at[source]
        return remote(part, part, d_send.at[k], d_recv.at[source], {"sp": peer})

    def key_copy(block, p):
        half = seqs // 2
        part = kv_all.at[p * half : (p + 1) * half, rows_at(block)]
        peer = lax.rem(z + 1, n)
        return remote(part, part, k_send.at[block, p], k_recv.at[block, p], {"sp": peer})

    for seq in range(seqs):
        paired = dot(k_one[seq], join[0]) + dot(k_two[seq], join[1])
        kv_all[seq, rows_at(z), :LANES] = rounded(paired)
        kv_all[seq, rows_at(z), LANES:] = vals_own[seq]

    @pl.when(z < n - 1)
    def _():
        for p in (0, 1):
            key_copy(z, p).start()

    slot = lax.broadcasted_iota(jnp.int32, (rows, total), 1)
    spot = lax.broadcasted_iota(jnp.int32, (rows, total), 0) + z * rows
    place = jnp.where(slot == spot, 1.0, 0.0).astype(jnp.bfloat16)
    padded = jnp.concatenate([wide(doc_ids[...]), jnp.zeros((8 - seqs, rows), jnp.float32)], axis=0)
    docs_all[z] = dot(rounded(padded), place)
    for k, peer in enumerate(peers):
        doc_copy(k, z, peer).start()

    out_copy = pltpu.make_async_copy(out_hbm, out_w, o_sem)
    out_copy.start()

    def tile_of(block, k):
        return per * block + k - low * spare

    def valid(block, k):
        tile = tile_of(block, k)
        return (tile >= 0) & (tile < tiles)

    def weight_from(m, tile):
        at = pl.ds(pl.multiple_of(jnp.clip(tile, 0, tiles - 1) * LANES, LANES), LANES)
        if m == 2:
            return down_hbm.at[at, :]
        return (gate_hbm, value_hbm)[m].at[:, at]

    def weight_to(m, source, k):
        if m == 2:
            across = pl.ds(pl.multiple_of(source * columns, columns), columns)
            return down_w.at[pl.ds(k * LANES, LANES), across]
        along = pl.ds(pl.multiple_of(source * depth, depth), depth)
        return up_w.at[along, pl.ds((2 * k + m) * LANES, LANES)]

    def over_z(m, k, source, dest):
        return lax.rem(k + m + source + dest, 2) == g

    def z_copy(m, k, peer):
        return remote(
            weight_from(m, tile_of(peer, k)), weight_to(m, z, k),
            w_send.at[peer, 3 * k + m], w_recv.at[z, 3 * k + m], {"sp": peer},
        )

    def y_copy(m, k, source):
        block = weight_to(m, source, k)
        at = 3 * k + m
        return remote(block, block, y_send.at[source, at], w_recv.at[source, at], other)

    def own_copy(m, k):
        return pltpu.make_async_copy(
            weight_from(m, tile_of(z, k)), weight_to(m, z, k), l_sem.at[3 * k + m]
        )

    def when_sent(m, k, act, way=None):
        for peer in peers:
            wanted = valid(peer, k) & over_z(m, k, z, peer)
            if way is not None:
                wanted = wanted & ((peer > z) if way else (peer < z))

            @pl.when(wanted)
            def _():
                act(z_copy(m, k, peer))

    def when_got(m, k, first, act):
        for source in reversed(peers):
            hop = over_z(m, k, source, z)

            @pl.when(valid(z, k) & (hop if first else jnp.logical_not(hop)))
            def _():
                act(y_copy(m, k, source))

    def send(m, k, way=None):
        when_sent(m, k, lambda copy: copy.start(), way)

    def relay(m, k):
        def act(copy):
            copy.wait_recv()
            copy.start()

        when_got(m, k, True, act)

    def settle(m, k):
        when_got(m, k, False, lambda copy: copy.wait_recv())

        @pl.when(valid(z, k))
        def _():
            own_copy(m, k).wait()

    phase("send_up")
    for k in range(per):
        for m in (0, 1):
            send(m, k, False)
    for step in range(1, n):
        block = z - step

        @pl.when(block >= 0)
        def _():
            for p in (0, 1):
                key_copy(block, p).wait_recv()

                @pl.when(z < n - 1)
                def _():
                    key_copy(block, p).start()

    for k in range(per):
        for m in (0, 1):
            send(m, k, True)
    for k in range(per):

        @pl.when(valid(z, k))
        def _():
            for m in (0, 1, 2):
                own_copy(m, k).start()

        @pl.when(jnp.logical_not(valid(z, k)))
        def _():
            pair = pl.ds(2 * k * LANES, 2 * LANES)
            up_w[:, pair] = jnp.zeros((up_w.shape[0], 2 * LANES), up_w.dtype)
            one = pl.ds(k * LANES, LANES)
            down_w[one, :] = jnp.zeros((LANES, down_w.shape[1]), down_w.dtype)

    for block in range(1, n):

        @pl.when(block > z)
        def _():
            blank = jnp.zeros((kv_all.shape[0], rows, kv_all.shape[2]), kv_all.dtype)
            kv_all[:, pl.ds(block * rows, rows)] = blank

    phase("wait_kv")
    for k, source in enumerate(peers):
        doc_copy(k, source, source).wait_recv()
    all_docs = functools.reduce(lambda a, b: a + b, [docs_all[i] for i in range(n)])
    for seq in range(seqs):
        docs_row[seq] = jnp.broadcast_to(all_docs[seq : seq + 1], (8, total))
    gain = jnp.concatenate([head_gain[...], head_gain[...]], axis=1)

    def iota(height, width, axis):
        return lax.broadcasted_iota(jnp.int32, (height, width), axis)

    def attend(seq, carry):
        doc_row = docs_row[seq][0:1]
        at_query = iota(rows, total, 0) + z * rows
        at_key = iota(rows, total, 1)
        doc_query = jnp.sum(jnp.where(at_key == at_query, doc_row, 0.0), axis=1, keepdims=True)
        allowed = (at_key <= at_query) & (doc_row == doc_query)
        bias = jnp.where(allowed, 0.0, NEG_BIG)
        bias = jnp.concatenate([bias] * 4, axis=0)
        q_cos, q_sin = cosine[rows_at(z)], sine[rows_at(z)]
        packed = kv_all[seq]
        spun = dot(packed[:, :LANES], spread[...])
        vals = wide(packed[:, LANES:])
        swapped = pltpu.roll(vals, LANES // 2, 1)
        lane = iota(total, LANES, 1)
        queries, keys = [], []
        width = cosine.shape[1]
        for index, source in enumerate((q_one, q_two)):
            block = source[seq]
            turned = wide(block) * q_cos + dot(block, turn[...]) * q_sin
            queries.append(rounded(turned))
            start = 2 * index * width
            straight = spun[:, start : start + width]
            crossed = spun[:, start + width : start + 2 * width]
            keys.append(rounded(straight * cosine[...] + crossed * sine[...]))
        q_lane = iota(rows, LANES, 1) // (LANES // 4)
        row4 = iota(4 * rows, 1, 0) // rows
        half_lane = iota(2 * rows, LANES, 1) < LANES // 2
        for c in range(2):
            across = slice(c * LANES, (c + 1) * LANES)
            pair = (vals, swapped) if c == 0 else (swapped, vals)
            both = rounded(jnp.where(lane < LANES // 2, pair[0], pair[1]))
            found = []
            for query, key in zip(queries, keys):
                local = wide(query[:, across])
                stack = jnp.concatenate(
                    [rounded(jnp.where(q_lane == j, local, 0.0)) for j in (0, 2, 1, 3)], axis=0
                )
                scores = lax.dot_general(
                    stack, key[:, across], (((1,), (1,)), ((), ())),
                    preferred_element_type=jnp.float32,
                )
                scores = scores * scale + bias
                expd = jnp.exp(scores - jnp.max(scores, axis=1, keepdims=True))
                summed = jnp.sum(expd, axis=1, keepdims=True)
                found.append(dot(rounded(expd), both) / summed)
            weights = jnp.where(
                row4 == 0, lam[4 * c],
                jnp.where(
                    row4 == 1, lam[4 * c + 2],
                    jnp.where(row4 == 2, lam[4 * c + 1], lam[4 * c + 3]),
                ),
            )
            mixed = found[0] - weights * found[1]
            meansq = jnp.sum(mixed * mixed, axis=1, keepdims=True) * (1.0 / LANES)
            normed = mixed * lax.rsqrt(meansq + NORM_EPS) * gain
            merged = rounded(jnp.where(half_lane, normed[: 2 * rows], normed[2 * rows :]))
            base = 2 * c * LANES
            heads[seq, :, base : base + LANES] = merged[:rows]
            heads[seq, :, base + LANES : base + 2 * LANES] = merged[rows:]
        return carry

    phase("attend")
    lax.fori_loop(0, seqs, attend, 0)
    phase("relay0")
    relay(0, 0)
    relay(1, 0)

    phase("proj")
    out_copy.wait()
    halves = got_one.shape[0]
    width = features // halves

    def c1_copy(i):
        cols = pl.ds(i * width, width)
        return remote(
            part_one.at[:, 1 - low, :, cols], got_one.at[i], c1_send.at[i], c1_recv.at[i], {"tp": near}
        )

    def x1_copy(i):
        return remote(sum_one.at[i], got_far.at[i], x1_send.at[i], x1_recv.at[i], {"tp": far})

    flat = heads[...].reshape(4 * rows, heads.shape[2])
    for i in range(halves):
        cols = pl.ds(i * width, width)
        made = rounded(dot(flat, out_w[:, cols]))
        part_one[:, :, :, cols] = made.reshape(2, 2, rows, width)
        c1_copy(i).start()
    phase("wait_c1")
    for i in range(halves):
        cols = pl.ds(i * width, width)
        c1_copy(i).wait_recv()
        sum_one[i] = rounded(wide(part_one[1 - high, low, :, cols]) + wide(got_one[i, 1 - high]))
        x1_copy(i).start()
        kept = wide(part_one[high, low, :, cols]) + wide(got_one[i, high])
        mid[:, cols] = wide(resid[:, cols]) + kept
    phase("relay1")
    relay(0, 1)
    relay(1, 1)
    phase("wait_x1")
    for i in range(halves):
        cols = pl.ds(i * width, width)
        x1_copy(i).wait_recv()
        mid[:, cols] = mid[:, cols] + wide(got_far[i])
    phase("norm")
    held = mid[...]
    meansq = jnp.mean(held * held, axis=1, keepdims=True)
    rows_all[tp, rows_at(z)] = rounded(held * lax.rsqrt(meansq + NORM_EPS) * norm_gain[...])

    def x_copy(owner, block):
        part = rows_all.at[owner, rows_at(block)]
        return remote(part, part, ax_send.at[block], ax_recv.at[block], {"tp": far})

    def c_copy(owner, hop, block):
        part = rows_all.at[owner, rows_at(block)]
        return remote(part, part, ac_send.at[hop, block], ac_recv.at[hop, block], {"tp": near})

    def chain_copy(way, block):
        part = rows_all.at[tp, rows_at(block)]
        peer = lax.rem(z + (1 if way == 0 else n - 1), n)
        return remote(part, part, az_send.at[way, block], az_recv.at[block], {"sp": peer})

    def pass_on(block):
        @pl.when(z >= block)
        def _():
            @pl.when(z < n - 1)
            def _():
                chain_copy(0, block).start()

        @pl.when(z <= block)
        def _():
            @pl.when(z > 0)
            def _():
                chain_copy(1, block).start()

        x_copy(tp, block).start()
        c_copy(tp, 0, block).start()

    phase("ag_z")
    pass_on(z)
    send(2, 0)
    for k in range(2, per):
        relay(0, k)
        relay(1, k)
    for step in range(1, n):
        phase(f"ag_z{step}")
        for block in (z - step, z + step):

            @pl.when((block >= 0) & (block < n))
            def _():
                chain_copy(0, block).wait_recv()
                pass_on(block)

        if step < per:
            send(2, step)
        if step < n - 1 and step <= per - 1:
            phase(f"relay_d{step}")
            relay(2, step - 1)
    for k in range(n, per):
        send(2, k)
    phase("ag_x")
    for step in range(n):
        for block in (z - step, z + step) if step else (z,):

            @pl.when((block >= 0) & (block < n))
            def _():
                x_copy(far, block).wait_recv()
                c_copy(far, 1, block).start()

    phase("ag_c")
    for block in range(n):
        c_copy(near, 0, block).wait_recv()
        c_copy(diag, 1, block).wait_recv()
    phase("settle_up")
    for k in range(per):
        for m in (0, 1):
            settle(m, k)

    def lift(seq, carry):
        doc_row = docs_row[seq][0:1]
        at_row, at_col = iota(total, total, 0), iota(total, total, 1)
        doc_col = jnp.sum(jnp.where(at_row == at_col, doc_row, 0.0), axis=1, keepdims=True)
        same = jnp.where(doc_row == doc_col, 1.0, 0.0)
        back_one, back_two = [
            jnp.sum(jnp.where(at_col == at_row - back, same, 0.0), axis=1, keepdims=True)
            for back in (1, 2)
        ]

        def depthwise_of(current, taps):
            shown = wide(rounded(current))
            return (
                taps[2:3] * shown
                + taps[1:2] * (pltpu.roll(shown, 1, 0) * back_one)
                + taps[0:1] * (pltpu.roll(shown, 2, 0) * back_two)
            )

        for k in range(per):
            made = dot(rows_all[seq], up_w[:, 2 * k * LANES : (2 * k + 2) * LANES])
            tile = jnp.clip(tile_of(z, k), 0, tiles - 1)
            at = pl.ds(pl.multiple_of(tile * LANES, LANES), LANES)
            conv_g = depthwise_of(made[:, :LANES], taps_gate[:, at])
            conv_v = depthwise_of(made[:, LANES:], taps_value[:, at])
            unit = conv_g / (1.0 + jnp.exp(-conv_g)) * conv_v
            hidden[seq, :, k * LANES : (k + 1) * LANES] = rounded(unit)

        @pl.when(seq == seqs // 2 - 1)
        def _():
            for k in range(min(n - 2, per - 1), per):
                relay(2, k)

        return carry

    phase("lift")
    lax.fori_loop(0, rows_all.shape[0], lift, 0)
    phase("settle_d")
    for k in range(per):
        settle(2, k)

    def c2_copy(i, seq):
        return remote(part_two.at[seq], got_two.at[i], c2_send.at[i], c2_recv.at[i], {"tp": near})

    chunk = 512 if features % 512 == 0 else features
    shifts = sorted(range(n), key=lambda k: (k == 0, -min(k, n - k)))

    def x2_copy(block):
        return remote(
            sum_far.at[block], got_x.at[block], x2_send.at[block], x2_recv.at[block], {"tp": far}
        )

    def z2_copy(k, block, source):
        return remote(
            sum_z.at[k], got_z.at[source], z2_send.at[k], z2_recv.at[source], {"sp": block}
        )

    def lower(i, carry):
        seq = lax.rem(high + 1 - i // 2, 2) * 2 + lax.rem(low + 1 - lax.rem(i, 2), 2)
        for c in range(features // chunk):
            cols = slice(c * chunk, (c + 1) * chunk)
            part_two[seq, :, cols] = rounded(dot(hidden[seq], down_w[:, cols]))

        @pl.when(lax.rem(i, 2) == 0)
        def _():
            c2_copy(i // 2, seq).start()

        @pl.when(i == 2)
        def _():
            c2_copy(0, diag).wait_recv()
            for shift in shifts:
                block = lax.rem(z + shift, n)
                there = rows_at(block)
                sum_far[block] = rounded(wide(part_two[far, there]) + wide(got_two[0, there]))
                x2_copy(block).start()

        return carry

    phase("lower")
    lax.fori_loop(0, rows_all.shape[0], lower, 0)
    phase("x2")
    c2_copy(1, near).wait_recv()
    for k, shift in enumerate(shifts):
        block = lax.rem(z + shift, n)
        there = rows_at(block)
        x2_copy(block).wait_recv()
        both = wide(part_two[tp, there]) + wide(got_two[1, there]) + wide(got_x[block])
        if shift:
            sum_z[k] = rounded(both)
            z2_copy(k, block, z).start()
        else:
            own_z[...] = mid[...] + both
    phase("z2")
    answer = own_z[...]
    for k, source in enumerate(peers):
        z2_copy(k, source, source).wait_recv()
        answer = answer + wide(got_z[source])
    out[...] = answer.astype(out.dtype)

    phase("drain")
    for k, peer in enumerate(peers):
        doc_copy(k, z, peer).wait_send()
        z2_copy(k, peer, z).wait_send()
    for k in range(per):
        for m in (0, 1, 2):
            when_sent(m, k, lambda copy: copy.wait_send())
            when_got(m, k, True, lambda copy: copy.wait_send())
    for i in range(halves):
        c1_copy(i).wait_send()
        x1_copy(i).wait_send()
    for block in range(n):

        @pl.when((z >= block) & (z < n - 1))
        def _():
            chain_copy(0, block).wait_send()
            for p in (0, 1):
                key_copy(block, p).wait_send()

        @pl.when((z <= block) & (z > 0))
        def _():
            chain_copy(1, block).wait_send()

        x_copy(tp, block).wait_send()
        c_copy(tp, 0, block).wait_send()
        c_copy(far, 1, block).wait_send()
        x2_copy(block).wait_send()
    c2_copy(0, diag).wait_send()
    c2_copy(1, near).wait_send()
    phase(None)


def rope_tables(total, width, copies):
    half = width // 2
    freqs = np.float32(ROPE_BASE) ** (-np.arange(half, dtype=np.float32) * np.float32(2.0) / np.float32(width))
    angles = np.arange(total, dtype=np.float32)[:, None] * freqs.astype(np.float32)[None, :]
    tile = lambda table: np.tile(table.astype(np.float32), (1, 2 * copies))
    return tile(np.cos(angles)), tile(np.sin(angles))


def turn_matrix(width):
    half = width // 2
    at = np.arange(width)
    source = np.where(at < half, at + half, at - half)
    sign = np.where(at < half, -1.0, 1.0)
    return np.where(at[:, None] == source[None, :], sign[None, :], 0.0)


def spread_matrix(width, group, kv_local):
    straight = np.kron(np.eye(kv_local), np.tile(np.eye(width), (1, group)))
    crossed = np.kron(np.eye(kv_local), np.tile(turn_matrix(width), (1, group)))
    both = np.concatenate([straight, crossed], axis=1)
    return np.kron(np.eye(2), both)


def kernel_fits(resid_in, query_one, key_one, value, lam, gate_weight):
    heads = lam.shape[0]
    width = query_one.shape[2] // heads
    kv_local = key_one.shape[2] // width
    group = heads // kv_local
    seqs, rows = query_one.shape[:2]
    return (
        lax.axis_size("tp") == 4
        and lax.axis_size("grp") == 2
        and 2 <= lax.axis_size("sp") <= 8
        and kv_local == 2
        and group == 4
        and group * width == LANES
        and value.shape[2] == LANES
        and seqs == 4
        and resid_in.shape[0] == 1
        and rows % 16 == 0
        and rows * lax.axis_size("sp") <= 256
        and gate_weight.shape[0] <= 512
        and gate_weight.shape[1] % LANES == 0
        and gate_weight.shape[1] <= 1536
        and resid_in.shape[2] <= 2048
    )


def whole_layer(
    resid_in, query_one, key_one, query_two, key_two, value, lam, head_gain, doc_ids,
    out_weight, norm_gain, gate_weight, value_weight, conv_gate, conv_value, down_weight,
):
    n = lax.axis_size("sp")
    seqs, rows = query_one.shape[:2]
    heads = lam.shape[0]
    width = query_one.shape[2] // heads
    kv_local = key_one.shape[2] // width
    group = heads // kv_local
    features, total = resid_in.shape[2], n * rows
    depth, columns = gate_weight.shape[0], down_weight.shape[1]
    tiles = gate_weight.shape[1] // LANES
    per = -(-tiles // n)
    cosine, sine = rope_tables(total, width, heads)
    turn = np.kron(np.eye(heads), turn_matrix(width))
    spread = spread_matrix(width, group, kv_local)
    key_width = kv_local * width
    join = np.stack([np.eye(key_width, LANES), np.eye(key_width, LANES, LANES - key_width)])
    halves = 2
    bf16, f32 = jnp.bfloat16, jnp.float32
    dma = pltpu.SemaphoreType.DMA
    vmem = pltpu.VMEM
    scratch = [
        vmem((seqs, total, 2 * LANES), bf16),
        vmem((n, 8, total), f32),
        vmem((seqs, 8, total), f32),
        vmem(out_weight.shape, bf16),
        vmem((seqs, rows, out_weight.shape[0]), bf16),
        vmem((2, 2, rows, features), bf16),
        vmem((halves, 2, rows, features // halves), bf16),
        vmem((halves, rows, features // halves), bf16),
        vmem((halves, rows, features // halves), bf16),
        vmem((rows, features), f32),
        vmem((seqs, total, features), bf16),
        vmem((n * depth, 2 * per * LANES), bf16),
        vmem((per * LANES, n * columns), bf16),
        vmem((seqs, total, per * LANES), bf16),
        vmem((seqs, total, features), bf16),
        vmem((2, total, features), bf16),
        vmem((n, rows, features), bf16),
        vmem((n, rows, features), bf16),
        vmem((n, rows, features), bf16),
        vmem((rows, features), f32),
        vmem((n, rows, features), bf16),
        dma((n,)), dma((n,)), dma((n, 2)), dma((n, 2)), dma, dma((3 * per,)),
        dma((n, 3 * per)), dma((n, 3 * per)), dma((n, 3 * per)),
        dma((halves,)), dma((halves,)), dma((halves,)), dma((halves,)),
        dma((2, n)), dma((n,)), dma((n,)), dma((n,)), dma((2, n)), dma((2, n)),
        dma((2,)), dma((2,)), dma((n,)), dma((n,)), dma((n,)), dma((n,)),
    ]
    out = pl.pallas_call(
        functools.partial(layer_kernel, n, per, tiles, width ** (-0.5)),
        out_shape=jax.ShapeDtypeStruct((rows, features), resid_in.dtype),
        in_specs=[VMEM] * 7 + [SMEM] + [VMEM] * 9 + [HBM] * 4,
        out_specs=VMEM,
        scratch_shapes=scratch,
        compiler_params=pltpu.CompilerParams(
            collective_id=5, has_side_effects=True, vmem_limit_bytes=60 * 2**20
        ),
        name="whole_layer",
    )(
        resid_in.reshape(rows, features), query_one, query_two, key_one, key_two, value,
        doc_ids, lam, head_gain[None], norm_gain[None], conv_gate, conv_value,
        jnp.asarray(cosine), jnp.asarray(sine), jnp.asarray(turn, bf16), jnp.asarray(spread, bf16),
        jnp.asarray(join, bf16),
        out_weight, gate_weight, value_weight, down_weight,
    )
    return out.reshape(resid_in.shape)


def per_device_apart(
    resid_in,
    query_one,
    key_one,
    query_two,
    key_two,
    value,
    lam,
    head_gain,
    doc_ids,
    out_weight,
    norm_gain,
    gate_weight,
    value_weight,
    conv_gate,
    conv_value,
    down_weight,
):
    n_sp = lax.axis_size("sp")
    me = lax.axis_index("sp")
    depth, width = gate_weight.shape
    share = width // n_sp
    copies = lax.axis_size("grp")

    def cut(weight, row, column, size):
        return lax.dynamic_slice(weight, (row, column), size)

    def up_piece(dest, part):
        size = (depth // copies, share)
        row, column = part * size[0], dest * share
        return jnp.stack([cut(gate_weight, row, column, size), cut(value_weight, row, column, size)])

    def up_whole(dest):
        return jnp.stack([up_piece(dest, part) for part in range(copies)])

    def down_piece(dest, part):
        size = (share // copies, down_weight.shape[1])
        return cut(down_weight, dest * share + part * size[0], 0, size)

    def down_whole(dest):
        return jnp.stack([down_piece(dest, part) for part in range(copies)])

    up_all = exchange(up_piece, up_whole)
    down_all = exchange(down_piece, down_whole)
    gate_all = up_all[:, :, 0].reshape(-1, share)
    value_all = up_all[:, :, 1].reshape(-1, share)
    down_full = jnp.transpose(down_all, (1, 2, 0, 3)).reshape(share, -1)
    seqs = query_one.shape[0]
    rows = query_one.shape[1]
    heads = lam.shape[0]
    key_width = query_one.shape[2] // heads
    kv_local = key_one.shape[2] // key_width
    group = heads // kv_local
    head_width = value.shape[2] // kv_local
    scale = key_width ** (-0.5)
    positions = lax.axis_index("sp") * rows + jnp.arange(rows, dtype=jnp.int32)
    q_first = rotate(query_one, positions, heads).reshape(seqs, rows, kv_local, group, key_width)
    q_second = rotate(query_two, positions, heads).reshape(seqs, rows, kv_local, group, key_width)
    k_first = rotate(key_one, positions, kv_local).reshape(seqs, rows, kv_local * key_width)
    k_second = rotate(key_two, positions, kv_local).reshape(seqs, rows, kv_local * key_width)
    start_state = (
        jnp.full((seqs, kv_local, group, rows), NEG_BIG, jnp.float32),
        jnp.zeros((seqs, kv_local, group, rows), jnp.float32),
        jnp.zeros((seqs, kv_local, group, rows, head_width), jnp.float32),
    )
    packed = jnp.concatenate(
        [k_first, k_second, value, doc_ids.astype(jnp.bfloat16)[..., None]], axis=-1
    )
    packed = gather_sp(packed)
    key_cols = k_first.shape[2]
    keys_one = packed[..., :key_cols]
    keys_two = packed[..., key_cols : 2 * key_cols]
    vals = packed[..., 2 * key_cols : -1]
    docs = packed[..., -1].astype(jnp.int32)
    count = keys_one.shape[1]
    step_len = math.gcd(count, 512)

    def inner(state, index):
        offset = index * step_len
        ka = lax.dynamic_slice_in_dim(keys_one, offset, step_len, 1).reshape(
            seqs, step_len, kv_local, key_width
        )
        kb = lax.dynamic_slice_in_dim(keys_two, offset, step_len, 1).reshape(
            seqs, step_len, kv_local, key_width
        )
        va = lax.dynamic_slice_in_dim(vals, offset, step_len, 1).reshape(
            seqs, step_len, kv_local, head_width
        )
        dpiece = lax.dynamic_slice_in_dim(docs, offset, step_len, 1)
        key_pos = offset + jnp.arange(step_len, dtype=jnp.int32)
        allowed = (key_pos[None, None, :] <= positions[None, :, None]) & (
            dpiece[:, None, :] == doc_ids[:, :, None]
        )
        first = online_step(state[0], q_first, ka, va, allowed, scale)
        second = online_step(state[1], q_second, kb, va, allowed, scale)
        return ((first, second), None)

    def run(state):
        return lax.scan(inner, state, jnp.arange(count // step_len))[0]

    first, second = lax.cond(
        jnp.int32(0) <= positions[rows - 1], run, lambda state: state, (start_state, start_state)
    )
    weights = lam.reshape(kv_local, group)[None, :, :, None, None]
    mixed = first[2] / first[1][..., None] - weights * (second[2] / second[1][..., None])
    meansq = jnp.mean(mixed * mixed, axis=-1, keepdims=True)
    normed_heads = mixed * lax.rsqrt(meansq + NORM_EPS) * head_gain
    heads_out = jnp.transpose(normed_heads, (0, 3, 1, 2, 4)).reshape(
        seqs * rows, heads * head_width
    )
    heads_out = heads_out.astype(jnp.bfloat16)
    own = resid_in.shape[0]
    features = resid_in.shape[2]
    proj = jnp.dot(heads_out, out_weight, preferred_element_type=jnp.float32).astype(jnp.bfloat16)
    mid = reduce_rows(
        proj.reshape(-1, 1, own * rows, features),
        resid_in.astype(jnp.float32).reshape(own * rows, features),
        jnp.float32,
        False,
    )
    meansq_mid = jnp.mean(mid * mid, axis=-1, keepdims=True)
    normed = (mid * lax.rsqrt(meansq_mid + NORM_EPS) * norm_gain).astype(jnp.bfloat16)
    gathered = gather_rows(normed).reshape(-1, n_sp, own, rows, features)
    full_rows = jnp.transpose(gathered, (0, 2, 1, 3, 4)).reshape(-1, features)
    total_rows = n_sp * rows
    start = me * share
    taps_gate = lax.dynamic_slice_in_dim(conv_gate, start, share, 1)
    taps_value = lax.dynamic_slice_in_dim(conv_value, start, share, 1)
    up_gate = jnp.dot(full_rows, gate_all, preferred_element_type=jnp.float32)
    up_value = jnp.dot(full_rows, value_all, preferred_element_type=jnp.float32)
    up_gate = up_gate.astype(jnp.bfloat16).reshape(seqs, total_rows, share)
    up_value = up_value.astype(jnp.bfloat16).reshape(seqs, total_rows, share)
    conv_g = depthwise(up_gate, taps_gate, docs)
    conv_v = depthwise(up_value, taps_value, docs)
    hidden = (jax.nn.silu(conv_g) * conv_v).astype(jnp.bfloat16)
    hidden = hidden.reshape(-1, own, n_sp, rows, share)
    hidden = jnp.transpose(hidden, (0, 2, 1, 3, 4)).reshape(-1, share)
    partial_down = jnp.dot(hidden, down_full, preferred_element_type=jnp.float32)
    partial_down = partial_down.astype(jnp.bfloat16).reshape(-1, n_sp, own * rows, features)
    return reduce_rows(partial_down, mid, jnp.bfloat16, True).reshape(resid_in.shape)


def per_device(*args):
    resid_in, query_one, key_one, value, lam, gate_weight = [args[i] for i in (0, 1, 2, 5, 6, 11)]
    if kernel_fits(resid_in, query_one, key_one, value, lam, gate_weight):
        return whole_layer(*args)
    return per_device_apart(*args)


def solution(mesh):
    placed = (
        P(("grp", "tp"), "sp", None),
        P("grp", "sp", "tp"),
        P("grp", "sp", "tp"),
        P("grp", "sp", "tp"),
        P("grp", "sp", "tp"),
        P("grp", "sp", "tp"),
        P("tp"),
        P(),
        P("grp", "sp"),
        P("tp", None),
        P(),
        P("sp", "tp"),
        P("sp", "tp"),
        P(None, "tp"),
        P(None, "tp"),
        P("tp", "sp"),
    )
    return jax.shard_map(
        per_device,
        mesh=mesh,
        in_specs=placed,
        out_specs=P(("grp", "tp"), "sp", None),
        check_vma=False,
    )
```

```python
import functools
import math

import jax
import jax.numpy as jnp
import numpy as np
from jax import lax
from jax.experimental import pallas as pl
from jax.experimental.pallas import tpu as pltpu
from jax.sharding import PartitionSpec as P

NEG_BIG = -1e30
NORM_EPS = 1e-06
ROPE_BASE = 500000.0


MESH = pl.DeviceIdType.MESH
VMEM = pl.BlockSpec(memory_space=pltpu.VMEM)


def greet(devices):
    barrier = pltpu.get_barrier_semaphore()
    for device in devices:
        pl.semaphore_signal(barrier, inc=1, device_id=device, device_id_type=MESH)
    pl.semaphore_wait(barrier, len(devices))


def remote(src, dst, send_sem, recv_sem, device):
    return pltpu.make_async_remote_copy(
        src_ref=src,
        dst_ref=dst,
        send_sem=send_sem,
        recv_sem=recv_sem,
        device_id=device,
        device_id_type=MESH,
    )


def partners():
    at = lax.axis_index("tp")
    return at, at + 1 - 2 * lax.rem(at, 2), lax.rem(at + 2, 4)


def spread_kernel(n, own_ref, out_ref, send_sem, recv_sem):
    me = lax.axis_index("sp")
    peers = [lax.rem(me + shift, n) for shift in range(1, n)]
    greet([{"sp": peer} for peer in peers])
    copies = []
    for k, peer in enumerate(peers):
        copy = remote(
            own_ref, out_ref.at[:, me], send_sem.at[k], recv_sem.at[k], {"sp": peer}
        )
        copy.start()
        copies.append(copy)
    out_ref[:, me] = own_ref[...]
    for copy in copies:
        copy.wait_recv()
    for copy in copies:
        copy.wait_send()


def gather_sp(own):
    n = lax.axis_size("sp")
    if n > 8:
        return lax.all_gather(own, "sp", axis=1, tiled=True)
    outer, rows, width = own.shape
    out = pl.pallas_call(
        functools.partial(spread_kernel, n),
        out_shape=jax.ShapeDtypeStruct((outer, n, rows, width), own.dtype),
        in_specs=[VMEM],
        out_specs=VMEM,
        scratch_shapes=[pltpu.SemaphoreType.DMA((n - 1,)), pltpu.SemaphoreType.DMA((n - 1,))],
        compiler_params=pltpu.CompilerParams(collective_id=1, has_side_effects=True),
        cost_estimate=pl.CostEstimate(flops=0, bytes_accessed=30_000_000, transcendentals=0),
        name="gather_sp",
    )(own)
    return out.reshape(outer, n * rows, width)


def rows_kernel(n, own_ref, out_ref, z_send, z_recv, x_send, x_recv, c_send, c_recv):
    me = lax.axis_index("sp")
    tp, near, far = partners()
    greet([{"tp": near}, {"tp": far}] + [{"sp": lax.rem(me + k, n)} for k in range(1, n)])
    sources = [lax.rem(me - k + n, n) for k in range(n)]
    z_copies = []
    for k in range(1, n):
        copy = remote(
            own_ref,
            out_ref.at[tp, me],
            z_send.at[k - 1],
            z_recv.at[k - 1],
            {"sp": lax.rem(me + k, n)},
        )
        z_copies.append(copy)

    def along(owner, k, send, recv, device):
        block = out_ref.at[owner, sources[k]]
        return remote(block, block, send, recv, device)

    x_copies = [remote(own_ref, out_ref.at[tp, me], x_send.at[0], x_recv.at[0], {"tp": far})]
    c_copies = [remote(own_ref, out_ref.at[tp, me], c_send.at[0], c_recv.at[0], {"tp": near})]
    for k in range(1, n):
        x_copies.append(along(tp, k, x_send.at[k], x_recv.at[k], {"tp": far}))
        c_copies.append(along(tp, k, c_send.at[k], c_recv.at[k], {"tp": near}))
    f_copies = [along(far, k, c_send.at[n + k], c_recv.at[n + k], {"tp": near}) for k in range(n)]
    x_copies[0].start()
    for copy in z_copies:
        copy.start()
    c_copies[0].start()
    out_ref[tp, me] = own_ref[...]
    for k in range(1, n):
        z_copies[k - 1].wait_recv()
        x_copies[k].start()
        c_copies[k].start()
    for k in range(n):
        x_copies[k].wait_recv()
        f_copies[k].start()
    for copy in c_copies + f_copies:
        copy.wait_recv()
    for copy in z_copies + x_copies + c_copies + f_copies:
        copy.wait_send()


def gather_rows(own):
    n, wide = lax.axis_size("sp"), lax.axis_size("tp")
    if n > 8 or wide != 4:
        out = lax.all_gather(own, ("tp", "sp"), axis=0)
        return out.reshape((wide, n) + own.shape)
    dma = pltpu.SemaphoreType.DMA
    return pl.pallas_call(
        functools.partial(rows_kernel, n),
        out_shape=jax.ShapeDtypeStruct((wide, n) + own.shape, own.dtype),
        in_specs=[VMEM],
        out_specs=VMEM,
        scratch_shapes=[
            dma((n - 1,)),
            dma((n - 1,)),
            dma((n,)),
            dma((n,)),
            dma((2 * n,)),
            dma((2 * n,)),
        ],
        compiler_params=pltpu.CompilerParams(collective_id=2, has_side_effects=True),
        cost_estimate=pl.CostEstimate(flops=0, bytes_accessed=90_000_000, transcendentals=0),
        name="gather_rows",
    )(own)


def reduce_kernel(
    n, chunks, part_ref, base_ref, out_ref, got_c, sum_c, got_x, sum_x, got_z,
    c_send, c_recv, x_send, x_recv, z_send, z_recv,
):
    tp, near, far = partners()
    low, high = lax.rem(tp, 2), tp // 2
    shifts = range(1, n)
    me = lax.axis_index("sp") if n > 1 else 0
    greet([{"tp": near}, {"tp": far}] + [{"sp": lax.rem(me + k, n)} for k in shifts])
    width = part_ref.shape[-1] // chunks
    cols = [pl.ds(i * width, width) for i in range(chunks)]
    c_copies, x_copies, z_copies = [], [], []
    for i in range(chunks):
        copy = remote(
            part_ref.at[:, 1 - low, :, :, cols[i]],
            got_c.at[i],
            c_send.at[i],
            c_recv.at[i],
            {"tp": near},
        )
        copy.start()
        c_copies.append(copy)
    for i in range(chunks):
        c_copies[i].wait_recv()
        mine = part_ref[:, low, :, :, cols[i]].astype(jnp.float32)
        sum_c[i] = (mine + got_c[i].astype(jnp.float32)).astype(sum_c.dtype)
        copy = remote(
            sum_c.at[i, 1 - high], got_x.at[i], x_send.at[i], x_recv.at[i], {"tp": far}
        )
        copy.start()
        x_copies.append(copy)
    for i in range(chunks):
        x_copies[i].wait_recv()
        both = sum_c[i, high].astype(jnp.float32) + got_x[i].astype(jnp.float32)
        sum_x[i] = both.astype(sum_x.dtype)
        for k in shifts:
            peer = lax.rem(me + k, n)
            copy = remote(
                sum_x.at[i, peer],
                got_z.at[i, k - 1],
                z_send.at[i, k - 1],
                z_recv.at[i, k - 1],
                {"sp": peer},
            )
            copy.start()
            z_copies.append(copy)
    for i in range(chunks):
        total = sum_x[i, me].astype(jnp.float32)
        for k in shifts:
            z_copies[i * (n - 1) + k - 1].wait_recv()
            total = total + got_z[i, k - 1].astype(jnp.float32)
        out_ref[:, cols[i]] = (base_ref[:, cols[i]] + total).astype(out_ref.dtype)
    for copy in c_copies + x_copies + z_copies:
        copy.wait_send()


def reduce_rows(part, base, dtype, over_sp):
    wide, n = part.shape[:2]
    if n > 8 or wide != 4 or part.size > 8_000_000:
        axes = ("tp", "sp") if over_sp else "tp"
        flat = part.reshape(-1, part.shape[-1])
        total = lax.psum_scatter(flat, axes, scatter_dimension=0, tiled=True)
        return (base + total.astype(jnp.float32)).astype(dtype)
    rows, columns = part.shape[2:]
    chunks = 4 if columns % 512 == 0 else 1
    width = columns // chunks
    dma = pltpu.SemaphoreType.DMA
    zs = max(n - 1, 1)
    return pl.pallas_call(
        functools.partial(reduce_kernel, n, chunks),
        out_shape=jax.ShapeDtypeStruct((rows, columns), dtype),
        in_specs=[VMEM, VMEM],
        out_specs=VMEM,
        scratch_shapes=[
            pltpu.VMEM((chunks, 2, n, rows, width), part.dtype),
            pltpu.VMEM((chunks, 2, n, rows, width), part.dtype),
            pltpu.VMEM((chunks, n, rows, width), part.dtype),
            pltpu.VMEM((chunks, n, rows, width), part.dtype),
            pltpu.VMEM((chunks, zs, rows, width), part.dtype),
            dma((chunks,)),
            dma((chunks,)),
            dma((chunks,)),
            dma((chunks,)),
            dma((chunks, zs)),
            dma((chunks, zs)),
        ],
        compiler_params=pltpu.CompilerParams(
            collective_id=3 if over_sp else 4, has_side_effects=True
        ),
        cost_estimate=pl.CostEstimate(flops=0, bytes_accessed=60_000_000, transcendentals=0),
        name="reduce_all" if over_sp else "reduce_tp",
    )(part.reshape(2, 2, n, rows, columns), base)


def rotate(block, positions, heads):
    columns = block.shape[-1]
    width = columns // heads
    half = width // 2
    at = jnp.arange(columns, dtype=jnp.int32)
    freqs = ROPE_BASE ** (-(at % half).astype(jnp.float32) * 2.0 / width)
    angles = positions.astype(jnp.float32)[:, None] * freqs[None, :]
    source = jnp.where(at % width < half, at + half, at - half)
    sign = jnp.where(at % width < half, -1.0, 1.0)
    turn = jnp.where(at[:, None] == source[None, :], sign[None, :], 0.0).astype(jnp.bfloat16)
    flat = block.reshape(-1, columns)
    other = jnp.dot(flat, turn, preferred_element_type=jnp.float32).reshape(block.shape)
    turned = block.astype(jnp.float32) * jnp.cos(angles) + other * jnp.sin(angles)
    return turned.astype(jnp.bfloat16)


def depthwise(current, taps, docs):
    shown = current.astype(jnp.float32)
    total = taps[2] * shown
    for back in (1, 2):
        moved = jnp.pad(shown, ((0, 0), (back, 0), (0, 0)))[:, : shown.shape[1]]
        moved_docs = jnp.pad(docs, ((0, 0), (back, 0)), constant_values=-1)[:, : docs.shape[1]]
        total = total + jnp.where((moved_docs == docs)[..., None], taps[2 - back] * moved, 0.0)
    return total


def cyclic(array, axis, by):
    length = lax.axis_size(axis)
    return lax.ppermute(array, axis, [(i, (i + by) % length) for i in range(length)])


def exchange(piece, whole):
    count = lax.axis_size("sp")
    copies = lax.axis_size("grp")
    me = lax.axis_index("sp")
    mine = lax.axis_index("grp")
    if count > 8:
        pieces = jnp.stack([whole(dest) for dest in range(count)], axis=0)
        return lax.all_to_all(pieces, "sp", 0, 0)
    parts = []
    for shift in range(1, count):
        part = piece(lax.rem(me + shift, count), mine)
        parts.append(cyclic(part, "sp", shift))
    got = [jnp.stack(parts, axis=0)]
    for turn in range(1, copies):
        got.append(cyclic(got[0], "grp", turn))
    got = jnp.stack(got, axis=1)
    held = whole(me)
    held = jnp.broadcast_to(held[None], (1,) + held.shape)
    order = [lax.rem(mine - share + copies, copies) for share in range(copies)]
    out = []
    for source in range(count):
        shift = lax.rem(me - source + count, count)
        there = lax.max(shift - 1, 0)
        shares = [
            lax.dynamic_slice(got, (there, at) + (0,) * (got.ndim - 2), (1, 1) + got.shape[2:])[0]
            for at in order
        ]
        out.append(jnp.where(shift == 0, held, jnp.concatenate(shares, axis=0)[None]))
    return jnp.concatenate(out, axis=0)


def online_step(state, queries, keys, vals, allowed, scale):
    peak, total, accum = state
    scores = (
        jnp.einsum("sqhgd,skhd->shgqk", queries, keys, preferred_element_type=jnp.float32) * scale
    )
    mask = allowed[:, None, None]
    scores = jnp.where(mask, scores, NEG_BIG)
    new_peak = jnp.maximum(peak, jnp.max(scores, axis=-1))
    expd = jnp.where(mask, jnp.exp(scores - new_peak[..., None]), 0.0)
    fade = jnp.exp(peak - new_peak)
    new_total = total * fade + jnp.sum(expd, axis=-1)
    update = jnp.einsum(
        "shgqk,skhd->shgqd", expd.astype(jnp.bfloat16), vals, preferred_element_type=jnp.float32
    )
    return (new_peak, new_total, accum * fade[..., None] + update)


HBM = pl.BlockSpec(memory_space=pltpu.HBM)
SMEM = pl.BlockSpec(memory_space=pltpu.SMEM)
LANES = 128


def rounded(array):
    return array.astype(jnp.bfloat16)


def wide(array):
    return array.astype(jnp.float32)


def dot(left, right):
    return jnp.dot(left, right, preferred_element_type=jnp.float32)


class Phases:
    def __init__(self):
        self.open = None

    def __call__(self, name):
        if self.open is not None:
            self.open.__exit__(None, None, None)
        self.open = jax.named_scope(name) if name else None
        if name:
            self.open.__enter__()


def layer_kernel(
    n, per, tiles, scale,
    resid, q_one, q_two, k_one, k_two, vals_own, doc_ids, lam, head_gain, norm_gain,
    taps_gate, taps_value, cosine, sine, turn, spread, join, out_hbm, gate_hbm, value_hbm, down_hbm,
    out,
    kv_all, docs_all, docs_row, out_w, heads, part_one, got_one, sum_one, got_far, mid,
    rows_all, up_w, down_w, hidden, part_two, got_two, sum_far, got_x, sum_z, own_z, got_z,
    d_send, d_recv, k_send, k_recv, o_sem, w_send, w_recv, y_send,
    c1_send, c1_recv, x1_send, x1_recv,
    az_send, az_recv, ax_send, ax_recv, ac_send, ac_recv,
    c2_send, c2_recv, x2_send, x2_recv, z2_send, z2_recv,
):
    phase = Phases()
    z, g = lax.axis_index("sp"), lax.axis_index("grp")
    tp, near, far = partners()
    low, high = lax.rem(tp, 2), tp // 2
    diag = (1 - high) * 2 + 1 - low
    other = {"grp": 1 - g}
    spare = per * n - tiles
    seqs, rows = q_one.shape[:2]
    depth, columns = gate_hbm.shape[0], down_hbm.shape[1]
    features, total = resid.shape[1], n * rows
    peers = [lax.rem(z + k, n) for k in range(1, n)]
    phase("greet")
    greet([{"sp": peer} for peer in peers] + [{"tp": near}, {"tp": far}, other])

    def rows_at(block):
        return pl.ds(pl.multiple_of(block * rows, rows), rows)

    phase("send_kv")
    def doc_copy(k, source, peer):
        part = docs_all.at[source]
        return remote(part, part, d_send.at[k], d_recv.at[source], {"sp": peer})

    def key_copy(block, p):
        half = seqs // 2
        part = kv_all.at[p * half : (p + 1) * half, rows_at(block)]
        peer = lax.rem(z + 1, n)
        return remote(part, part, k_send.at[block, p], k_recv.at[block, p], {"sp": peer})

    for seq in range(seqs):
        paired = dot(k_one[seq], join[0]) + dot(k_two[seq], join[1])
        kv_all[seq, rows_at(z), :LANES] = rounded(paired)
        kv_all[seq, rows_at(z), LANES:] = vals_own[seq]

    @pl.when(z < n - 1)
    def _():
        for p in (0, 1):
            key_copy(z, p).start()

    slot = lax.broadcasted_iota(jnp.int32, (rows, total), 1)
    spot = lax.broadcasted_iota(jnp.int32, (rows, total), 0) + z * rows
    place = jnp.where(slot == spot, 1.0, 0.0).astype(jnp.bfloat16)
    padded = jnp.concatenate([wide(doc_ids[...]), jnp.zeros((8 - seqs, rows), jnp.float32)], axis=0)
    docs_all[z] = dot(rounded(padded), place)
    for k, peer in enumerate(peers):
        doc_copy(k, z, peer).start()

    out_copy = pltpu.make_async_copy(out_hbm, out_w, o_sem)
    out_copy.start()

    def tile_of(block, k):
        return per * block + k - low * spare

    def valid(block, k):
        tile = tile_of(block, k)
        return (tile >= 0) & (tile < tiles)

    def weight_from(m, tile):
        at = pl.ds(pl.multiple_of(jnp.clip(tile, 0, tiles - 1) * LANES, LANES), LANES)
        if m == 2:
            return down_hbm.at[at, :]
        return (gate_hbm, value_hbm)[m].at[:, at]

    def weight_to(m, source, k):
        if m == 2:
            across = pl.ds(pl.multiple_of(source * columns, columns), columns)
            return down_w.at[pl.ds(k * LANES, LANES), across]
        along = pl.ds(pl.multiple_of(source * depth, depth), depth)
        return up_w.at[along, pl.ds((2 * k + m) * LANES, LANES)]

    def over_z(m, k, source, dest):
        return lax.rem(k + m + source + dest, 2) == g

    def z_copy(m, k, peer):
        return remote(
            weight_from(m, tile_of(peer, k)), weight_to(m, z, k),
            w_send.at[peer, (3 * k + m) // 2], w_recv.at[z, 3 * k + m], {"sp": peer},
        )

    def y_copy(m, k, source):
        block = weight_to(m, source, k)
        at = 3 * k + m
        return remote(block, block, y_send.at[source, at // 2], w_recv.at[source, at], other)

    def own_copy(m, k):
        return pltpu.make_async_copy(
            weight_from(m, tile_of(z, k)), weight_to(m, z, k), w_recv.at[z, 3 * k + m]
        )

    def at_distance(d):
        return ((lax.rem(z - d + n, n), z - d >= 0), (lax.rem(z + d, n), z + d < n))

    def when_sent(d, items, act, ways=(0, 1)):
        for way in ways:
            peer, there = at_distance(d)[way]
            for k, m in items:

                @pl.when(there & valid(peer, k) & over_z(m, k, z, peer))
                def _():
                    act(z_copy(m, k, peer))

    def when_hopped(d, items, act):
        for k, m in items:
            for source, there in at_distance(d):

                @pl.when(there & valid(z, k) & over_z(m, k, source, z))
                def _():
                    act(y_copy(m, k, source))

    def send(d, items, ways=(0, 1)):
        when_sent(d, items, lambda copy: copy.start(), ways)

    def relay(d, items):
        def act(copy):
            copy.wait_recv()
            copy.start()

        when_hopped(d, items, act)

    ups = [(k, m) for k in range(per) for m in (0, 1)]
    downs = [(k, 2) for k in range(per)]
    early, middle, late = ups[: 2 * per - 2], ups[2 * per - 2 : 2 * per - 1], ups[2 * per - 1 :]

    def settle(m, k):
        for source in peers:

            @pl.when(valid(z, k) & jnp.logical_not(over_z(m, k, source, z)))
            def _():
                y_copy(m, k, source).wait_recv()

        @pl.when(valid(z, k))
        def _():
            own_copy(m, k).wait()

    phase("send_up")
    for d in range(1, n):
        send(d, early + middle, (0,))
    for step in range(1, n):
        block = z - step

        @pl.when(block >= 0)
        def _():
            for p in (0, 1):
                key_copy(block, p).wait_recv()

                @pl.when(z < n - 1)
                def _():
                    key_copy(block, p).start()

    for d in range(1, n):
        send(d, early, (1,))
    for k in range(per):

        @pl.when(valid(z, k))
        def _():
            for m in (0, 1, 2):
                own_copy(m, k).start()

        @pl.when(jnp.logical_not(valid(z, k)))
        def _():
            pair = pl.ds(2 * k * LANES, 2 * LANES)
            up_w[:, pair] = jnp.zeros((up_w.shape[0], 2 * LANES), up_w.dtype)
            one = pl.ds(k * LANES, LANES)
            down_w[one, :] = jnp.zeros((LANES, down_w.shape[1]), down_w.dtype)

    for block in range(1, n):

        @pl.when(block > z)
        def _():
            blank = jnp.zeros((kv_all.shape[0], rows, kv_all.shape[2]), kv_all.dtype)
            kv_all[:, pl.ds(block * rows, rows)] = blank

    phase("wait_kv")
    for k, source in enumerate(peers):
        doc_copy(k, source, source).wait_recv()
    all_docs = functools.reduce(lambda a, b: a + b, [docs_all[i] for i in range(n)])
    for seq in range(seqs):
        docs_row[seq] = jnp.broadcast_to(all_docs[seq : seq + 1], (8, total))
    gain = jnp.concatenate([head_gain[...], head_gain[...]], axis=1)

    def iota(height, width, axis):
        return lax.broadcasted_iota(jnp.int32, (height, width), axis)

    def attend(seq, carry):
        doc_row = docs_row[seq][0:1]
        at_query = iota(rows, total, 0) + z * rows
        at_key = iota(rows, total, 1)
        doc_query = jnp.sum(jnp.where(at_key == at_query, doc_row, 0.0), axis=1, keepdims=True)
        allowed = (at_key <= at_query) & (doc_row == doc_query)
        bias = jnp.where(allowed, 0.0, NEG_BIG)
        bias = jnp.concatenate([bias] * 4, axis=0)
        q_cos, q_sin = cosine[rows_at(z)], sine[rows_at(z)]
        packed = kv_all[seq]
        spun = dot(packed[:, :LANES], spread[...])
        vals = wide(packed[:, LANES:])
        swapped = pltpu.roll(vals, LANES // 2, 1)
        lane = iota(total, LANES, 1)
        queries, keys = [], []
        width = cosine.shape[1]
        for index, source in enumerate((q_one, q_two)):
            block = source[seq]
            turned = wide(block) * q_cos + dot(block, turn[...]) * q_sin
            queries.append(rounded(turned))
            start = 2 * index * width
            straight = spun[:, start : start + width]
            crossed = spun[:, start + width : start + 2 * width]
            keys.append(rounded(straight * cosine[...] + crossed * sine[...]))
        q_lane = iota(rows, LANES, 1) // (LANES // 4)
        row4 = iota(4 * rows, 1, 0) // rows
        half_lane = iota(2 * rows, LANES, 1) < LANES // 2
        for c in range(2):
            across = slice(c * LANES, (c + 1) * LANES)
            pair = (vals, swapped) if c == 0 else (swapped, vals)
            both = rounded(jnp.where(lane < LANES // 2, pair[0], pair[1]))
            found = []
            for query, key in zip(queries, keys):
                local = wide(query[:, across])
                stack = jnp.concatenate(
                    [rounded(jnp.where(q_lane == j, local, 0.0)) for j in (0, 2, 1, 3)], axis=0
                )
                scores = lax.dot_general(
                    stack, key[:, across], (((1,), (1,)), ((), ())),
                    preferred_element_type=jnp.float32,
                )
                scores = scores * scale + bias
                expd = jnp.exp(scores - jnp.max(scores, axis=1, keepdims=True))
                summed = jnp.sum(expd, axis=1, keepdims=True)
                found.append(dot(rounded(expd), both) / summed)
            weights = jnp.where(
                row4 == 0, lam[4 * c],
                jnp.where(
                    row4 == 1, lam[4 * c + 2],
                    jnp.where(row4 == 2, lam[4 * c + 1], lam[4 * c + 3]),
                ),
            )
            mixed = found[0] - weights * found[1]
            meansq = jnp.sum(mixed * mixed, axis=1, keepdims=True) * (1.0 / LANES)
            normed = mixed * lax.rsqrt(meansq + NORM_EPS) * gain
            merged = rounded(jnp.where(half_lane, normed[: 2 * rows], normed[2 * rows :]))
            base = 2 * c * LANES
            heads[seq, :, base : base + LANES] = merged[:rows]
            heads[seq, :, base + LANES : base + 2 * LANES] = merged[rows:]
        return carry

    phase("attend")
    lax.fori_loop(0, seqs, attend, 0)

    phase("proj")
    out_copy.wait()
    halves = got_one.shape[0]
    width = features // halves

    def c1_copy(i):
        cols = pl.ds(i * width, width)
        return remote(
            part_one.at[:, 1 - low, :, cols], got_one.at[i], c1_send.at[i], c1_recv.at[i], {"tp": near}
        )

    def x1_copy(i):
        return remote(sum_one.at[i], got_far.at[i], x1_send.at[i], x1_recv.at[i], {"tp": far})

    flat = heads[...].reshape(4 * rows, heads.shape[2])
    for i in range(halves):
        cols = pl.ds(i * width, width)
        made = rounded(dot(flat, out_w[:, cols]))
        part_one[:, :, :, cols] = made.reshape(2, 2, rows, width)
        c1_copy(i).start()
    phase("wait_c1")
    for i in range(halves):
        cols = pl.ds(i * width, width)
        c1_copy(i).wait_recv()
        sum_one[i] = rounded(wide(part_one[1 - high, low, :, cols]) + wide(got_one[i, 1 - high]))
        x1_copy(i).start()
        kept = wide(part_one[high, low, :, cols]) + wide(got_one[i, high])
        mid[:, cols] = wide(resid[:, cols]) + kept
    phase("relay_u1")
    relay(1, early)
    phase("wait_x1")
    for i in range(halves):
        cols = pl.ds(i * width, width)
        x1_copy(i).wait_recv()
        mid[:, cols] = mid[:, cols] + wide(got_far[i])
    phase("norm")
    held = mid[...]
    meansq = jnp.mean(held * held, axis=1, keepdims=True)
    rows_all[tp, rows_at(z)] = rounded(held * lax.rsqrt(meansq + NORM_EPS) * norm_gain[...])

    cuts = 2
    part_rows = rows // cuts

    def piece_of(owner, block, p):
        first = pl.multiple_of(block * rows + p * part_rows, part_rows)
        return rows_all.at[owner, pl.ds(first, part_rows)]

    def x_copy(owner, block, p):
        part = piece_of(owner, block, p)
        return remote(part, part, ax_send.at[block, p], ax_recv.at[block, p], {"tp": far})

    def c_copy(owner, hop, block, p):
        part = piece_of(owner, block, p)
        sems = (ac_send.at[hop, block, p], ac_recv.at[hop, block, p])
        return remote(part, part, *sems, {"tp": near})

    def chain_copy(way, block, p):
        part = piece_of(tp, block, p)
        peer = lax.rem(z + (1 if way == 0 else n - 1), n)
        return remote(part, part, az_send.at[way, block, p], az_recv.at[block, p], {"sp": peer})

    def pass_on(block, p):
        @pl.when((z >= block) & (z < n - 1))
        def _():
            chain_copy(0, block, p).start()

        @pl.when((z <= block) & (z > 0))
        def _():
            chain_copy(1, block, p).start()

        x_copy(tp, block, p).start()
        c_copy(tp, 0, block, p).start()

    def chain(step):
        for p in range(cuts):
            for block in (z - step, z + step):

                @pl.when((block >= 0) & (block < n))
                def _():
                    chain_copy(0, block, p).wait_recv()
                    pass_on(block, p)

    phase("ag_start")
    for p in range(cuts):
        pass_on(z, p)

    phase("relay_u2")
    for d in range(2, n):
        relay(d, early)
    for step in range(1, n):
        phase(f"ag_z{step}")
        chain(step)
        if step == 1:
            for d in range(1, n):
                send(d, middle, (1,))
                send(d, late)
            for d in range(1, n):
                send(d, downs)
    phase("relay_u3")
    for d in range(1, n):
        relay(d, middle + late)
    phase("relay_d3")
    relay(1, downs)
    phase("settle_up")
    for k, m in ups:
        settle(m, k)

    def cross():
        for step in range(n):
            for p in range(cuts):
                for block in (z - step, z + step) if step else (z,):

                    @pl.when((block >= 0) & (block < n))
                    def _():
                        x_copy(far, block, p).wait_recv()
                        c_copy(far, 1, block, p).start()

    def lift(i, carry):
        seq = lax.rem(high + i // 2, 2) * 2 + lax.rem(low + i, 2)
        for turn_at, (owner, hop) in ((1, (near, 0)), (3, (diag, 1))):

            @pl.when(i == turn_at)
            def _():
                for block in range(n):
                    for p in range(cuts):
                        c_copy(owner, hop, block, p).wait_recv()

        @pl.when(i == 2)
        def _():
            cross()
            for d in range(2, n):
                relay(d, downs)

        doc_row = docs_row[seq][0:1]
        at_row, at_col = iota(total, total, 0), iota(total, total, 1)
        doc_col = jnp.sum(jnp.where(at_row == at_col, doc_row, 0.0), axis=1, keepdims=True)
        same = jnp.where(doc_row == doc_col, 1.0, 0.0)
        back_one, back_two = [
            jnp.sum(jnp.where(at_col == at_row - back, same, 0.0), axis=1, keepdims=True)
            for back in (1, 2)
        ]

        def depthwise_of(current, taps):
            shown = wide(rounded(current))
            return (
                taps[2:3] * shown
                + taps[1:2] * (pltpu.roll(shown, 1, 0) * back_one)
                + taps[0:1] * (pltpu.roll(shown, 2, 0) * back_two)
            )

        for k in range(per):
            made = dot(rows_all[seq], up_w[:, 2 * k * LANES : (2 * k + 2) * LANES])
            tile = jnp.clip(tile_of(z, k), 0, tiles - 1)
            at = pl.ds(pl.multiple_of(tile * LANES, LANES), LANES)
            conv_g = depthwise_of(made[:, :LANES], taps_gate[:, at])
            conv_v = depthwise_of(made[:, LANES:], taps_value[:, at])
            unit = conv_g / (1.0 + jnp.exp(-conv_g)) * conv_v
            hidden[seq, :, k * LANES : (k + 1) * LANES] = rounded(unit)
        return carry

    phase("lift")
    lax.fori_loop(0, rows_all.shape[0], lift, 0)
    phase("settle_d")
    for k in range(per):
        settle(2, k)

    def c2_copy(i, seq, block):
        there = rows_at(block)
        sems = (c2_send.at[i, block], c2_recv.at[i, block])
        return remote(part_two.at[seq, there], got_two.at[i, there], *sems, {"tp": near})

    chunk = 512 if features % 512 == 0 else features
    shifts = sorted(range(n), key=lambda k: (k == 0, -min(k, n - k)))

    def slot(p):
        return pl.ds(p * part_rows, part_rows)

    def piece_rows(block, p):
        return pl.ds(pl.multiple_of(block * rows + p * part_rows, part_rows), part_rows)

    def x2_copy(block, p):
        sems = (x2_send.at[block, p], x2_recv.at[block, p])
        return remote(sum_far.at[block, slot(p)], got_x.at[block, slot(p)], *sems, {"tp": far})

    def z2_copy(k, block, source, p):
        sems = (z2_send.at[k, p], z2_recv.at[source, p])
        return remote(sum_z.at[k, slot(p)], got_z.at[source, slot(p)], *sems, {"sp": block})

    def lower(i, carry):
        seq = lax.rem(high + 1 - i // 2, 2) * 2 + lax.rem(low + 1 - lax.rem(i, 2), 2)
        for c in range(features // chunk):
            cols = slice(c * chunk, (c + 1) * chunk)
            part_two[seq, :, cols] = rounded(dot(hidden[seq], down_w[:, cols]))

        @pl.when(lax.rem(i, 2) == 0)
        def _():
            for shift in shifts:
                c2_copy(i // 2, seq, lax.rem(z + shift, n)).start()

        @pl.when(i == 1)
        def _():
            for shift in shifts:
                block = lax.rem(z + shift, n)
                c2_copy(0, diag, block).wait_recv()
                for p in range(cuts):
                    there = piece_rows(block, p)
                    both = wide(part_two[far, there]) + wide(got_two[0, there])
                    sum_far[block, slot(p)] = rounded(both)
                    x2_copy(block, p).start()

        return carry

    phase("lower")
    lax.fori_loop(0, rows_all.shape[0], lower, 0)
    phase("x2")
    for k, shift in enumerate(shifts):
        block = lax.rem(z + shift, n)
        c2_copy(1, near, block).wait_recv()
        for p in range(cuts):
            there = piece_rows(block, p)
            x2_copy(block, p).wait_recv()
            both = wide(part_two[tp, there]) + wide(got_two[1, there]) + wide(got_x[block, slot(p)])
            if shift:
                sum_z[k, slot(p)] = rounded(both)
                z2_copy(k, block, z, p).start()
            else:
                own_z[slot(p)] = mid[slot(p)] + both
    phase("z2")
    for p in range(cuts):
        answer = own_z[slot(p)]
        for shift in shifts[:-1]:
            source = lax.rem(z - shift + n, n)
            z2_copy(0, source, source, p).wait_recv()
            answer = answer + wide(got_z[source, slot(p)])
        out[slot(p)] = answer.astype(out.dtype)

    phase("drain")
    for k, peer in enumerate(peers):
        doc_copy(k, z, peer).wait_send()
        for p in range(cuts):
            z2_copy(k, peer, z, p).wait_send()
    for d in range(1, n):
        when_sent(d, ups + downs, lambda copy: copy.wait_send())
        when_hopped(d, ups + downs, lambda copy: copy.wait_send())
    for i in range(halves):
        c1_copy(i).wait_send()
        x1_copy(i).wait_send()
    for block in range(n):

        @pl.when((z >= block) & (z < n - 1))
        def _():
            for p in range(cuts):
                chain_copy(0, block, p).wait_send()
            for p in (0, 1):
                key_copy(block, p).wait_send()

        @pl.when((z <= block) & (z > 0))
        def _():
            for p in range(cuts):
                chain_copy(1, block, p).wait_send()

        for p in range(cuts):
            x_copy(tp, block, p).wait_send()
            x2_copy(block, p).wait_send()
            c_copy(tp, 0, block, p).wait_send()
            c_copy(far, 1, block, p).wait_send()
        c2_copy(0, diag, block).wait_send()
        c2_copy(1, near, block).wait_send()
    phase(None)


def rope_tables(total, width, copies):
    half = width // 2
    freqs = np.float32(ROPE_BASE) ** (-np.arange(half, dtype=np.float32) * np.float32(2.0) / np.float32(width))
    angles = np.arange(total, dtype=np.float32)[:, None] * freqs.astype(np.float32)[None, :]
    tile = lambda table: np.tile(table.astype(np.float32), (1, 2 * copies))
    return tile(np.cos(angles)), tile(np.sin(angles))


def turn_matrix(width):
    half = width // 2
    at = np.arange(width)
    source = np.where(at < half, at + half, at - half)
    sign = np.where(at < half, -1.0, 1.0)
    return np.where(at[:, None] == source[None, :], sign[None, :], 0.0)


def spread_matrix(width, group, kv_local):
    straight = np.kron(np.eye(kv_local), np.tile(np.eye(width), (1, group)))
    crossed = np.kron(np.eye(kv_local), np.tile(turn_matrix(width), (1, group)))
    both = np.concatenate([straight, crossed], axis=1)
    return np.kron(np.eye(2), both)


def kernel_fits(resid_in, query_one, key_one, value, lam, gate_weight):
    heads = lam.shape[0]
    width = query_one.shape[2] // heads
    kv_local = key_one.shape[2] // width
    group = heads // kv_local
    seqs, rows = query_one.shape[:2]
    return (
        lax.axis_size("tp") == 4
        and lax.axis_size("grp") == 2
        and 2 <= lax.axis_size("sp") <= 8
        and kv_local == 2
        and group == 4
        and group * width == LANES
        and value.shape[2] == LANES
        and seqs == 4
        and resid_in.shape[0] == 1
        and rows % 16 == 0
        and rows * lax.axis_size("sp") <= 256
        and gate_weight.shape[0] <= 512
        and gate_weight.shape[1] % LANES == 0
        and gate_weight.shape[1] <= 1536
        and resid_in.shape[2] <= 2048
    )


def whole_layer(
    resid_in, query_one, key_one, query_two, key_two, value, lam, head_gain, doc_ids,
    out_weight, norm_gain, gate_weight, value_weight, conv_gate, conv_value, down_weight,
):
    n = lax.axis_size("sp")
    seqs, rows = query_one.shape[:2]
    heads = lam.shape[0]
    width = query_one.shape[2] // heads
    kv_local = key_one.shape[2] // width
    group = heads // kv_local
    features, total = resid_in.shape[2], n * rows
    depth, columns = gate_weight.shape[0], down_weight.shape[1]
    tiles = gate_weight.shape[1] // LANES
    per = -(-tiles // n)
    cosine, sine = rope_tables(total, width, heads)
    turn = np.kron(np.eye(heads), turn_matrix(width))
    spread = spread_matrix(width, group, kv_local)
    key_width = kv_local * width
    join = np.stack([np.eye(key_width, LANES), np.eye(key_width, LANES, LANES - key_width)])
    halves = 2
    bf16, f32 = jnp.bfloat16, jnp.float32
    dma = pltpu.SemaphoreType.DMA
    vmem = pltpu.VMEM
    scratch = [
        vmem((seqs, total, 2 * LANES), bf16),
        vmem((n, 8, total), f32),
        vmem((seqs, 8, total), f32),
        vmem(out_weight.shape, bf16),
        vmem((seqs, rows, out_weight.shape[0]), bf16),
        vmem((2, 2, rows, features), bf16),
        vmem((halves, 2, rows, features // halves), bf16),
        vmem((halves, rows, features // halves), bf16),
        vmem((halves, rows, features // halves), bf16),
        vmem((rows, features), f32),
        vmem((seqs, total, features), bf16),
        vmem((n * depth, 2 * per * LANES), bf16),
        vmem((per * LANES, n * columns), bf16),
        vmem((seqs, total, per * LANES), bf16),
        vmem((seqs, total, features), bf16),
        vmem((2, total, features), bf16),
        vmem((n, rows, features), bf16),
        vmem((n, rows, features), bf16),
        vmem((n, rows, features), bf16),
        vmem((rows, features), f32),
        vmem((n, rows, features), bf16),
        dma((n,)), dma((n,)), dma((n, 2)), dma((n, 2)), dma,
        dma((n, 3 * per // 2 + 1)), dma((n, 3 * per)), dma((n, 3 * per // 2 + 1)),
        dma((halves,)), dma((halves,)), dma((halves,)), dma((halves,)),
        dma((2, n, 2)), dma((n, 2)), dma((n, 2)), dma((n, 2)), dma((2, n, 2)), dma((2, n, 2)),
        dma((2, n)), dma((2, n)), dma((n, 2)), dma((n, 2)), dma((n, 2)), dma((n, 2)),
    ]
    out = pl.pallas_call(
        functools.partial(layer_kernel, n, per, tiles, width ** (-0.5)),
        out_shape=jax.ShapeDtypeStruct((rows, features), resid_in.dtype),
        in_specs=[VMEM] * 7 + [SMEM] + [VMEM] * 9 + [HBM] * 4,
        out_specs=VMEM,
        scratch_shapes=scratch,
        compiler_params=pltpu.CompilerParams(
            collective_id=5, has_side_effects=True, vmem_limit_bytes=60 * 2**20
        ),
        name="whole_layer",
    )(
        resid_in.reshape(rows, features), query_one, query_two, key_one, key_two, value,
        doc_ids, lam, head_gain[None], norm_gain[None], conv_gate, conv_value,
        jnp.asarray(cosine), jnp.asarray(sine), jnp.asarray(turn, bf16), jnp.asarray(spread, bf16),
        jnp.asarray(join, bf16),
        out_weight, gate_weight, value_weight, down_weight,
    )
    return out.reshape(resid_in.shape)


def per_device_apart(
    resid_in,
    query_one,
    key_one,
    query_two,
    key_two,
    value,
    lam,
    head_gain,
    doc_ids,
    out_weight,
    norm_gain,
    gate_weight,
    value_weight,
    conv_gate,
    conv_value,
    down_weight,
):
    n_sp = lax.axis_size("sp")
    me = lax.axis_index("sp")
    depth, width = gate_weight.shape
    share = width // n_sp
    copies = lax.axis_size("grp")

    def cut(weight, row, column, size):
        return lax.dynamic_slice(weight, (row, column), size)

    def up_piece(dest, part):
        size = (depth // copies, share)
        row, column = part * size[0], dest * share
        return jnp.stack([cut(gate_weight, row, column, size), cut(value_weight, row, column, size)])

    def up_whole(dest):
        return jnp.stack([up_piece(dest, part) for part in range(copies)])

    def down_piece(dest, part):
        size = (share // copies, down_weight.shape[1])
        return cut(down_weight, dest * share + part * size[0], 0, size)

    def down_whole(dest):
        return jnp.stack([down_piece(dest, part) for part in range(copies)])

    up_all = exchange(up_piece, up_whole)
    down_all = exchange(down_piece, down_whole)
    gate_all = up_all[:, :, 0].reshape(-1, share)
    value_all = up_all[:, :, 1].reshape(-1, share)
    down_full = jnp.transpose(down_all, (1, 2, 0, 3)).reshape(share, -1)
    seqs = query_one.shape[0]
    rows = query_one.shape[1]
    heads = lam.shape[0]
    key_width = query_one.shape[2] // heads
    kv_local = key_one.shape[2] // key_width
    group = heads // kv_local
    head_width = value.shape[2] // kv_local
    scale = key_width ** (-0.5)
    positions = lax.axis_index("sp") * rows + jnp.arange(rows, dtype=jnp.int32)
    q_first = rotate(query_one, positions, heads).reshape(seqs, rows, kv_local, group, key_width)
    q_second = rotate(query_two, positions, heads).reshape(seqs, rows, kv_local, group, key_width)
    k_first = rotate(key_one, positions, kv_local).reshape(seqs, rows, kv_local * key_width)
    k_second = rotate(key_two, positions, kv_local).reshape(seqs, rows, kv_local * key_width)
    start_state = (
        jnp.full((seqs, kv_local, group, rows), NEG_BIG, jnp.float32),
        jnp.zeros((seqs, kv_local, group, rows), jnp.float32),
        jnp.zeros((seqs, kv_local, group, rows, head_width), jnp.float32),
    )
    packed = jnp.concatenate(
        [k_first, k_second, value, doc_ids.astype(jnp.bfloat16)[..., None]], axis=-1
    )
    packed = gather_sp(packed)
    key_cols = k_first.shape[2]
    keys_one = packed[..., :key_cols]
    keys_two = packed[..., key_cols : 2 * key_cols]
    vals = packed[..., 2 * key_cols : -1]
    docs = packed[..., -1].astype(jnp.int32)
    count = keys_one.shape[1]
    step_len = math.gcd(count, 512)

    def inner(state, index):
        offset = index * step_len
        ka = lax.dynamic_slice_in_dim(keys_one, offset, step_len, 1).reshape(
            seqs, step_len, kv_local, key_width
        )
        kb = lax.dynamic_slice_in_dim(keys_two, offset, step_len, 1).reshape(
            seqs, step_len, kv_local, key_width
        )
        va = lax.dynamic_slice_in_dim(vals, offset, step_len, 1).reshape(
            seqs, step_len, kv_local, head_width
        )
        dpiece = lax.dynamic_slice_in_dim(docs, offset, step_len, 1)
        key_pos = offset + jnp.arange(step_len, dtype=jnp.int32)
        allowed = (key_pos[None, None, :] <= positions[None, :, None]) & (
            dpiece[:, None, :] == doc_ids[:, :, None]
        )
        first = online_step(state[0], q_first, ka, va, allowed, scale)
        second = online_step(state[1], q_second, kb, va, allowed, scale)
        return ((first, second), None)

    def run(state):
        return lax.scan(inner, state, jnp.arange(count // step_len))[0]

    first, second = lax.cond(
        jnp.int32(0) <= positions[rows - 1], run, lambda state: state, (start_state, start_state)
    )
    weights = lam.reshape(kv_local, group)[None, :, :, None, None]
    mixed = first[2] / first[1][..., None] - weights * (second[2] / second[1][..., None])
    meansq = jnp.mean(mixed * mixed, axis=-1, keepdims=True)
    normed_heads = mixed * lax.rsqrt(meansq + NORM_EPS) * head_gain
    heads_out = jnp.transpose(normed_heads, (0, 3, 1, 2, 4)).reshape(
        seqs * rows, heads * head_width
    )
    heads_out = heads_out.astype(jnp.bfloat16)
    own = resid_in.shape[0]
    features = resid_in.shape[2]
    proj = jnp.dot(heads_out, out_weight, preferred_element_type=jnp.float32).astype(jnp.bfloat16)
    mid = reduce_rows(
        proj.reshape(-1, 1, own * rows, features),
        resid_in.astype(jnp.float32).reshape(own * rows, features),
        jnp.float32,
        False,
    )
    meansq_mid = jnp.mean(mid * mid, axis=-1, keepdims=True)
    normed = (mid * lax.rsqrt(meansq_mid + NORM_EPS) * norm_gain).astype(jnp.bfloat16)
    gathered = gather_rows(normed).reshape(-1, n_sp, own, rows, features)
    full_rows = jnp.transpose(gathered, (0, 2, 1, 3, 4)).reshape(-1, features)
    total_rows = n_sp * rows
    start = me * share
    taps_gate = lax.dynamic_slice_in_dim(conv_gate, start, share, 1)
    taps_value = lax.dynamic_slice_in_dim(conv_value, start, share, 1)
    up_gate = jnp.dot(full_rows, gate_all, preferred_element_type=jnp.float32)
    up_value = jnp.dot(full_rows, value_all, preferred_element_type=jnp.float32)
    up_gate = up_gate.astype(jnp.bfloat16).reshape(seqs, total_rows, share)
    up_value = up_value.astype(jnp.bfloat16).reshape(seqs, total_rows, share)
    conv_g = depthwise(up_gate, taps_gate, docs)
    conv_v = depthwise(up_value, taps_value, docs)
    hidden = (jax.nn.silu(conv_g) * conv_v).astype(jnp.bfloat16)
    hidden = hidden.reshape(-1, own, n_sp, rows, share)
    hidden = jnp.transpose(hidden, (0, 2, 1, 3, 4)).reshape(-1, share)
    partial_down = jnp.dot(hidden, down_full, preferred_element_type=jnp.float32)
    partial_down = partial_down.astype(jnp.bfloat16).reshape(-1, n_sp, own * rows, features)
    return reduce_rows(partial_down, mid, jnp.bfloat16, True).reshape(resid_in.shape)


def per_device(*args):
    resid_in, query_one, key_one, value, lam, gate_weight = [args[i] for i in (0, 1, 2, 5, 6, 11)]
    if kernel_fits(resid_in, query_one, key_one, value, lam, gate_weight):
        return whole_layer(*args)
    return per_device_apart(*args)


def solution(mesh):
    placed = (
        P(("grp", "tp"), "sp", None),
        P("grp", "sp", "tp"),
        P("grp", "sp", "tp"),
        P("grp", "sp", "tp"),
        P("grp", "sp", "tp"),
        P("grp", "sp", "tp"),
        P("tp"),
        P(),
        P("grp", "sp"),
        P("tp", None),
        P(),
        P("sp", "tp"),
        P("sp", "tp"),
        P(None, "tp"),
        P(None, "tp"),
        P("tp", "sp"),
    )
    return jax.shard_map(
        per_device,
        mesh=mesh,
        in_specs=placed,
        out_specs=P(("grp", "tp"), "sp", None),
        check_vma=False,
    )
```

```python
import functools
import math

import jax
import jax.numpy as jnp
import numpy as np
from jax import lax
from jax.experimental import pallas as pl
from jax.experimental.pallas import tpu as pltpu
from jax.sharding import PartitionSpec as P

NEG_BIG = -1e30
NORM_EPS = 1e-06
ROPE_BASE = 500000.0


MESH = pl.DeviceIdType.MESH
VMEM = pl.BlockSpec(memory_space=pltpu.VMEM)


def greet(devices):
    barrier = pltpu.get_barrier_semaphore()
    for device in devices:
        pl.semaphore_signal(barrier, inc=1, device_id=device, device_id_type=MESH)
    pl.semaphore_wait(barrier, len(devices))


def remote(src, dst, send_sem, recv_sem, device):
    return pltpu.make_async_remote_copy(
        src_ref=src,
        dst_ref=dst,
        send_sem=send_sem,
        recv_sem=recv_sem,
        device_id=device,
        device_id_type=MESH,
    )


def partners():
    at = lax.axis_index("tp")
    return at, at + 1 - 2 * lax.rem(at, 2), lax.rem(at + 2, 4)


def spread_kernel(n, own_ref, out_ref, send_sem, recv_sem):
    me = lax.axis_index("sp")
    peers = [lax.rem(me + shift, n) for shift in range(1, n)]
    greet([{"sp": peer} for peer in peers])
    copies = []
    for k, peer in enumerate(peers):
        copy = remote(
            own_ref, out_ref.at[:, me], send_sem.at[k], recv_sem.at[k], {"sp": peer}
        )
        copy.start()
        copies.append(copy)
    out_ref[:, me] = own_ref[...]
    for copy in copies:
        copy.wait_recv()
    for copy in copies:
        copy.wait_send()


def gather_sp(own):
    n = lax.axis_size("sp")
    if n > 8:
        return lax.all_gather(own, "sp", axis=1, tiled=True)
    outer, rows, width = own.shape
    out = pl.pallas_call(
        functools.partial(spread_kernel, n),
        out_shape=jax.ShapeDtypeStruct((outer, n, rows, width), own.dtype),
        in_specs=[VMEM],
        out_specs=VMEM,
        scratch_shapes=[pltpu.SemaphoreType.DMA((n - 1,)), pltpu.SemaphoreType.DMA((n - 1,))],
        compiler_params=pltpu.CompilerParams(collective_id=1, has_side_effects=True),
        cost_estimate=pl.CostEstimate(flops=0, bytes_accessed=30_000_000, transcendentals=0),
        name="gather_sp",
    )(own)
    return out.reshape(outer, n * rows, width)


def rows_kernel(n, own_ref, out_ref, z_send, z_recv, x_send, x_recv, c_send, c_recv):
    me = lax.axis_index("sp")
    tp, near, far = partners()
    greet([{"tp": near}, {"tp": far}] + [{"sp": lax.rem(me + k, n)} for k in range(1, n)])
    sources = [lax.rem(me - k + n, n) for k in range(n)]
    z_copies = []
    for k in range(1, n):
        copy = remote(
            own_ref,
            out_ref.at[tp, me],
            z_send.at[k - 1],
            z_recv.at[k - 1],
            {"sp": lax.rem(me + k, n)},
        )
        z_copies.append(copy)

    def along(owner, k, send, recv, device):
        block = out_ref.at[owner, sources[k]]
        return remote(block, block, send, recv, device)

    x_copies = [remote(own_ref, out_ref.at[tp, me], x_send.at[0], x_recv.at[0], {"tp": far})]
    c_copies = [remote(own_ref, out_ref.at[tp, me], c_send.at[0], c_recv.at[0], {"tp": near})]
    for k in range(1, n):
        x_copies.append(along(tp, k, x_send.at[k], x_recv.at[k], {"tp": far}))
        c_copies.append(along(tp, k, c_send.at[k], c_recv.at[k], {"tp": near}))
    f_copies = [along(far, k, c_send.at[n + k], c_recv.at[n + k], {"tp": near}) for k in range(n)]
    x_copies[0].start()
    for copy in z_copies:
        copy.start()
    c_copies[0].start()
    out_ref[tp, me] = own_ref[...]
    for k in range(1, n):
        z_copies[k - 1].wait_recv()
        x_copies[k].start()
        c_copies[k].start()
    for k in range(n):
        x_copies[k].wait_recv()
        f_copies[k].start()
    for copy in c_copies + f_copies:
        copy.wait_recv()
    for copy in z_copies + x_copies + c_copies + f_copies:
        copy.wait_send()


def gather_rows(own):
    n, wide = lax.axis_size("sp"), lax.axis_size("tp")
    if n > 8 or wide != 4:
        out = lax.all_gather(own, ("tp", "sp"), axis=0)
        return out.reshape((wide, n) + own.shape)
    dma = pltpu.SemaphoreType.DMA
    return pl.pallas_call(
        functools.partial(rows_kernel, n),
        out_shape=jax.ShapeDtypeStruct((wide, n) + own.shape, own.dtype),
        in_specs=[VMEM],
        out_specs=VMEM,
        scratch_shapes=[
            dma((n - 1,)),
            dma((n - 1,)),
            dma((n,)),
            dma((n,)),
            dma((2 * n,)),
            dma((2 * n,)),
        ],
        compiler_params=pltpu.CompilerParams(collective_id=2, has_side_effects=True),
        cost_estimate=pl.CostEstimate(flops=0, bytes_accessed=90_000_000, transcendentals=0),
        name="gather_rows",
    )(own)


def reduce_kernel(
    n, chunks, part_ref, base_ref, out_ref, got_c, sum_c, got_x, sum_x, got_z,
    c_send, c_recv, x_send, x_recv, z_send, z_recv,
):
    tp, near, far = partners()
    low, high = lax.rem(tp, 2), tp // 2
    shifts = range(1, n)
    me = lax.axis_index("sp") if n > 1 else 0
    greet([{"tp": near}, {"tp": far}] + [{"sp": lax.rem(me + k, n)} for k in shifts])
    width = part_ref.shape[-1] // chunks
    cols = [pl.ds(i * width, width) for i in range(chunks)]
    c_copies, x_copies, z_copies = [], [], []
    for i in range(chunks):
        copy = remote(
            part_ref.at[:, 1 - low, :, :, cols[i]],
            got_c.at[i],
            c_send.at[i],
            c_recv.at[i],
            {"tp": near},
        )
        copy.start()
        c_copies.append(copy)
    for i in range(chunks):
        c_copies[i].wait_recv()
        mine = part_ref[:, low, :, :, cols[i]].astype(jnp.float32)
        sum_c[i] = (mine + got_c[i].astype(jnp.float32)).astype(sum_c.dtype)
        copy = remote(
            sum_c.at[i, 1 - high], got_x.at[i], x_send.at[i], x_recv.at[i], {"tp": far}
        )
        copy.start()
        x_copies.append(copy)
    for i in range(chunks):
        x_copies[i].wait_recv()
        both = sum_c[i, high].astype(jnp.float32) + got_x[i].astype(jnp.float32)
        sum_x[i] = both.astype(sum_x.dtype)
        for k in shifts:
            peer = lax.rem(me + k, n)
            copy = remote(
                sum_x.at[i, peer],
                got_z.at[i, k - 1],
                z_send.at[i, k - 1],
                z_recv.at[i, k - 1],
                {"sp": peer},
            )
            copy.start()
            z_copies.append(copy)
    for i in range(chunks):
        total = sum_x[i, me].astype(jnp.float32)
        for k in shifts:
            z_copies[i * (n - 1) + k - 1].wait_recv()
            total = total + got_z[i, k - 1].astype(jnp.float32)
        out_ref[:, cols[i]] = (base_ref[:, cols[i]] + total).astype(out_ref.dtype)
    for copy in c_copies + x_copies + z_copies:
        copy.wait_send()


def reduce_rows(part, base, dtype, over_sp):
    wide, n = part.shape[:2]
    if n > 8 or wide != 4 or part.size > 8_000_000:
        axes = ("tp", "sp") if over_sp else "tp"
        flat = part.reshape(-1, part.shape[-1])
        total = lax.psum_scatter(flat, axes, scatter_dimension=0, tiled=True)
        return (base + total.astype(jnp.float32)).astype(dtype)
    rows, columns = part.shape[2:]
    chunks = 4 if columns % 512 == 0 else 1
    width = columns // chunks
    dma = pltpu.SemaphoreType.DMA
    zs = max(n - 1, 1)
    return pl.pallas_call(
        functools.partial(reduce_kernel, n, chunks),
        out_shape=jax.ShapeDtypeStruct((rows, columns), dtype),
        in_specs=[VMEM, VMEM],
        out_specs=VMEM,
        scratch_shapes=[
            pltpu.VMEM((chunks, 2, n, rows, width), part.dtype),
            pltpu.VMEM((chunks, 2, n, rows, width), part.dtype),
            pltpu.VMEM((chunks, n, rows, width), part.dtype),
            pltpu.VMEM((chunks, n, rows, width), part.dtype),
            pltpu.VMEM((chunks, zs, rows, width), part.dtype),
            dma((chunks,)),
            dma((chunks,)),
            dma((chunks,)),
            dma((chunks,)),
            dma((chunks, zs)),
            dma((chunks, zs)),
        ],
        compiler_params=pltpu.CompilerParams(
            collective_id=3 if over_sp else 4, has_side_effects=True
        ),
        cost_estimate=pl.CostEstimate(flops=0, bytes_accessed=60_000_000, transcendentals=0),
        name="reduce_all" if over_sp else "reduce_tp",
    )(part.reshape(2, 2, n, rows, columns), base)


def rotate(block, positions, heads):
    columns = block.shape[-1]
    width = columns // heads
    half = width // 2
    at = jnp.arange(columns, dtype=jnp.int32)
    freqs = ROPE_BASE ** (-(at % half).astype(jnp.float32) * 2.0 / width)
    angles = positions.astype(jnp.float32)[:, None] * freqs[None, :]
    source = jnp.where(at % width < half, at + half, at - half)
    sign = jnp.where(at % width < half, -1.0, 1.0)
    turn = jnp.where(at[:, None] == source[None, :], sign[None, :], 0.0).astype(jnp.bfloat16)
    flat = block.reshape(-1, columns)
    other = jnp.dot(flat, turn, preferred_element_type=jnp.float32).reshape(block.shape)
    turned = block.astype(jnp.float32) * jnp.cos(angles) + other * jnp.sin(angles)
    return turned.astype(jnp.bfloat16)


def depthwise(current, taps, docs):
    shown = current.astype(jnp.float32)
    total = taps[2] * shown
    for back in (1, 2):
        moved = jnp.pad(shown, ((0, 0), (back, 0), (0, 0)))[:, : shown.shape[1]]
        moved_docs = jnp.pad(docs, ((0, 0), (back, 0)), constant_values=-1)[:, : docs.shape[1]]
        total = total + jnp.where((moved_docs == docs)[..., None], taps[2 - back] * moved, 0.0)
    return total


def cyclic(array, axis, by):
    length = lax.axis_size(axis)
    return lax.ppermute(array, axis, [(i, (i + by) % length) for i in range(length)])


def exchange(piece, whole):
    count = lax.axis_size("sp")
    copies = lax.axis_size("grp")
    me = lax.axis_index("sp")
    mine = lax.axis_index("grp")
    if count > 8:
        pieces = jnp.stack([whole(dest) for dest in range(count)], axis=0)
        return lax.all_to_all(pieces, "sp", 0, 0)
    parts = []
    for shift in range(1, count):
        part = piece(lax.rem(me + shift, count), mine)
        parts.append(cyclic(part, "sp", shift))
    got = [jnp.stack(parts, axis=0)]
    for turn in range(1, copies):
        got.append(cyclic(got[0], "grp", turn))
    got = jnp.stack(got, axis=1)
    held = whole(me)
    held = jnp.broadcast_to(held[None], (1,) + held.shape)
    order = [lax.rem(mine - share + copies, copies) for share in range(copies)]
    out = []
    for source in range(count):
        shift = lax.rem(me - source + count, count)
        there = lax.max(shift - 1, 0)
        shares = [
            lax.dynamic_slice(got, (there, at) + (0,) * (got.ndim - 2), (1, 1) + got.shape[2:])[0]
            for at in order
        ]
        out.append(jnp.where(shift == 0, held, jnp.concatenate(shares, axis=0)[None]))
    return jnp.concatenate(out, axis=0)


def online_step(state, queries, keys, vals, allowed, scale):
    peak, total, accum = state
    scores = (
        jnp.einsum("sqhgd,skhd->shgqk", queries, keys, preferred_element_type=jnp.float32) * scale
    )
    mask = allowed[:, None, None]
    scores = jnp.where(mask, scores, NEG_BIG)
    new_peak = jnp.maximum(peak, jnp.max(scores, axis=-1))
    expd = jnp.where(mask, jnp.exp(scores - new_peak[..., None]), 0.0)
    fade = jnp.exp(peak - new_peak)
    new_total = total * fade + jnp.sum(expd, axis=-1)
    update = jnp.einsum(
        "shgqk,skhd->shgqd", expd.astype(jnp.bfloat16), vals, preferred_element_type=jnp.float32
    )
    return (new_peak, new_total, accum * fade[..., None] + update)


HBM = pl.BlockSpec(memory_space=pltpu.HBM)
SMEM = pl.BlockSpec(memory_space=pltpu.SMEM)
LANES = 128


def rounded(array):
    return array.astype(jnp.bfloat16)


def wide(array):
    return array.astype(jnp.float32)


def dot(left, right):
    return jnp.dot(left, right, preferred_element_type=jnp.float32)


class Phases:
    def __init__(self):
        self.open = None

    def __call__(self, name):
        if self.open is not None:
            self.open.__exit__(None, None, None)
        self.open = jax.named_scope(name) if name else None
        if name:
            self.open.__enter__()


def layer_kernel(
    n, per, tiles, scale,
    q_one, q_two, k_one, k_two, vals_own, doc_ids, lam, head_gain, norm_gain,
    taps_gate, taps_value, join, cosine_hbm, sine_hbm, turn_hbm, spread_hbm, resid_hbm, out_hbm, gate_hbm, value_hbm, down_hbm,
    out,
    cosine, sine, turn, spread, resid,
    kv_all, docs_all, docs_row, out_w, heads, part_one, got_one, sum_one, got_far, mid,
    rows_all, up_w, down_w, hidden, part_two, got_two, sum_far, got_x, sum_z, own_z, got_z, got_in, held_z,
    t_sem, d_send, d_recv, k_send, k_recv, o_sem, w_send, w_recv, y_send,
    c1_send, c1_recv, x1_send, x1_recv,
    az_send, az_recv, ax_send, ax_recv, ac_send, ac_recv,
    c2_send, c2_recv, x2_send, x2_recv, z2_send, z2_recv,
):
    phase = Phases()
    z, g = lax.axis_index("sp"), lax.axis_index("grp")
    tp, near, far = partners()
    low, high = lax.rem(tp, 2), tp // 2
    diag = (1 - high) * 2 + 1 - low
    other = {"grp": 1 - g}
    spare = per * n - tiles
    seqs, rows = q_one.shape[:2]
    depth, columns = gate_hbm.shape[0], down_hbm.shape[1]
    features, total = resid.shape[1], n * rows
    loads = [
        pltpu.make_async_copy(there, here, t_sem.at[at])
        for at, (there, here) in enumerate(
            ((cosine_hbm, cosine), (sine_hbm, sine), (turn_hbm, turn), (spread_hbm, spread), (resid_hbm, resid))
        )
    ]
    for load in loads:
        load.start()
    peers = [lax.rem(z + k, n) for k in range(1, n)]
    phase("greet")
    greet([{"sp": peer} for peer in peers] + [{"tp": near}, {"tp": far}, other])

    def rows_at(block):
        return pl.ds(pl.multiple_of(block * rows, rows), rows)

    phase("send_kv")
    def doc_copy(k, source, peer):
        part = docs_all.at[source]
        return remote(part, part, d_send.at[k], d_recv.at[source], {"sp": peer})

    def key_copy(block, p):
        half = seqs // 2
        part = kv_all.at[p * half : (p + 1) * half, rows_at(block)]
        peer = lax.rem(z + 1, n)
        return remote(part, part, k_send.at[block, p], k_recv.at[block, p], {"sp": peer})

    for seq in range(seqs):
        paired = dot(k_one[seq], join[0]) + dot(k_two[seq], join[1])
        kv_all[seq, rows_at(z), :LANES] = rounded(paired)
        kv_all[seq, rows_at(z), LANES:] = vals_own[seq]

    @pl.when(z < n - 1)
    def _():
        for p in (0, 1):
            key_copy(z, p).start()

    slot = lax.broadcasted_iota(jnp.int32, (rows, total), 1)
    spot = lax.broadcasted_iota(jnp.int32, (rows, total), 0) + z * rows
    place = jnp.where(slot == spot, 1.0, 0.0).astype(jnp.bfloat16)
    padded = jnp.concatenate([wide(doc_ids[...]), jnp.zeros((8 - seqs, rows), jnp.float32)], axis=0)
    docs_all[z] = dot(rounded(padded), place)
    for k, peer in enumerate(peers):
        doc_copy(k, z, peer).start()

    out_copy = pltpu.make_async_copy(out_hbm, out_w, o_sem)
    out_copy.start()

    def tile_of(block, k):
        return per * block + k - low * spare

    def valid(block, k):
        tile = tile_of(block, k)
        return (tile >= 0) & (tile < tiles)

    def weight_from(m, tile):
        at = pl.ds(pl.multiple_of(jnp.clip(tile, 0, tiles - 1) * LANES, LANES), LANES)
        if m == 2:
            return down_hbm.at[at, :]
        return (gate_hbm, value_hbm)[m].at[:, at]

    def weight_to(m, source, k):
        if m == 2:
            across = pl.ds(pl.multiple_of(source * columns, columns), columns)
            return down_w.at[pl.ds(k * LANES, LANES), across]
        along = pl.ds(pl.multiple_of(source * depth, depth), depth)
        return up_w.at[along, pl.ds((2 * k + m) * LANES, LANES)]

    def over_z(m, k, source, dest):
        return lax.rem(k + m + source + dest, 2) == g

    def z_copy(m, k, peer):
        return remote(
            weight_from(m, tile_of(peer, k)), weight_to(m, z, k),
            w_send.at[peer, (3 * k + m) // 2], w_recv.at[z, 3 * k + m], {"sp": peer},
        )

    def y_copy(m, k, source):
        block = weight_to(m, source, k)
        at = 3 * k + m
        return remote(block, block, y_send.at[source, at // 2], w_recv.at[source, at], other)

    def own_copy(m, k):
        return pltpu.make_async_copy(
            weight_from(m, tile_of(z, k)), weight_to(m, z, k), w_recv.at[z, 3 * k + m]
        )

    def at_distance(d):
        return ((lax.rem(z - d + n, n), z - d >= 0), (lax.rem(z + d, n), z + d < n))

    def when_sent(d, items, act, ways=(0, 1)):
        for way in ways:
            peer, there = at_distance(d)[way]
            for k, m in items:

                @pl.when(there & valid(peer, k) & over_z(m, k, z, peer))
                def _():
                    act(z_copy(m, k, peer))

    def when_hopped(d, items, act):
        for k, m in items:
            for source, there in at_distance(d):

                @pl.when(there & valid(z, k) & over_z(m, k, source, z))
                def _():
                    act(y_copy(m, k, source))

    def send(d, items, ways=(0, 1)):
        when_sent(d, items, lambda copy: copy.start(), ways)

    def relay(d, items):
        def act(copy):
            copy.wait_recv()
            copy.start()

        when_hopped(d, items, act)

    ups = [(k, m) for k in range(per) for m in (0, 1)]
    downs = [(k, 2) for k in range(per)]
    early, middle, late = ups[: 2 * per - 2], ups[2 * per - 2 : 2 * per - 1], ups[2 * per - 1 :]

    def settle(m, k):
        for source in peers:

            @pl.when(valid(z, k) & jnp.logical_not(over_z(m, k, source, z)))
            def _():
                y_copy(m, k, source).wait_recv()

        @pl.when(valid(z, k))
        def _():
            own_copy(m, k).wait()

    phase("send_up")
    for d in range(1, n):
        send(d, early + middle, (0,))
    for step in range(1, n):
        block = z - step

        @pl.when(block >= 0)
        def _():
            for p in (0, 1):
                key_copy(block, p).wait_recv()

                @pl.when(z < n - 1)
                def _():
                    key_copy(block, p).start()

    for d in range(1, n):
        send(d, early, (1,))
    for k in range(per):

        @pl.when(valid(z, k))
        def _():
            for m in (0, 1, 2):
                own_copy(m, k).start()

        @pl.when(jnp.logical_not(valid(z, k)))
        def _():
            pair = pl.ds(2 * k * LANES, 2 * LANES)
            up_w[:, pair] = jnp.zeros((up_w.shape[0], 2 * LANES), up_w.dtype)
            one = pl.ds(k * LANES, LANES)
            down_w[one, :] = jnp.zeros((LANES, down_w.shape[1]), down_w.dtype)

    for block in range(1, n):

        @pl.when(block > z)
        def _():
            blank = jnp.zeros((kv_all.shape[0], rows, kv_all.shape[2]), kv_all.dtype)
            kv_all[:, pl.ds(block * rows, rows)] = blank

    phase("wait_kv")
    for k, source in enumerate(peers):
        doc_copy(k, source, source).wait_recv()
    all_docs = functools.reduce(lambda a, b: a + b, [docs_all[i] for i in range(n)])
    for seq in range(seqs):
        docs_row[seq] = jnp.broadcast_to(all_docs[seq : seq + 1], (8, total))
    gain = jnp.concatenate([head_gain[...], head_gain[...]], axis=1)

    def iota(height, width, axis):
        return lax.broadcasted_iota(jnp.int32, (height, width), axis)

    def attend(seq, carry):
        doc_row = docs_row[seq][0:1]
        at_query = iota(rows, total, 0) + z * rows
        at_key = iota(rows, total, 1)
        doc_query = jnp.sum(jnp.where(at_key == at_query, doc_row, 0.0), axis=1, keepdims=True)
        allowed = (at_key <= at_query) & (doc_row == doc_query)
        bias = jnp.where(allowed, 0.0, NEG_BIG)
        bias = jnp.concatenate([bias] * 4, axis=0)
        q_cos, q_sin = cosine[rows_at(z)], sine[rows_at(z)]
        packed = kv_all[seq]
        spun = dot(packed[:, :LANES], spread[...])
        vals = wide(packed[:, LANES:])
        swapped = pltpu.roll(vals, LANES // 2, 1)
        lane = iota(total, LANES, 1)
        queries, keys = [], []
        width = cosine.shape[1]
        for index, source in enumerate((q_one, q_two)):
            block = source[seq]
            turned = wide(block) * q_cos + dot(block, turn[...]) * q_sin
            queries.append(rounded(turned))
            start = 2 * index * width
            straight = spun[:, start : start + width]
            crossed = spun[:, start + width : start + 2 * width]
            keys.append(rounded(straight * cosine[...] + crossed * sine[...]))
        q_lane = iota(rows, LANES, 1) // (LANES // 4)
        row4 = iota(4 * rows, 1, 0) // rows
        half_lane = iota(2 * rows, LANES, 1) < LANES // 2
        for c in range(2):
            across = slice(c * LANES, (c + 1) * LANES)
            pair = (vals, swapped) if c == 0 else (swapped, vals)
            both = rounded(jnp.where(lane < LANES // 2, pair[0], pair[1]))
            found = []
            for query, key in zip(queries, keys):
                local = wide(query[:, across])
                stack = jnp.concatenate(
                    [rounded(jnp.where(q_lane == j, local, 0.0)) for j in (0, 2, 1, 3)], axis=0
                )
                scores = lax.dot_general(
                    stack, key[:, across], (((1,), (1,)), ((), ())),
                    preferred_element_type=jnp.float32,
                )
                scores = scores * scale + bias
                expd = jnp.exp(scores - jnp.max(scores, axis=1, keepdims=True))
                summed = jnp.sum(expd, axis=1, keepdims=True)
                found.append(dot(rounded(expd), both) / summed)
            weights = jnp.where(
                row4 == 0, lam[4 * c],
                jnp.where(
                    row4 == 1, lam[4 * c + 2],
                    jnp.where(row4 == 2, lam[4 * c + 1], lam[4 * c + 3]),
                ),
            )
            mixed = found[0] - weights * found[1]
            meansq = jnp.sum(mixed * mixed, axis=1, keepdims=True) * (1.0 / LANES)
            normed = mixed * lax.rsqrt(meansq + NORM_EPS) * gain
            merged = rounded(jnp.where(half_lane, normed[: 2 * rows], normed[2 * rows :]))
            base = 2 * c * LANES
            heads[seq, :, base : base + LANES] = merged[:rows]
            heads[seq, :, base + LANES : base + 2 * LANES] = merged[rows:]
        return carry

    for load in loads:
        load.wait()
    phase("attend")
    lax.fori_loop(0, seqs, attend, 0)

    phase("proj")
    out_copy.wait()
    halves = got_one.shape[0]
    width = features // halves

    def c1_copy(i):
        cols = pl.ds(i * width, width)
        return remote(
            part_one.at[:, 1 - low, :, cols], got_one.at[i], c1_send.at[i], c1_recv.at[i], {"tp": near}
        )

    def x1_copy(i):
        return remote(sum_one.at[i], got_far.at[i], x1_send.at[i], x1_recv.at[i], {"tp": far})

    flat = heads[...].reshape(4 * rows, heads.shape[2])
    for i in range(halves):
        cols = pl.ds(i * width, width)
        made = rounded(dot(flat, out_w[:, cols]))
        part_one[:, :, :, cols] = made.reshape(2, 2, rows, width)
        c1_copy(i).start()
    phase("wait_c1")
    for i in range(halves):
        cols = pl.ds(i * width, width)
        c1_copy(i).wait_recv()
        sum_one[i] = rounded(wide(part_one[1 - high, low, :, cols]) + wide(got_one[i, 1 - high]))
        x1_copy(i).start()
        kept = wide(part_one[high, low, :, cols]) + wide(got_one[i, high])
        mid[:, cols] = wide(resid[:, cols]) + kept
    phase("relay_u1")
    relay(1, early)
    phase("wait_x1")
    for i in range(halves):
        cols = pl.ds(i * width, width)
        x1_copy(i).wait_recv()
        mid[:, cols] = mid[:, cols] + wide(got_far[i])
    phase("norm")
    held = mid[...]
    meansq = jnp.mean(held * held, axis=1, keepdims=True)
    rows_all[tp, rows_at(z)] = rounded(held * lax.rsqrt(meansq + NORM_EPS) * norm_gain[...])

    cuts = 2
    part_rows = rows // cuts

    def piece_of(owner, block, p):
        first = pl.multiple_of(block * rows + p * part_rows, part_rows)
        return rows_all.at[owner, pl.ds(first, part_rows)]

    def x_copy(owner, block, p):
        part = piece_of(owner, block, p)
        return remote(part, part, ax_send.at[block, p], ax_recv.at[block, p], {"tp": far})

    def c_copy(owner, hop, block):
        part = rows_all.at[owner, rows_at(block)]
        sems = (ac_send.at[hop, block], ac_recv.at[hop, block])
        return remote(part, part, *sems, {"tp": near})

    def chain_copy(way, block, p):
        part = piece_of(tp, block, p)
        peer = lax.rem(z + (1 if way == 0 else n - 1), n)
        return remote(part, part, az_send.at[way, block, p], az_recv.at[block, p], {"sp": peer})

    def pass_on(block, p):
        @pl.when((z >= block) & (z < n - 1))
        def _():
            chain_copy(0, block, p).start()

        @pl.when((z <= block) & (z > 0))
        def _():
            chain_copy(1, block, p).start()

        x_copy(tp, block, p).start()
        if p == cuts - 1:
            c_copy(tp, 0, block).start()

    def chain(step):
        for p in range(cuts):
            for block in (z - step, z + step):

                @pl.when((block >= 0) & (block < n))
                def _():
                    chain_copy(0, block, p).wait_recv()
                    pass_on(block, p)

    phase("ag_start")
    for p in range(cuts):
        pass_on(z, p)

    phase("relay_u2")
    for d in range(2, n):
        relay(d, early)
    for step in range(1, n):
        phase(f"ag_z{step}")
        chain(step)
        ends = (z == 0) | (z == n - 1)
        for at, items in ((2, (late, middle + late)), (2, (downs, downs))):

            @pl.when((ends & (step == at)) | (jnp.logical_not(ends) & (step == 1)))
            def _():
                for d in range(1, n):
                    for way in (0, 1):
                        send(d, items[way], (way,))

    phase("relay_u3")
    for d in range(1, n):
        relay(d, middle + late)
    phase("relay_d3")
    relay(1, downs)
    relay(2, downs)
    phase("settle_up")
    for k, m in ups:
        settle(m, k)

    def cross():
        for step in range(n):
            for p in range(cuts):
                for block in (z - step, z + step) if step else (z,):

                    @pl.when((block >= 0) & (block < n))
                    def _():
                        x_copy(far, block, p).wait_recv()
                        if p == cuts - 1:
                            c_copy(far, 1, block).start()

    def lift(i, carry):
        seq = lax.rem(high + i // 2, 2) * 2 + lax.rem(low + i, 2)
        for turn_at, (owner, hop) in ((1, (near, 0)), (3, (diag, 1))):

            @pl.when(i == turn_at)
            def _():
                for block in range(n):
                    c_copy(owner, hop, block).wait_recv()

        @pl.when(i == 1)
        def _():
            for d in range(3, n):
                relay(d, downs)

        @pl.when(i == 2)
        def _():
            cross()

        doc_row = docs_row[seq][0:1]
        at_row, at_col = iota(total, total, 0), iota(total, total, 1)
        doc_col = jnp.sum(jnp.where(at_row == at_col, doc_row, 0.0), axis=1, keepdims=True)
        same = jnp.where(doc_row == doc_col, 1.0, 0.0)
        back_one, back_two = [
            jnp.sum(jnp.where(at_col == at_row - back, same, 0.0), axis=1, keepdims=True)
            for back in (1, 2)
        ]

        def depthwise_of(current, taps):
            shown = wide(rounded(current))
            return (
                taps[2:3] * shown
                + taps[1:2] * (pltpu.roll(shown, 1, 0) * back_one)
                + taps[0:1] * (pltpu.roll(shown, 2, 0) * back_two)
            )

        for k in range(per):
            made = dot(rows_all[seq], up_w[:, 2 * k * LANES : (2 * k + 2) * LANES])
            tile = jnp.clip(tile_of(z, k), 0, tiles - 1)
            at = pl.ds(pl.multiple_of(tile * LANES, LANES), LANES)
            conv_g = depthwise_of(made[:, :LANES], taps_gate[:, at])
            conv_v = depthwise_of(made[:, LANES:], taps_value[:, at])
            unit = conv_g / (1.0 + jnp.exp(-conv_g)) * conv_v
            hidden[seq, :, k * LANES : (k + 1) * LANES] = rounded(unit)
        return carry

    phase("lift")
    lax.fori_loop(0, rows_all.shape[0], lift, 0)
    phase("settle_d")
    for k in range(per):
        settle(2, k)

    def c2_copy(i, seq, block):
        there = rows_at(block)
        sems = (c2_send.at[i, block], c2_recv.at[i, block])
        return remote(part_two.at[seq, there], got_two.at[i, there], *sems, {"tp": near})

    chunk = 512 if features % 512 == 0 else features
    upper = z // (n // 2)
    mate = n // 2 - 1 - z + upper * n
    gate = (z == n // 2 - 1) | (z == n // 2)
    across = [upper * j + (1 - upper) * (n - 1 - j) for j in range(n // 2)]
    order = across + [mate, z]
    stops = [(j, p) for j in range(len(order)) for p in range(cuts)]

    def slot(p):
        return pl.ds(p * part_rows, part_rows)

    def piece_rows(block, p):
        return pl.ds(pl.multiple_of(block * rows + p * part_rows, part_rows), part_rows)

    def x2_copy(block, p):
        sems = (x2_send.at[block, p], x2_recv.at[block, p])
        return remote(sum_far.at[block, slot(p)], got_x.at[block, slot(p)], *sems, {"tp": far})

    def mate_copy(p):
        sems = (z2_send.at[2, p], z2_recv.at[2, p])
        return remote(sum_z.at[2, slot(p)], got_z.at[0, slot(p)], *sems, {"sp": mate})

    def inner_copy(j, p):
        sems = (z2_send.at[j, p], z2_recv.at[j, p])
        return remote(sum_z.at[j, slot(p)], got_in.at[j, slot(p)], *sems, {"sp": mate})

    def outer_copy(j, p):
        sems = (z2_send.at[j, p], z2_recv.at[3, p])
        return remote(sum_z.at[j, slot(p)], got_z.at[1, slot(p)], *sems, {"sp": across[j]})

    def combine(j, p):
        @pl.when(gate)
        def _():
            inner_copy(j, p).wait_recv()
            sum_z[j, slot(p)] = rounded(held_z[j, slot(p)] + wide(got_in[j, slot(p)]))
            outer_copy(j, p).start()

    def lower(i, carry):
        seq = lax.rem(high + 1 - i // 2, 2) * 2 + lax.rem(low + 1 - lax.rem(i, 2), 2)
        for c in range(features // chunk):
            cols = slice(c * chunk, (c + 1) * chunk)
            part_two[seq, :, cols] = rounded(dot(hidden[seq], down_w[:, cols]))

        @pl.when(lax.rem(i, 2) == 0)
        def _():
            for block in order:
                c2_copy(i // 2, seq, block).start()

        @pl.when(i == 1)
        def _():
            for block in order:
                c2_copy(0, diag, block).wait_recv()
                for p in range(cuts):
                    there = piece_rows(block, p)
                    both = wide(part_two[far, there]) + wide(got_two[0, there])
                    sum_far[block, slot(p)] = rounded(both)
                    x2_copy(block, p).start()

        return carry

    phase("lower")
    lax.fori_loop(0, rows_all.shape[0], lower, 0)
    phase("x2")
    lag = 2
    for t, (j, p) in enumerate(stops):
        block = order[j]
        if p == 0:
            c2_copy(1, near, block).wait_recv()
        there = piece_rows(block, p)
        x2_copy(block, p).wait_recv()
        both = wide(part_two[tp, there]) + wide(got_two[1, there]) + wide(got_x[block, slot(p)])
        if j < len(across):

            @pl.when(gate)
            def _():
                held_z[j, slot(p)] = both

            @pl.when(jnp.logical_not(gate))
            def _():
                sum_z[j, slot(p)] = rounded(both)
                inner_copy(j, p).start()

        elif j == len(across):
            sum_z[j, slot(p)] = rounded(both)
            mate_copy(p).start()
        else:
            own_z[slot(p)] = mid[slot(p)] + both
        if t >= lag and stops[t - lag][0] < len(across):
            combine(*stops[t - lag])
    phase("z2")
    for p in range(cuts):
        mate_copy(p).wait_recv()
        outer_copy(0, p).wait_recv()
        answer = own_z[slot(p)] + wide(got_z[0, slot(p)]) + wide(got_z[1, slot(p)])
        out[slot(p)] = answer.astype(out.dtype)

    phase("drain")
    for k, peer in enumerate(peers):
        doc_copy(k, z, peer).wait_send()
    for p in range(cuts):
        mate_copy(p).wait_send()
        for j in range(len(across)):
            inner_copy(j, p).wait_send()
    for d in range(1, n):
        when_sent(d, ups + downs, lambda copy: copy.wait_send())
        when_hopped(d, ups + downs, lambda copy: copy.wait_send())
    for i in range(halves):
        c1_copy(i).wait_send()
        x1_copy(i).wait_send()
    for block in range(n):

        @pl.when((z >= block) & (z < n - 1))
        def _():
            for p in range(cuts):
                chain_copy(0, block, p).wait_send()
            for p in (0, 1):
                key_copy(block, p).wait_send()

        @pl.when((z <= block) & (z > 0))
        def _():
            for p in range(cuts):
                chain_copy(1, block, p).wait_send()

        for p in range(cuts):
            x_copy(tp, block, p).wait_send()
            x2_copy(block, p).wait_send()
        c_copy(tp, 0, block).wait_send()
        c_copy(far, 1, block).wait_send()
        c2_copy(0, diag, block).wait_send()
        c2_copy(1, near, block).wait_send()
    phase(None)


def rope_tables(total, width, copies):
    half = width // 2
    freqs = np.float32(ROPE_BASE) ** (-np.arange(half, dtype=np.float32) * np.float32(2.0) / np.float32(width))
    angles = np.arange(total, dtype=np.float32)[:, None] * freqs.astype(np.float32)[None, :]
    tile = lambda table: np.tile(table.astype(np.float32), (1, 2 * copies))
    return tile(np.cos(angles)), tile(np.sin(angles))


def turn_matrix(width):
    half = width // 2
    at = np.arange(width)
    source = np.where(at < half, at + half, at - half)
    sign = np.where(at < half, -1.0, 1.0)
    return np.where(at[:, None] == source[None, :], sign[None, :], 0.0)


def spread_matrix(width, group, kv_local):
    straight = np.kron(np.eye(kv_local), np.tile(np.eye(width), (1, group)))
    crossed = np.kron(np.eye(kv_local), np.tile(turn_matrix(width), (1, group)))
    both = np.concatenate([straight, crossed], axis=1)
    return np.kron(np.eye(2), both)


def kernel_fits(resid_in, query_one, key_one, value, lam, gate_weight):
    heads = lam.shape[0]
    width = query_one.shape[2] // heads
    kv_local = key_one.shape[2] // width
    group = heads // kv_local
    seqs, rows = query_one.shape[:2]
    return (
        lax.axis_size("tp") == 4
        and lax.axis_size("grp") == 2
        and lax.axis_size("sp") == 4
        and kv_local == 2
        and group == 4
        and group * width == LANES
        and value.shape[2] == LANES
        and seqs == 4
        and resid_in.shape[0] == 1
        and rows % 16 == 0
        and rows * lax.axis_size("sp") <= 256
        and gate_weight.shape[0] <= 512
        and gate_weight.shape[1] % LANES == 0
        and gate_weight.shape[1] <= 1536
        and resid_in.shape[2] <= 2048
    )


def whole_layer(
    resid_in, query_one, key_one, query_two, key_two, value, lam, head_gain, doc_ids,
    out_weight, norm_gain, gate_weight, value_weight, conv_gate, conv_value, down_weight,
):
    n = lax.axis_size("sp")
    seqs, rows = query_one.shape[:2]
    heads = lam.shape[0]
    width = query_one.shape[2] // heads
    kv_local = key_one.shape[2] // width
    group = heads // kv_local
    features, total = resid_in.shape[2], n * rows
    depth, columns = gate_weight.shape[0], down_weight.shape[1]
    tiles = gate_weight.shape[1] // LANES
    per = -(-tiles // n)
    cosine, sine = rope_tables(total, width, heads)
    turn = np.kron(np.eye(heads), turn_matrix(width))
    spread = spread_matrix(width, group, kv_local)
    key_width = kv_local * width
    join = np.stack([np.eye(key_width, LANES), np.eye(key_width, LANES, LANES - key_width)])
    halves = 2
    bf16, f32 = jnp.bfloat16, jnp.float32
    dma = pltpu.SemaphoreType.DMA
    vmem = pltpu.VMEM
    scratch = [
        vmem(cosine.shape, f32),
        vmem(sine.shape, f32),
        vmem(turn.shape, bf16),
        vmem(spread.shape, bf16),
        vmem((rows, features), bf16),
        vmem((seqs, total, 2 * LANES), bf16),
        vmem((n, 8, total), f32),
        vmem((seqs, 8, total), f32),
        vmem(out_weight.shape, bf16),
        vmem((seqs, rows, out_weight.shape[0]), bf16),
        vmem((2, 2, rows, features), bf16),
        vmem((halves, 2, rows, features // halves), bf16),
        vmem((halves, rows, features // halves), bf16),
        vmem((halves, rows, features // halves), bf16),
        vmem((rows, features), f32),
        vmem((seqs, total, features), bf16),
        vmem((n * depth, 2 * per * LANES), bf16),
        vmem((per * LANES, n * columns), bf16),
        vmem((seqs, total, per * LANES), bf16),
        vmem((seqs, total, features), bf16),
        vmem((2, total, features), bf16),
        vmem((n, rows, features), bf16),
        vmem((n, rows, features), bf16),
        vmem((n - 1, rows, features), bf16),
        vmem((rows, features), f32),
        vmem((2, rows, features), bf16),
        vmem((2, rows, features), bf16),
        vmem((2, rows, features), f32),
        dma((5,)), dma((n,)), dma((n,)), dma((n, 2)), dma((n, 2)), dma,
        dma((n, 3 * per // 2 + 1)), dma((n, 3 * per)), dma((n, 3 * per // 2 + 1)),
        dma((halves,)), dma((halves,)), dma((halves,)), dma((halves,)),
        dma((2, n, 2)), dma((n, 2)), dma((n, 2)), dma((n, 2)), dma((2, n)), dma((2, n)),
        dma((2, n)), dma((2, n)), dma((n, 2)), dma((n, 2)), dma((3, 2)), dma((n, 2)),
    ]
    out = pl.pallas_call(
        functools.partial(layer_kernel, n, per, tiles, width ** (-0.5)),
        out_shape=jax.ShapeDtypeStruct((rows, features), f32),
        in_specs=[VMEM] * 6 + [SMEM] + [VMEM] * 5 + [HBM] * 9,
        out_specs=VMEM,
        scratch_shapes=scratch,
        compiler_params=pltpu.CompilerParams(
            collective_id=5, has_side_effects=True, vmem_limit_bytes=60 * 2**20
        ),
        name="whole_layer",
    )(
        query_one, query_two, key_one, key_two, value,
        doc_ids, lam, head_gain[None], norm_gain[None], conv_gate, conv_value,
        jnp.asarray(join, bf16), jnp.asarray(cosine), jnp.asarray(sine), jnp.asarray(turn, bf16),
        jnp.asarray(spread, bf16), resid_in.reshape(rows, features),
        out_weight, gate_weight, value_weight, down_weight,
    )
    return out.astype(resid_in.dtype).reshape(resid_in.shape)


def per_device_apart(
    resid_in,
    query_one,
    key_one,
    query_two,
    key_two,
    value,
    lam,
    head_gain,
    doc_ids,
    out_weight,
    norm_gain,
    gate_weight,
    value_weight,
    conv_gate,
    conv_value,
    down_weight,
):
    n_sp = lax.axis_size("sp")
    me = lax.axis_index("sp")
    depth, width = gate_weight.shape
    share = width // n_sp
    copies = lax.axis_size("grp")

    def cut(weight, row, column, size):
        return lax.dynamic_slice(weight, (row, column), size)

    def up_piece(dest, part):
        size = (depth // copies, share)
        row, column = part * size[0], dest * share
        return jnp.stack([cut(gate_weight, row, column, size), cut(value_weight, row, column, size)])

    def up_whole(dest):
        return jnp.stack([up_piece(dest, part) for part in range(copies)])

    def down_piece(dest, part):
        size = (share // copies, down_weight.shape[1])
        return cut(down_weight, dest * share + part * size[0], 0, size)

    def down_whole(dest):
        return jnp.stack([down_piece(dest, part) for part in range(copies)])

    up_all = exchange(up_piece, up_whole)
    down_all = exchange(down_piece, down_whole)
    gate_all = up_all[:, :, 0].reshape(-1, share)
    value_all = up_all[:, :, 1].reshape(-1, share)
    down_full = jnp.transpose(down_all, (1, 2, 0, 3)).reshape(share, -1)
    seqs = query_one.shape[0]
    rows = query_one.shape[1]
    heads = lam.shape[0]
    key_width = query_one.shape[2] // heads
    kv_local = key_one.shape[2] // key_width
    group = heads // kv_local
    head_width = value.shape[2] // kv_local
    scale = key_width ** (-0.5)
    positions = lax.axis_index("sp") * rows + jnp.arange(rows, dtype=jnp.int32)
    q_first = rotate(query_one, positions, heads).reshape(seqs, rows, kv_local, group, key_width)
    q_second = rotate(query_two, positions, heads).reshape(seqs, rows, kv_local, group, key_width)
    k_first = rotate(key_one, positions, kv_local).reshape(seqs, rows, kv_local * key_width)
    k_second = rotate(key_two, positions, kv_local).reshape(seqs, rows, kv_local * key_width)
    start_state = (
        jnp.full((seqs, kv_local, group, rows), NEG_BIG, jnp.float32),
        jnp.zeros((seqs, kv_local, group, rows), jnp.float32),
        jnp.zeros((seqs, kv_local, group, rows, head_width), jnp.float32),
    )
    packed = jnp.concatenate(
        [k_first, k_second, value, doc_ids.astype(jnp.bfloat16)[..., None]], axis=-1
    )
    packed = gather_sp(packed)
    key_cols = k_first.shape[2]
    keys_one = packed[..., :key_cols]
    keys_two = packed[..., key_cols : 2 * key_cols]
    vals = packed[..., 2 * key_cols : -1]
    docs = packed[..., -1].astype(jnp.int32)
    count = keys_one.shape[1]
    step_len = math.gcd(count, 512)

    def inner(state, index):
        offset = index * step_len
        ka = lax.dynamic_slice_in_dim(keys_one, offset, step_len, 1).reshape(
            seqs, step_len, kv_local, key_width
        )
        kb = lax.dynamic_slice_in_dim(keys_two, offset, step_len, 1).reshape(
            seqs, step_len, kv_local, key_width
        )
        va = lax.dynamic_slice_in_dim(vals, offset, step_len, 1).reshape(
            seqs, step_len, kv_local, head_width
        )
        dpiece = lax.dynamic_slice_in_dim(docs, offset, step_len, 1)
        key_pos = offset + jnp.arange(step_len, dtype=jnp.int32)
        allowed = (key_pos[None, None, :] <= positions[None, :, None]) & (
            dpiece[:, None, :] == doc_ids[:, :, None]
        )
        first = online_step(state[0], q_first, ka, va, allowed, scale)
        second = online_step(state[1], q_second, kb, va, allowed, scale)
        return ((first, second), None)

    def run(state):
        return lax.scan(inner, state, jnp.arange(count // step_len))[0]

    first, second = lax.cond(
        jnp.int32(0) <= positions[rows - 1], run, lambda state: state, (start_state, start_state)
    )
    weights = lam.reshape(kv_local, group)[None, :, :, None, None]
    mixed = first[2] / first[1][..., None] - weights * (second[2] / second[1][..., None])
    meansq = jnp.mean(mixed * mixed, axis=-1, keepdims=True)
    normed_heads = mixed * lax.rsqrt(meansq + NORM_EPS) * head_gain
    heads_out = jnp.transpose(normed_heads, (0, 3, 1, 2, 4)).reshape(
        seqs * rows, heads * head_width
    )
    heads_out = heads_out.astype(jnp.bfloat16)
    own = resid_in.shape[0]
    features = resid_in.shape[2]
    proj = jnp.dot(heads_out, out_weight, preferred_element_type=jnp.float32).astype(jnp.bfloat16)
    mid = reduce_rows(
        proj.reshape(-1, 1, own * rows, features),
        resid_in.astype(jnp.float32).reshape(own * rows, features),
        jnp.float32,
        False,
    )
    meansq_mid = jnp.mean(mid * mid, axis=-1, keepdims=True)
    normed = (mid * lax.rsqrt(meansq_mid + NORM_EPS) * norm_gain).astype(jnp.bfloat16)
    gathered = gather_rows(normed).reshape(-1, n_sp, own, rows, features)
    full_rows = jnp.transpose(gathered, (0, 2, 1, 3, 4)).reshape(-1, features)
    total_rows = n_sp * rows
    start = me * share
    taps_gate = lax.dynamic_slice_in_dim(conv_gate, start, share, 1)
    taps_value = lax.dynamic_slice_in_dim(conv_value, start, share, 1)
    up_gate = jnp.dot(full_rows, gate_all, preferred_element_type=jnp.float32)
    up_value = jnp.dot(full_rows, value_all, preferred_element_type=jnp.float32)
    up_gate = up_gate.astype(jnp.bfloat16).reshape(seqs, total_rows, share)
    up_value = up_value.astype(jnp.bfloat16).reshape(seqs, total_rows, share)
    conv_g = depthwise(up_gate, taps_gate, docs)
    conv_v = depthwise(up_value, taps_value, docs)
    hidden = (jax.nn.silu(conv_g) * conv_v).astype(jnp.bfloat16)
    hidden = hidden.reshape(-1, own, n_sp, rows, share)
    hidden = jnp.transpose(hidden, (0, 2, 1, 3, 4)).reshape(-1, share)
    partial_down = jnp.dot(hidden, down_full, preferred_element_type=jnp.float32)
    partial_down = partial_down.astype(jnp.bfloat16).reshape(-1, n_sp, own * rows, features)
    return reduce_rows(partial_down, mid, jnp.bfloat16, True).reshape(resid_in.shape)


def per_device(*args):
    resid_in, query_one, key_one, value, lam, gate_weight = [args[i] for i in (0, 1, 2, 5, 6, 11)]
    if kernel_fits(resid_in, query_one, key_one, value, lam, gate_weight):
        return whole_layer(*args)
    return per_device_apart(*args)


def solution(mesh):
    placed = (
        P(("grp", "tp"), "sp", None),
        P("grp", "sp", "tp"),
        P("grp", "sp", "tp"),
        P("grp", "sp", "tp"),
        P("grp", "sp", "tp"),
        P("grp", "sp", "tp"),
        P("tp"),
        P(),
        P("grp", "sp"),
        P("tp", None),
        P(),
        P("sp", "tp"),
        P("sp", "tp"),
        P(None, "tp"),
        P(None, "tp"),
        P("tp", "sp"),
    )
    return jax.shard_map(
        per_device,
        mesh=mesh,
        in_specs=placed,
        out_specs=P(("grp", "tp"), "sp", None),
        check_vma=False,
    )
```

```python
import functools
import math

import jax
import jax.numpy as jnp
import numpy as np
from jax import lax
from jax.experimental import pallas as pl
from jax.experimental.pallas import tpu as pltpu
from jax.sharding import PartitionSpec as P

NEG_BIG = -1e30
NORM_EPS = 1e-06
ROPE_BASE = 500000.0


MESH = pl.DeviceIdType.MESH
VMEM = pl.BlockSpec(memory_space=pltpu.VMEM)


def greet(devices):
    barrier = pltpu.get_barrier_semaphore()
    for device in devices:
        pl.semaphore_signal(barrier, inc=1, device_id=device, device_id_type=MESH)
    pl.semaphore_wait(barrier, len(devices))


def remote(src, dst, send_sem, recv_sem, device):
    return pltpu.make_async_remote_copy(
        src_ref=src,
        dst_ref=dst,
        send_sem=send_sem,
        recv_sem=recv_sem,
        device_id=device,
        device_id_type=MESH,
    )


def partners():
    at = lax.axis_index("tp")
    return at, at + 1 - 2 * lax.rem(at, 2), lax.rem(at + 2, 4)


def spread_kernel(n, own_ref, out_ref, send_sem, recv_sem):
    me = lax.axis_index("sp")
    peers = [lax.rem(me + shift, n) for shift in range(1, n)]
    greet([{"sp": peer} for peer in peers])
    copies = []
    for k, peer in enumerate(peers):
        copy = remote(
            own_ref, out_ref.at[:, me], send_sem.at[k], recv_sem.at[k], {"sp": peer}
        )
        copy.start()
        copies.append(copy)
    out_ref[:, me] = own_ref[...]
    for copy in copies:
        copy.wait_recv()
    for copy in copies:
        copy.wait_send()


def gather_sp(own):
    n = lax.axis_size("sp")
    if n > 8:
        return lax.all_gather(own, "sp", axis=1, tiled=True)
    outer, rows, width = own.shape
    out = pl.pallas_call(
        functools.partial(spread_kernel, n),
        out_shape=jax.ShapeDtypeStruct((outer, n, rows, width), own.dtype),
        in_specs=[VMEM],
        out_specs=VMEM,
        scratch_shapes=[pltpu.SemaphoreType.DMA((n - 1,)), pltpu.SemaphoreType.DMA((n - 1,))],
        compiler_params=pltpu.CompilerParams(collective_id=1, has_side_effects=True),
        cost_estimate=pl.CostEstimate(flops=0, bytes_accessed=30_000_000, transcendentals=0),
        name="gather_sp",
    )(own)
    return out.reshape(outer, n * rows, width)


def rows_kernel(n, own_ref, out_ref, z_send, z_recv, x_send, x_recv, c_send, c_recv):
    me = lax.axis_index("sp")
    tp, near, far = partners()
    greet([{"tp": near}, {"tp": far}] + [{"sp": lax.rem(me + k, n)} for k in range(1, n)])
    sources = [lax.rem(me - k + n, n) for k in range(n)]
    z_copies = []
    for k in range(1, n):
        copy = remote(
            own_ref,
            out_ref.at[tp, me],
            z_send.at[k - 1],
            z_recv.at[k - 1],
            {"sp": lax.rem(me + k, n)},
        )
        z_copies.append(copy)

    def along(owner, k, send, recv, device):
        block = out_ref.at[owner, sources[k]]
        return remote(block, block, send, recv, device)

    x_copies = [remote(own_ref, out_ref.at[tp, me], x_send.at[0], x_recv.at[0], {"tp": far})]
    c_copies = [remote(own_ref, out_ref.at[tp, me], c_send.at[0], c_recv.at[0], {"tp": near})]
    for k in range(1, n):
        x_copies.append(along(tp, k, x_send.at[k], x_recv.at[k], {"tp": far}))
        c_copies.append(along(tp, k, c_send.at[k], c_recv.at[k], {"tp": near}))
    f_copies = [along(far, k, c_send.at[n + k], c_recv.at[n + k], {"tp": near}) for k in range(n)]
    x_copies[0].start()
    for copy in z_copies:
        copy.start()
    c_copies[0].start()
    out_ref[tp, me] = own_ref[...]
    for k in range(1, n):
        z_copies[k - 1].wait_recv()
        x_copies[k].start()
        c_copies[k].start()
    for k in range(n):
        x_copies[k].wait_recv()
        f_copies[k].start()
    for copy in c_copies + f_copies:
        copy.wait_recv()
    for copy in z_copies + x_copies + c_copies + f_copies:
        copy.wait_send()


def gather_rows(own):
    n, wide = lax.axis_size("sp"), lax.axis_size("tp")
    if n > 8 or wide != 4:
        out = lax.all_gather(own, ("tp", "sp"), axis=0)
        return out.reshape((wide, n) + own.shape)
    dma = pltpu.SemaphoreType.DMA
    return pl.pallas_call(
        functools.partial(rows_kernel, n),
        out_shape=jax.ShapeDtypeStruct((wide, n) + own.shape, own.dtype),
        in_specs=[VMEM],
        out_specs=VMEM,
        scratch_shapes=[
            dma((n - 1,)),
            dma((n - 1,)),
            dma((n,)),
            dma((n,)),
            dma((2 * n,)),
            dma((2 * n,)),
        ],
        compiler_params=pltpu.CompilerParams(collective_id=2, has_side_effects=True),
        cost_estimate=pl.CostEstimate(flops=0, bytes_accessed=90_000_000, transcendentals=0),
        name="gather_rows",
    )(own)


def reduce_kernel(
    n, chunks, part_ref, base_ref, out_ref, got_c, sum_c, got_x, sum_x, got_z,
    c_send, c_recv, x_send, x_recv, z_send, z_recv,
):
    tp, near, far = partners()
    low, high = lax.rem(tp, 2), tp // 2
    shifts = range(1, n)
    me = lax.axis_index("sp") if n > 1 else 0
    greet([{"tp": near}, {"tp": far}] + [{"sp": lax.rem(me + k, n)} for k in shifts])
    width = part_ref.shape[-1] // chunks
    cols = [pl.ds(i * width, width) for i in range(chunks)]
    c_copies, x_copies, z_copies = [], [], []
    for i in range(chunks):
        copy = remote(
            part_ref.at[:, 1 - low, :, :, cols[i]],
            got_c.at[i],
            c_send.at[i],
            c_recv.at[i],
            {"tp": near},
        )
        copy.start()
        c_copies.append(copy)
    for i in range(chunks):
        c_copies[i].wait_recv()
        mine = part_ref[:, low, :, :, cols[i]].astype(jnp.float32)
        sum_c[i] = (mine + got_c[i].astype(jnp.float32)).astype(sum_c.dtype)
        copy = remote(
            sum_c.at[i, 1 - high], got_x.at[i], x_send.at[i], x_recv.at[i], {"tp": far}
        )
        copy.start()
        x_copies.append(copy)
    for i in range(chunks):
        x_copies[i].wait_recv()
        both = sum_c[i, high].astype(jnp.float32) + got_x[i].astype(jnp.float32)
        sum_x[i] = both.astype(sum_x.dtype)
        for k in shifts:
            peer = lax.rem(me + k, n)
            copy = remote(
                sum_x.at[i, peer],
                got_z.at[i, k - 1],
                z_send.at[i, k - 1],
                z_recv.at[i, k - 1],
                {"sp": peer},
            )
            copy.start()
            z_copies.append(copy)
    for i in range(chunks):
        total = sum_x[i, me].astype(jnp.float32)
        for k in shifts:
            z_copies[i * (n - 1) + k - 1].wait_recv()
            total = total + got_z[i, k - 1].astype(jnp.float32)
        out_ref[:, cols[i]] = (base_ref[:, cols[i]] + total).astype(out_ref.dtype)
    for copy in c_copies + x_copies + z_copies:
        copy.wait_send()


def reduce_rows(part, base, dtype, over_sp):
    wide, n = part.shape[:2]
    if n > 8 or wide != 4 or part.size > 8_000_000:
        axes = ("tp", "sp") if over_sp else "tp"
        flat = part.reshape(-1, part.shape[-1])
        total = lax.psum_scatter(flat, axes, scatter_dimension=0, tiled=True)
        return (base + total.astype(jnp.float32)).astype(dtype)
    rows, columns = part.shape[2:]
    chunks = 4 if columns % 512 == 0 else 1
    width = columns // chunks
    dma = pltpu.SemaphoreType.DMA
    zs = max(n - 1, 1)
    return pl.pallas_call(
        functools.partial(reduce_kernel, n, chunks),
        out_shape=jax.ShapeDtypeStruct((rows, columns), dtype),
        in_specs=[VMEM, VMEM],
        out_specs=VMEM,
        scratch_shapes=[
            pltpu.VMEM((chunks, 2, n, rows, width), part.dtype),
            pltpu.VMEM((chunks, 2, n, rows, width), part.dtype),
            pltpu.VMEM((chunks, n, rows, width), part.dtype),
            pltpu.VMEM((chunks, n, rows, width), part.dtype),
            pltpu.VMEM((chunks, zs, rows, width), part.dtype),
            dma((chunks,)),
            dma((chunks,)),
            dma((chunks,)),
            dma((chunks,)),
            dma((chunks, zs)),
            dma((chunks, zs)),
        ],
        compiler_params=pltpu.CompilerParams(
            collective_id=3 if over_sp else 4, has_side_effects=True
        ),
        cost_estimate=pl.CostEstimate(flops=0, bytes_accessed=60_000_000, transcendentals=0),
        name="reduce_all" if over_sp else "reduce_tp",
    )(part.reshape(2, 2, n, rows, columns), base)


def rotate(block, positions, heads):
    columns = block.shape[-1]
    width = columns // heads
    half = width // 2
    at = jnp.arange(columns, dtype=jnp.int32)
    freqs = ROPE_BASE ** (-(at % half).astype(jnp.float32) * 2.0 / width)
    angles = positions.astype(jnp.float32)[:, None] * freqs[None, :]
    source = jnp.where(at % width < half, at + half, at - half)
    sign = jnp.where(at % width < half, -1.0, 1.0)
    turn = jnp.where(at[:, None] == source[None, :], sign[None, :], 0.0).astype(jnp.bfloat16)
    flat = block.reshape(-1, columns)
    other = jnp.dot(flat, turn, preferred_element_type=jnp.float32).reshape(block.shape)
    turned = block.astype(jnp.float32) * jnp.cos(angles) + other * jnp.sin(angles)
    return turned.astype(jnp.bfloat16)


def depthwise(current, taps, docs):
    shown = current.astype(jnp.float32)
    total = taps[2] * shown
    for back in (1, 2):
        moved = jnp.pad(shown, ((0, 0), (back, 0), (0, 0)))[:, : shown.shape[1]]
        moved_docs = jnp.pad(docs, ((0, 0), (back, 0)), constant_values=-1)[:, : docs.shape[1]]
        total = total + jnp.where((moved_docs == docs)[..., None], taps[2 - back] * moved, 0.0)
    return total


def cyclic(array, axis, by):
    length = lax.axis_size(axis)
    return lax.ppermute(array, axis, [(i, (i + by) % length) for i in range(length)])


def exchange(piece, whole):
    count = lax.axis_size("sp")
    copies = lax.axis_size("grp")
    me = lax.axis_index("sp")
    mine = lax.axis_index("grp")
    if count > 8:
        pieces = jnp.stack([whole(dest) for dest in range(count)], axis=0)
        return lax.all_to_all(pieces, "sp", 0, 0)
    parts = []
    for shift in range(1, count):
        part = piece(lax.rem(me + shift, count), mine)
        parts.append(cyclic(part, "sp", shift))
    got = [jnp.stack(parts, axis=0)]
    for turn in range(1, copies):
        got.append(cyclic(got[0], "grp", turn))
    got = jnp.stack(got, axis=1)
    held = whole(me)
    held = jnp.broadcast_to(held[None], (1,) + held.shape)
    order = [lax.rem(mine - share + copies, copies) for share in range(copies)]
    out = []
    for source in range(count):
        shift = lax.rem(me - source + count, count)
        there = lax.max(shift - 1, 0)
        shares = [
            lax.dynamic_slice(got, (there, at) + (0,) * (got.ndim - 2), (1, 1) + got.shape[2:])[0]
            for at in order
        ]
        out.append(jnp.where(shift == 0, held, jnp.concatenate(shares, axis=0)[None]))
    return jnp.concatenate(out, axis=0)


def online_step(state, queries, keys, vals, allowed, scale):
    peak, total, accum = state
    scores = (
        jnp.einsum("sqhgd,skhd->shgqk", queries, keys, preferred_element_type=jnp.float32) * scale
    )
    mask = allowed[:, None, None]
    scores = jnp.where(mask, scores, NEG_BIG)
    new_peak = jnp.maximum(peak, jnp.max(scores, axis=-1))
    expd = jnp.where(mask, jnp.exp(scores - new_peak[..., None]), 0.0)
    fade = jnp.exp(peak - new_peak)
    new_total = total * fade + jnp.sum(expd, axis=-1)
    update = jnp.einsum(
        "shgqk,skhd->shgqd", expd.astype(jnp.bfloat16), vals, preferred_element_type=jnp.float32
    )
    return (new_peak, new_total, accum * fade[..., None] + update)


HBM = pl.BlockSpec(memory_space=pltpu.HBM)
SMEM = pl.BlockSpec(memory_space=pltpu.SMEM)
LANES = 128


def rounded(array):
    return array.astype(jnp.bfloat16)


def wide(array):
    return array.astype(jnp.float32)


def dot(left, right):
    return jnp.dot(left, right, preferred_element_type=jnp.float32)


class Phases:
    def __init__(self):
        self.open = None

    def __call__(self, name):
        if self.open is not None:
            self.open.__exit__(None, None, None)
        self.open = jax.named_scope(name) if name else None
        if name:
            self.open.__enter__()


def layer_kernel(
    n, per, tiles, scale,
    q_one, q_two, k_one, k_two, vals_own, doc_ids, lam, head_gain, norm_gain,
    taps_gate, taps_value, join, cosine_hbm, sine_hbm, turn_hbm, spread_hbm, resid_hbm, out_hbm, gate_hbm, value_hbm, down_hbm,
    out,
    cosine, sine, turn, spread, resid,
    kv_all, docs_all, docs_row, out_w, heads, part_one, got_one, sum_one, got_far, mid,
    rows_all, up_w, down_w, hidden, part_two, got_two, sum_far, got_x, sum_z, own_z, got_z, got_in, held_z,
    d_send, d_recv, k_send, k_recv, o_sem, w_send, w_recv, y_send,
    c1_send, c1_recv, x1_send, x1_recv,
    az_send, az_recv, ax_send, ax_recv, ac_send, ac_recv,
    c2_recv, x2_recv, z2_recv,
):
    phase = Phases()
    z, g = lax.axis_index("sp"), lax.axis_index("grp")
    tp, near, far = partners()
    low, high = lax.rem(tp, 2), tp // 2
    diag = (1 - high) * 2 + 1 - low
    other = {"grp": 1 - g}
    spare = per * n - tiles
    seqs, rows = q_one.shape[:2]
    depth, columns = gate_hbm.shape[0], down_hbm.shape[1]
    features, total = resid.shape[1], n * rows
    loads = [
        pltpu.make_async_copy(there, here, y_send.at[z, at])
        for at, (there, here) in enumerate(
            ((cosine_hbm, cosine), (sine_hbm, sine), (turn_hbm, turn), (spread_hbm, spread), (resid_hbm, resid))
        )
    ]
    for load in loads:
        load.start()
    peers = [lax.rem(z + k, n) for k in range(1, n)]
    phase("greet")
    greet([{"sp": peer} for peer in peers] + [{"tp": near}, {"tp": far}, other])

    def rows_at(block):
        return pl.ds(pl.multiple_of(block * rows, rows), rows)

    phase("send_kv")
    def doc_copy(k, source, peer):
        part = docs_all.at[source]
        return remote(part, part, d_send.at[k], d_recv.at[source], {"sp": peer})

    def key_copy(block, p):
        half = seqs // 2
        part = kv_all.at[p * half : (p + 1) * half, rows_at(block)]
        peer = lax.rem(z + 1, n)
        return remote(part, part, k_send.at[block, p], k_recv.at[block, p], {"sp": peer})

    for seq in range(seqs):
        paired = dot(k_one[seq], join[0]) + dot(k_two[seq], join[1])
        kv_all[seq, rows_at(z), :LANES] = rounded(paired)
        kv_all[seq, rows_at(z), LANES:] = vals_own[seq]

    @pl.when(z < n - 1)
    def _():
        for p in (0, 1):
            key_copy(z, p).start()

    slot = lax.broadcasted_iota(jnp.int32, (rows, total), 1)
    spot = lax.broadcasted_iota(jnp.int32, (rows, total), 0) + z * rows
    place = jnp.where(slot == spot, 1.0, 0.0).astype(jnp.bfloat16)
    padded = jnp.concatenate([wide(doc_ids[...]), jnp.zeros((8 - seqs, rows), jnp.float32)], axis=0)
    docs_all[z] = dot(rounded(padded), place)
    for k, peer in enumerate(peers):
        doc_copy(k, z, peer).start()

    out_copy = pltpu.make_async_copy(out_hbm, out_w, o_sem)
    out_copy.start()

    def tile_of(block, k):
        return per * block + k - low * spare

    def valid(block, k):
        tile = tile_of(block, k)
        return (tile >= 0) & (tile < tiles)

    def weight_from(m, tile):
        at = pl.ds(pl.multiple_of(jnp.clip(tile, 0, tiles - 1) * LANES, LANES), LANES)
        if m >= 2:
            first = jnp.clip(tile, 0, tiles - 1) * LANES + (m - 2) * (LANES // 2)
            half = pl.ds(pl.multiple_of(first, LANES // 2), LANES // 2)
            return down_hbm.at[half, :]
        return (gate_hbm, value_hbm)[m].at[:, at]

    def weight_to(m, source, k):
        if m >= 2:
            across = pl.ds(pl.multiple_of(source * columns, columns), columns)
            return down_w.at[pl.ds(k * LANES + (m - 2) * (LANES // 2), LANES // 2), across]
        along = pl.ds(pl.multiple_of(source * depth, depth), depth)
        return up_w.at[along, pl.ds((2 * k + m) * LANES, LANES)]

    def over_z(m, k, source, dest):
        return lax.rem(k + m + source + dest, 2) == g

    def z_copy(m, k, peer):
        return remote(
            weight_from(m, tile_of(peer, k)), weight_to(m, z, k),
            w_send.at[peer, (4 * k + m) // 2], w_recv.at[z, 4 * k + m], {"sp": peer},
        )

    def y_copy(m, k, source):
        block = weight_to(m, source, k)
        at = 4 * k + m
        return remote(block, block, y_send.at[source, at // 2], w_recv.at[source, at], other)

    def own_copy(m, k):
        return pltpu.make_async_copy(
            weight_from(m, tile_of(z, k)), weight_to(m, z, k), w_recv.at[z, 4 * k + m]
        )

    def at_distance(d):
        return ((lax.rem(z - d + n, n), z - d >= 0), (lax.rem(z + d, n), z + d < n))

    def when_sent(d, items, act, ways=(0, 1)):
        for way in ways:
            peer, there = at_distance(d)[way]
            for k, m in items:

                @pl.when(there & valid(peer, k) & over_z(m, k, z, peer))
                def _():
                    act(z_copy(m, k, peer))

    def when_hopped(d, items, act, sides=(0, 1)):
        for k, m in items:
            for source, there in [at_distance(d)[side] for side in sides]:

                @pl.when(there & valid(z, k) & over_z(m, k, source, z))
                def _():
                    act(y_copy(m, k, source))

    def send(d, items, ways=(0, 1)):
        when_sent(d, items, lambda copy: copy.start(), ways)

    def relay(d, items, sides=(0, 1)):
        def act(copy):
            copy.wait_recv()
            copy.start()

        when_hopped(d, items, act, sides)

    ups = [(k, m) for k in range(per) for m in (0, 1)]
    downs = [(k, m) for k in range(per) for m in (2, 3)]
    early, middle, late = ups[: 2 * per - 2], ups[2 * per - 2 : 2 * per - 1], ups[2 * per - 1 :]

    def settle(m, k):
        for source in peers:

            @pl.when(valid(z, k) & jnp.logical_not(over_z(m, k, source, z)))
            def _():
                y_copy(m, k, source).wait_recv()

        @pl.when(valid(z, k))
        def _():
            own_copy(m, k).wait()

    phase("send_up")
    for d in range(1, n):
        send(d, early + middle, (0,))
    for step in range(1, n):
        block = z - step

        @pl.when(block >= 0)
        def _():
            for p in (0, 1):
                key_copy(block, p).wait_recv()

                @pl.when(z < n - 1)
                def _():
                    key_copy(block, p).start()

    for d in range(1, n):
        send(d, early, (1,))
    for k in range(per):

        @pl.when(valid(z, k))
        def _():
            for m in range(4):
                own_copy(m, k).start()

        @pl.when(jnp.logical_not(valid(z, k)))
        def _():
            pair = pl.ds(2 * k * LANES, 2 * LANES)
            up_w[:, pair] = jnp.zeros((up_w.shape[0], 2 * LANES), up_w.dtype)
            one = pl.ds(k * LANES, LANES)
            down_w[one, :] = jnp.zeros((LANES, down_w.shape[1]), down_w.dtype)

    for block in range(1, n):

        @pl.when(block > z)
        def _():
            blank = jnp.zeros((kv_all.shape[0], rows, kv_all.shape[2]), kv_all.dtype)
            kv_all[:, pl.ds(block * rows, rows)] = blank

    phase("wait_kv")
    for k, source in enumerate(peers):
        doc_copy(k, source, source).wait_recv()
    all_docs = functools.reduce(lambda a, b: a + b, [docs_all[i] for i in range(n)])
    for seq in range(seqs):
        docs_row[seq] = jnp.broadcast_to(all_docs[seq : seq + 1], (8, total))
    gain = jnp.concatenate([head_gain[...], head_gain[...]], axis=1)

    def iota(height, width, axis):
        return lax.broadcasted_iota(jnp.int32, (height, width), axis)

    def attend(seq, carry):
        doc_row = docs_row[seq][0:1]
        at_query = iota(rows, total, 0) + z * rows
        at_key = iota(rows, total, 1)
        doc_query = jnp.sum(jnp.where(at_key == at_query, doc_row, 0.0), axis=1, keepdims=True)
        allowed = (at_key <= at_query) & (doc_row == doc_query)
        bias = jnp.where(allowed, 0.0, NEG_BIG)
        bias = jnp.concatenate([bias] * 4, axis=0)
        q_cos, q_sin = cosine[rows_at(z)], sine[rows_at(z)]
        packed = kv_all[seq]
        spun = dot(packed[:, :LANES], spread[...])
        vals = wide(packed[:, LANES:])
        swapped = pltpu.roll(vals, LANES // 2, 1)
        lane = iota(total, LANES, 1)
        queries, keys = [], []
        width = cosine.shape[1]
        for index, source in enumerate((q_one, q_two)):
            block = source[seq]
            turned = wide(block) * q_cos + dot(block, turn[...]) * q_sin
            queries.append(rounded(turned))
            start = 2 * index * width
            straight = spun[:, start : start + width]
            crossed = spun[:, start + width : start + 2 * width]
            keys.append(rounded(straight * cosine[...] + crossed * sine[...]))
        q_lane = iota(rows, LANES, 1) // (LANES // 4)
        row4 = iota(4 * rows, 1, 0) // rows
        half_lane = iota(2 * rows, LANES, 1) < LANES // 2
        for c in range(2):
            across = slice(c * LANES, (c + 1) * LANES)
            pair = (vals, swapped) if c == 0 else (swapped, vals)
            both = rounded(jnp.where(lane < LANES // 2, pair[0], pair[1]))
            found = []
            for query, key in zip(queries, keys):
                local = wide(query[:, across])
                stack = jnp.concatenate(
                    [rounded(jnp.where(q_lane == j, local, 0.0)) for j in (0, 2, 1, 3)], axis=0
                )
                scores = lax.dot_general(
                    stack, key[:, across], (((1,), (1,)), ((), ())),
                    preferred_element_type=jnp.float32,
                )
                scores = scores * scale + bias
                expd = jnp.exp(scores - jnp.max(scores, axis=1, keepdims=True))
                summed = jnp.sum(expd, axis=1, keepdims=True)
                found.append(dot(rounded(expd), both) / summed)
            weights = jnp.where(
                row4 == 0, lam[4 * c],
                jnp.where(
                    row4 == 1, lam[4 * c + 2],
                    jnp.where(row4 == 2, lam[4 * c + 1], lam[4 * c + 3]),
                ),
            )
            mixed = found[0] - weights * found[1]
            meansq = jnp.sum(mixed * mixed, axis=1, keepdims=True) * (1.0 / LANES)
            normed = mixed * lax.rsqrt(meansq + NORM_EPS) * gain
            merged = rounded(jnp.where(half_lane, normed[: 2 * rows], normed[2 * rows :]))
            base = 2 * c * LANES
            heads[seq, :, base : base + LANES] = merged[:rows]
            heads[seq, :, base + LANES : base + 2 * LANES] = merged[rows:]
        return carry

    for load in loads:
        load.wait()
    phase("attend")
    lax.fori_loop(0, seqs, attend, 0)

    phase("proj")
    out_copy.wait()
    halves = got_one.shape[0]
    width = features // halves

    def c1_copy(i):
        cols = pl.ds(i * width, width)
        return remote(
            part_one.at[:, 1 - low, :, cols], got_one.at[i], c1_send.at[i], c1_recv.at[i], {"tp": near}
        )

    def x1_copy(i):
        return remote(sum_one.at[i], got_far.at[i], x1_send.at[i], x1_recv.at[i], {"tp": far})

    flat = heads[...].reshape(4 * rows, heads.shape[2])
    for i in range(halves):
        cols = pl.ds(i * width, width)
        made = rounded(dot(flat, out_w[:, cols]))
        part_one[:, :, :, cols] = made.reshape(2, 2, rows, width)
        c1_copy(i).start()
    phase("wait_c1")
    for i in range(halves):
        cols = pl.ds(i * width, width)
        c1_copy(i).wait_recv()
        sum_one[i] = rounded(wide(part_one[1 - high, low, :, cols]) + wide(got_one[i, 1 - high]))
        x1_copy(i).start()
        kept = wide(part_one[high, low, :, cols]) + wide(got_one[i, high])
        mid[:, cols] = wide(resid[:, cols]) + kept
    phase("relay_u1")
    relay(1, early)
    phase("wait_x1")
    for i in range(halves):
        cols = pl.ds(i * width, width)
        x1_copy(i).wait_recv()
        mid[:, cols] = mid[:, cols] + wide(got_far[i])
    phase("norm")
    held = mid[...]
    meansq = jnp.mean(held * held, axis=1, keepdims=True)
    rows_all[tp, rows_at(z)] = rounded(held * lax.rsqrt(meansq + NORM_EPS) * norm_gain[...])

    cuts = 2
    part_rows = rows // cuts

    def piece_of(owner, block, p):
        first = pl.multiple_of(block * rows + p * part_rows, part_rows)
        return rows_all.at[owner, pl.ds(first, part_rows)]

    def x_copy(owner, block, p):
        part = piece_of(owner, block, p)
        return remote(part, part, ax_send.at[block, p], ax_recv.at[block, p], {"tp": far})

    def c_copy(owner, hop, block):
        part = rows_all.at[owner, rows_at(block)]
        sems = (ac_send.at[hop, block], ac_recv.at[hop, block])
        return remote(part, part, *sems, {"tp": near})

    def chain_copy(way, block, p):
        part = piece_of(tp, block, p)
        peer = lax.rem(z + (1 if way == 0 else n - 1), n)
        return remote(part, part, az_send.at[way, block, p], az_recv.at[block, p], {"sp": peer})

    def pass_on(block, p):
        @pl.when((z >= block) & (z < n - 1))
        def _():
            chain_copy(0, block, p).start()

        @pl.when((z <= block) & (z > 0))
        def _():
            chain_copy(1, block, p).start()

        x_copy(tp, block, p).start()
        if p == cuts - 1:
            c_copy(tp, 0, block).start()

    def chain(step):
        for p in range(cuts):
            for block in (z - step, z + step):

                @pl.when((block >= 0) & (block < n))
                def _():
                    chain_copy(0, block, p).wait_recv()
                    pass_on(block, p)

    phase("ag_start")
    for p in range(cuts):
        pass_on(z, p)

    phase("relay_u2")
    for d in range(2, n):
        relay(d, early)
    for d in range(1, n):
        relay(d, middle, (1,))
    for step in range(1, n):
        phase(f"ag_z{step}")
        chain(step)
        ends = (z == 0) | (z == n - 1)
        for at, items in ((2, (late, middle + late)), (2, (downs, downs))):

            @pl.when((ends & (step == at)) | (jnp.logical_not(ends) & (step == 1)))
            def _():
                for d in range(1, n):
                    for way in (0, 1):
                        send(d, items[way], (way,))

    phase("relay_u3")
    for d in range(1, n):
        relay(d, middle, (0,))
        relay(d, late)
    phase("relay_d3")
    relay(1, downs)
    relay(2, downs)
    phase("settle_up")
    for k, m in ups:
        settle(m, k)

    def cross():
        for step in range(n):
            for p in range(cuts):
                for block in (z - step, z + step) if step else (z,):

                    @pl.when((block >= 0) & (block < n))
                    def _():
                        x_copy(far, block, p).wait_recv()
                        if p == cuts - 1:
                            c_copy(far, 1, block).start()

    def lift(i, carry):
        seq = lax.rem(high + i // 2, 2) * 2 + lax.rem(low + i, 2)
        for turn_at, (owner, hop) in ((1, (near, 0)), (3, (diag, 1))):

            @pl.when(i == turn_at)
            def _():
                for block in range(n):
                    c_copy(owner, hop, block).wait_recv()

        @pl.when(i == 0)
        def _():
            for d in range(3, n):
                relay(d, downs)

        @pl.when(i == 2)
        def _():
            cross()

        doc_row = docs_row[seq][0:1]
        at_row, at_col = iota(total, total, 0), iota(total, total, 1)
        doc_col = jnp.sum(jnp.where(at_row == at_col, doc_row, 0.0), axis=1, keepdims=True)
        same = jnp.where(doc_row == doc_col, 1.0, 0.0)
        back_one, back_two = [
            jnp.sum(jnp.where(at_col == at_row - back, same, 0.0), axis=1, keepdims=True)
            for back in (1, 2)
        ]

        def depthwise_of(current, taps):
            shown = wide(rounded(current))
            return (
                taps[2:3] * shown
                + taps[1:2] * (pltpu.roll(shown, 1, 0) * back_one)
                + taps[0:1] * (pltpu.roll(shown, 2, 0) * back_two)
            )

        for k in range(per):
            made = dot(rows_all[seq], up_w[:, 2 * k * LANES : (2 * k + 2) * LANES])
            tile = jnp.clip(tile_of(z, k), 0, tiles - 1)
            at = pl.ds(pl.multiple_of(tile * LANES, LANES), LANES)
            conv_g = depthwise_of(made[:, :LANES], taps_gate[:, at])
            conv_v = depthwise_of(made[:, LANES:], taps_value[:, at])
            unit = conv_g / (1.0 + jnp.exp(-conv_g)) * conv_v
            hidden[seq, :, k * LANES : (k + 1) * LANES] = rounded(unit)
        return carry

    phase("lift")
    lax.fori_loop(0, rows_all.shape[0], lift, 0)
    phase("settle_d")
    for k, m in downs:
        settle(m, k)

    def c2_copy(i, seq, block):
        there = rows_at(block)
        sems = (ac_send.at[i, block], c2_recv.at[i, block])
        return remote(part_two.at[seq, there], got_two.at[i, there], *sems, {"tp": near})

    chunk = 512 if features % 512 == 0 else features
    upper = z // (n // 2)
    mate = n // 2 - 1 - z + upper * n
    gate = (z == n // 2 - 1) | (z == n // 2)
    across = [upper * j + (1 - upper) * (n - 1 - j) for j in range(n // 2)]
    order = across + [mate, z]
    stops = [(j, p) for j in range(len(order)) for p in range(cuts)]

    def slot(p):
        return pl.ds(p * part_rows, part_rows)

    def piece_rows(block, p):
        return pl.ds(pl.multiple_of(block * rows + p * part_rows, part_rows), part_rows)

    def x2_copy(block, p):
        sems = (ax_send.at[block, p], x2_recv.at[block, p])
        return remote(sum_far.at[block, slot(p)], got_x.at[block, slot(p)], *sems, {"tp": far})

    def mate_copy(p):
        sems = (k_send.at[2, p], z2_recv.at[2, p])
        return remote(sum_z.at[2, slot(p)], got_z.at[0, slot(p)], *sems, {"sp": mate})

    def inner_copy(j, p):
        sems = (k_send.at[j, p], z2_recv.at[j, p])
        return remote(sum_z.at[j, slot(p)], got_in.at[j, slot(p)], *sems, {"sp": mate})

    def outer_copy(j, p):
        sems = (k_send.at[j, p], z2_recv.at[3, p])
        return remote(sum_z.at[j, slot(p)], got_z.at[1, slot(p)], *sems, {"sp": across[j]})

    def combine(j, p):
        @pl.when(gate)
        def _():
            inner_copy(j, p).wait_recv()
            sum_z[j, slot(p)] = rounded(held_z[j, slot(p)] + wide(got_in[j, slot(p)]))
            outer_copy(j, p).start()

    def lower(i, carry):
        seq = lax.rem(high + 1 - i // 2, 2) * 2 + lax.rem(low + 1 - lax.rem(i, 2), 2)
        for c in range(features // chunk):
            cols = slice(c * chunk, (c + 1) * chunk)
            part_two[seq, :, cols] = rounded(dot(hidden[seq], down_w[:, cols]))

        @pl.when(lax.rem(i, 2) == 0)
        def _():
            for block in order:
                c2_copy(i // 2, seq, block).start()

        @pl.when(i == 1)
        def _():
            for block in order:
                c2_copy(0, diag, block).wait_recv()
                for p in range(cuts):
                    there = piece_rows(block, p)
                    both = wide(part_two[far, there]) + wide(got_two[0, there])
                    sum_far[block, slot(p)] = rounded(both)
                    x2_copy(block, p).start()

        return carry

    for block in range(n):

        @pl.when((z >= block) & (z < n - 1))
        def _():
            for p in (0, 1):
                key_copy(block, p).wait_send()

        for p in range(cuts):
            x_copy(tp, block, p).wait_send()
        c_copy(tp, 0, block).wait_send()
        c_copy(far, 1, block).wait_send()
    phase("lower")
    lax.fori_loop(0, rows_all.shape[0], lower, 0)
    phase("x2")
    lag = 2
    for t, (j, p) in enumerate(stops):
        block = order[j]
        if p == 0:
            c2_copy(1, near, block).wait_recv()
        there = piece_rows(block, p)
        x2_copy(block, p).wait_recv()
        both = wide(part_two[tp, there]) + wide(got_two[1, there]) + wide(got_x[block, slot(p)])
        if j < len(across):

            @pl.when(gate)
            def _():
                held_z[j, slot(p)] = both

            @pl.when(jnp.logical_not(gate))
            def _():
                sum_z[j, slot(p)] = rounded(both)
                inner_copy(j, p).start()

        elif j == len(across):
            sum_z[j, slot(p)] = rounded(both)
            mate_copy(p).start()
        else:
            own_z[slot(p)] = mid[slot(p)] + both
        if t >= lag and stops[t - lag][0] < len(across):
            combine(*stops[t - lag])
    phase("z2")
    for p in range(cuts):
        mate_copy(p).wait_recv()
        outer_copy(0, p).wait_recv()
        answer = own_z[slot(p)] + wide(got_z[0, slot(p)]) + wide(got_z[1, slot(p)])
        out[slot(p)] = answer.astype(out.dtype)

    phase("drain")
    for k, peer in enumerate(peers):
        doc_copy(k, z, peer).wait_send()
    for p in range(cuts):
        mate_copy(p).wait_send()
        for j in range(len(across)):
            inner_copy(j, p).wait_send()
    for d in range(1, n):
        when_sent(d, ups + downs, lambda copy: copy.wait_send())
        when_hopped(d, ups + downs, lambda copy: copy.wait_send())
    for i in range(halves):
        c1_copy(i).wait_send()
        x1_copy(i).wait_send()
    for block in range(n):

        @pl.when((z >= block) & (z < n - 1))
        def _():
            for p in range(cuts):
                chain_copy(0, block, p).wait_send()

        @pl.when((z <= block) & (z > 0))
        def _():
            for p in range(cuts):
                chain_copy(1, block, p).wait_send()

        for p in range(cuts):
            x2_copy(block, p).wait_send()
        c2_copy(0, diag, block).wait_send()
        c2_copy(1, near, block).wait_send()
    phase(None)


def rope_tables(total, width, copies):
    half = width // 2
    freqs = np.float32(ROPE_BASE) ** (-np.arange(half, dtype=np.float32) * np.float32(2.0) / np.float32(width))
    angles = np.arange(total, dtype=np.float32)[:, None] * freqs.astype(np.float32)[None, :]
    tile = lambda table: np.tile(table.astype(np.float32), (1, 2 * copies))
    return tile(np.cos(angles)), tile(np.sin(angles))


def turn_matrix(width):
    half = width // 2
    at = np.arange(width)
    source = np.where(at < half, at + half, at - half)
    sign = np.where(at < half, -1.0, 1.0)
    return np.where(at[:, None] == source[None, :], sign[None, :], 0.0)


def spread_matrix(width, group, kv_local):
    straight = np.kron(np.eye(kv_local), np.tile(np.eye(width), (1, group)))
    crossed = np.kron(np.eye(kv_local), np.tile(turn_matrix(width), (1, group)))
    both = np.concatenate([straight, crossed], axis=1)
    return np.kron(np.eye(2), both)


def kernel_fits(resid_in, query_one, key_one, value, lam, gate_weight):
    heads = lam.shape[0]
    width = query_one.shape[2] // heads
    kv_local = key_one.shape[2] // width
    group = heads // kv_local
    seqs, rows = query_one.shape[:2]
    return (
        lax.axis_size("tp") == 4
        and lax.axis_size("grp") == 2
        and lax.axis_size("sp") == 4
        and kv_local == 2
        and group == 4
        and group * width == LANES
        and value.shape[2] == LANES
        and seqs == 4
        and resid_in.shape[0] == 1
        and rows % 16 == 0
        and rows * lax.axis_size("sp") <= 256
        and gate_weight.shape[0] <= 512
        and gate_weight.shape[1] % LANES == 0
        and gate_weight.shape[1] <= 1536
        and resid_in.shape[2] <= 2048
    )


def whole_layer(
    resid_in, query_one, key_one, query_two, key_two, value, lam, head_gain, doc_ids,
    out_weight, norm_gain, gate_weight, value_weight, conv_gate, conv_value, down_weight,
):
    n = lax.axis_size("sp")
    seqs, rows = query_one.shape[:2]
    heads = lam.shape[0]
    width = query_one.shape[2] // heads
    kv_local = key_one.shape[2] // width
    group = heads // kv_local
    features, total = resid_in.shape[2], n * rows
    depth, columns = gate_weight.shape[0], down_weight.shape[1]
    tiles = gate_weight.shape[1] // LANES
    per = -(-tiles // n)
    cosine, sine = rope_tables(total, width, heads)
    turn = np.kron(np.eye(heads), turn_matrix(width))
    spread = spread_matrix(width, group, kv_local)
    key_width = kv_local * width
    join = np.stack([np.eye(key_width, LANES), np.eye(key_width, LANES, LANES - key_width)])
    halves = 2
    bf16, f32 = jnp.bfloat16, jnp.float32
    dma = pltpu.SemaphoreType.DMA
    vmem = pltpu.VMEM
    scratch = [
        vmem(cosine.shape, f32),
        vmem(sine.shape, f32),
        vmem(turn.shape, bf16),
        vmem(spread.shape, bf16),
        vmem((rows, features), bf16),
        vmem((seqs, total, 2 * LANES), bf16),
        vmem((n, 8, total), f32),
        vmem((seqs, 8, total), f32),
        vmem(out_weight.shape, bf16),
        vmem((seqs, rows, out_weight.shape[0]), bf16),
        vmem((2, 2, rows, features), bf16),
        vmem((halves, 2, rows, features // halves), bf16),
        vmem((halves, rows, features // halves), bf16),
        vmem((halves, rows, features // halves), bf16),
        vmem((rows, features), f32),
        vmem((seqs, total, features), bf16),
        vmem((n * depth, 2 * per * LANES), bf16),
        vmem((per * LANES, n * columns), bf16),
        vmem((seqs, total, per * LANES), bf16),
        vmem((seqs, total, features), bf16),
        vmem((2, total, features), bf16),
        vmem((n, rows, features), bf16),
        vmem((n, rows, features), bf16),
        vmem((n - 1, rows, features), bf16),
        vmem((rows, features), f32),
        vmem((2, rows, features), bf16),
        vmem((2, rows, features), bf16),
        vmem((2, rows, features), f32),
        dma((n,)), dma((n,)), dma((n, 2)), dma((n, 2)), dma,
        dma((n, 2 * per)), dma((n, 4 * per)), dma((n, 2 * per)),
        dma((halves,)), dma((halves,)), dma((halves,)), dma((halves,)),
        dma((2, n, 2)), dma((n, 2)), dma((n, 2)), dma((n, 2)), dma((2, n)), dma((2, n)),
        dma((2, n)), dma((n, 2)), dma((n, 2)),
    ]
    out = pl.pallas_call(
        functools.partial(layer_kernel, n, per, tiles, width ** (-0.5)),
        out_shape=jax.ShapeDtypeStruct((rows, features), resid_in.dtype),
        in_specs=[VMEM] * 6 + [SMEM] + [VMEM] * 5 + [HBM] * 9,
        out_specs=VMEM,
        scratch_shapes=scratch,
        compiler_params=pltpu.CompilerParams(
            collective_id=5, has_side_effects=True, vmem_limit_bytes=60 * 2**20
        ),
        name="whole_layer",
    )(
        query_one, query_two, key_one, key_two, value,
        doc_ids, lam, head_gain[None], norm_gain[None], conv_gate, conv_value,
        jnp.asarray(join, bf16), jnp.asarray(cosine), jnp.asarray(sine), jnp.asarray(turn, bf16),
        jnp.asarray(spread, bf16), resid_in.reshape(rows, features),
        out_weight, gate_weight, value_weight, down_weight,
    )
    return out.reshape(resid_in.shape)


def per_device_apart(
    resid_in,
    query_one,
    key_one,
    query_two,
    key_two,
    value,
    lam,
    head_gain,
    doc_ids,
    out_weight,
    norm_gain,
    gate_weight,
    value_weight,
    conv_gate,
    conv_value,
    down_weight,
):
    n_sp = lax.axis_size("sp")
    me = lax.axis_index("sp")
    depth, width = gate_weight.shape
    share = width // n_sp
    copies = lax.axis_size("grp")

    def cut(weight, row, column, size):
        return lax.dynamic_slice(weight, (row, column), size)

    def up_piece(dest, part):
        size = (depth // copies, share)
        row, column = part * size[0], dest * share
        return jnp.stack([cut(gate_weight, row, column, size), cut(value_weight, row, column, size)])

    def up_whole(dest):
        return jnp.stack([up_piece(dest, part) for part in range(copies)])

    def down_piece(dest, part):
        size = (share // copies, down_weight.shape[1])
        return cut(down_weight, dest * share + part * size[0], 0, size)

    def down_whole(dest):
        return jnp.stack([down_piece(dest, part) for part in range(copies)])

    up_all = exchange(up_piece, up_whole)
    down_all = exchange(down_piece, down_whole)
    gate_all = up_all[:, :, 0].reshape(-1, share)
    value_all = up_all[:, :, 1].reshape(-1, share)
    down_full = jnp.transpose(down_all, (1, 2, 0, 3)).reshape(share, -1)
    seqs = query_one.shape[0]
    rows = query_one.shape[1]
    heads = lam.shape[0]
    key_width = query_one.shape[2] // heads
    kv_local = key_one.shape[2] // key_width
    group = heads // kv_local
    head_width = value.shape[2] // kv_local
    scale = key_width ** (-0.5)
    positions = lax.axis_index("sp") * rows + jnp.arange(rows, dtype=jnp.int32)
    q_first = rotate(query_one, positions, heads).reshape(seqs, rows, kv_local, group, key_width)
    q_second = rotate(query_two, positions, heads).reshape(seqs, rows, kv_local, group, key_width)
    k_first = rotate(key_one, positions, kv_local).reshape(seqs, rows, kv_local * key_width)
    k_second = rotate(key_two, positions, kv_local).reshape(seqs, rows, kv_local * key_width)
    start_state = (
        jnp.full((seqs, kv_local, group, rows), NEG_BIG, jnp.float32),
        jnp.zeros((seqs, kv_local, group, rows), jnp.float32),
        jnp.zeros((seqs, kv_local, group, rows, head_width), jnp.float32),
    )
    packed = jnp.concatenate(
        [k_first, k_second, value, doc_ids.astype(jnp.bfloat16)[..., None]], axis=-1
    )
    packed = gather_sp(packed)
    key_cols = k_first.shape[2]
    keys_one = packed[..., :key_cols]
    keys_two = packed[..., key_cols : 2 * key_cols]
    vals = packed[..., 2 * key_cols : -1]
    docs = packed[..., -1].astype(jnp.int32)
    count = keys_one.shape[1]
    step_len = math.gcd(count, 512)

    def inner(state, index):
        offset = index * step_len
        ka = lax.dynamic_slice_in_dim(keys_one, offset, step_len, 1).reshape(
            seqs, step_len, kv_local, key_width
        )
        kb = lax.dynamic_slice_in_dim(keys_two, offset, step_len, 1).reshape(
            seqs, step_len, kv_local, key_width
        )
        va = lax.dynamic_slice_in_dim(vals, offset, step_len, 1).reshape(
            seqs, step_len, kv_local, head_width
        )
        dpiece = lax.dynamic_slice_in_dim(docs, offset, step_len, 1)
        key_pos = offset + jnp.arange(step_len, dtype=jnp.int32)
        allowed = (key_pos[None, None, :] <= positions[None, :, None]) & (
            dpiece[:, None, :] == doc_ids[:, :, None]
        )
        first = online_step(state[0], q_first, ka, va, allowed, scale)
        second = online_step(state[1], q_second, kb, va, allowed, scale)
        return ((first, second), None)

    def run(state):
        return lax.scan(inner, state, jnp.arange(count // step_len))[0]

    first, second = lax.cond(
        jnp.int32(0) <= positions[rows - 1], run, lambda state: state, (start_state, start_state)
    )
    weights = lam.reshape(kv_local, group)[None, :, :, None, None]
    mixed = first[2] / first[1][..., None] - weights * (second[2] / second[1][..., None])
    meansq = jnp.mean(mixed * mixed, axis=-1, keepdims=True)
    normed_heads = mixed * lax.rsqrt(meansq + NORM_EPS) * head_gain
    heads_out = jnp.transpose(normed_heads, (0, 3, 1, 2, 4)).reshape(
        seqs * rows, heads * head_width
    )
    heads_out = heads_out.astype(jnp.bfloat16)
    own = resid_in.shape[0]
    features = resid_in.shape[2]
    proj = jnp.dot(heads_out, out_weight, preferred_element_type=jnp.float32).astype(jnp.bfloat16)
    mid = reduce_rows(
        proj.reshape(-1, 1, own * rows, features),
        resid_in.astype(jnp.float32).reshape(own * rows, features),
        jnp.float32,
        False,
    )
    meansq_mid = jnp.mean(mid * mid, axis=-1, keepdims=True)
    normed = (mid * lax.rsqrt(meansq_mid + NORM_EPS) * norm_gain).astype(jnp.bfloat16)
    gathered = gather_rows(normed).reshape(-1, n_sp, own, rows, features)
    full_rows = jnp.transpose(gathered, (0, 2, 1, 3, 4)).reshape(-1, features)
    total_rows = n_sp * rows
    start = me * share
    taps_gate = lax.dynamic_slice_in_dim(conv_gate, start, share, 1)
    taps_value = lax.dynamic_slice_in_dim(conv_value, start, share, 1)
    up_gate = jnp.dot(full_rows, gate_all, preferred_element_type=jnp.float32)
    up_value = jnp.dot(full_rows, value_all, preferred_element_type=jnp.float32)
    up_gate = up_gate.astype(jnp.bfloat16).reshape(seqs, total_rows, share)
    up_value = up_value.astype(jnp.bfloat16).reshape(seqs, total_rows, share)
    conv_g = depthwise(up_gate, taps_gate, docs)
    conv_v = depthwise(up_value, taps_value, docs)
    hidden = (jax.nn.silu(conv_g) * conv_v).astype(jnp.bfloat16)
    hidden = hidden.reshape(-1, own, n_sp, rows, share)
    hidden = jnp.transpose(hidden, (0, 2, 1, 3, 4)).reshape(-1, share)
    partial_down = jnp.dot(hidden, down_full, preferred_element_type=jnp.float32)
    partial_down = partial_down.astype(jnp.bfloat16).reshape(-1, n_sp, own * rows, features)
    return reduce_rows(partial_down, mid, jnp.bfloat16, True).reshape(resid_in.shape)


def per_device(*args):
    resid_in, query_one, key_one, value, lam, gate_weight = [args[i] for i in (0, 1, 2, 5, 6, 11)]
    if kernel_fits(resid_in, query_one, key_one, value, lam, gate_weight):
        return whole_layer(*args)
    return per_device_apart(*args)


def solution(mesh):
    placed = (
        P(("grp", "tp"), "sp", None),
        P("grp", "sp", "tp"),
        P("grp", "sp", "tp"),
        P("grp", "sp", "tp"),
        P("grp", "sp", "tp"),
        P("grp", "sp", "tp"),
        P("tp"),
        P(),
        P("grp", "sp"),
        P("tp", None),
        P(),
        P("sp", "tp"),
        P("sp", "tp"),
        P(None, "tp"),
        P(None, "tp"),
        P("tp", "sp"),
    )
    return jax.shard_map(
        per_device,
        mesh=mesh,
        in_specs=placed,
        out_specs=P(("grp", "tp"), "sp", None),
        check_vma=False,
    )
```

```python
import functools
import math

import jax
import jax.numpy as jnp
import numpy as np
from jax import lax
from jax.experimental import pallas as pl
from jax.experimental.pallas import tpu as pltpu
from jax.sharding import PartitionSpec as P

NEG_BIG = -1e30
NORM_EPS = 1e-06
ROPE_BASE = 500000.0


MESH = pl.DeviceIdType.MESH
VMEM = pl.BlockSpec(memory_space=pltpu.VMEM)


def greet(devices):
    barrier = pltpu.get_barrier_semaphore()
    for device in devices:
        pl.semaphore_signal(barrier, inc=1, device_id=device, device_id_type=MESH)
    pl.semaphore_wait(barrier, len(devices))


def remote(src, dst, send_sem, recv_sem, device):
    return pltpu.make_async_remote_copy(
        src_ref=src,
        dst_ref=dst,
        send_sem=send_sem,
        recv_sem=recv_sem,
        device_id=device,
        device_id_type=MESH,
    )


def partners():
    at = lax.axis_index("tp")
    return at, at + 1 - 2 * lax.rem(at, 2), lax.rem(at + 2, 4)


def spread_kernel(n, own_ref, out_ref, send_sem, recv_sem):
    me = lax.axis_index("sp")
    peers = [lax.rem(me + shift, n) for shift in range(1, n)]
    greet([{"sp": peer} for peer in peers])
    copies = []
    for k, peer in enumerate(peers):
        copy = remote(
            own_ref, out_ref.at[:, me], send_sem.at[k], recv_sem.at[k], {"sp": peer}
        )
        copy.start()
        copies.append(copy)
    out_ref[:, me] = own_ref[...]
    for copy in copies:
        copy.wait_recv()
    for copy in copies:
        copy.wait_send()


def gather_sp(own):
    n = lax.axis_size("sp")
    if n > 8:
        return lax.all_gather(own, "sp", axis=1, tiled=True)
    outer, rows, width = own.shape
    out = pl.pallas_call(
        functools.partial(spread_kernel, n),
        out_shape=jax.ShapeDtypeStruct((outer, n, rows, width), own.dtype),
        in_specs=[VMEM],
        out_specs=VMEM,
        scratch_shapes=[pltpu.SemaphoreType.DMA((n - 1,)), pltpu.SemaphoreType.DMA((n - 1,))],
        compiler_params=pltpu.CompilerParams(collective_id=1, has_side_effects=True),
        cost_estimate=pl.CostEstimate(flops=0, bytes_accessed=30_000_000, transcendentals=0),
        name="gather_sp",
    )(own)
    return out.reshape(outer, n * rows, width)


def rows_kernel(n, own_ref, out_ref, z_send, z_recv, x_send, x_recv, c_send, c_recv):
    me = lax.axis_index("sp")
    tp, near, far = partners()
    greet([{"tp": near}, {"tp": far}] + [{"sp": lax.rem(me + k, n)} for k in range(1, n)])
    sources = [lax.rem(me - k + n, n) for k in range(n)]
    z_copies = []
    for k in range(1, n):
        copy = remote(
            own_ref,
            out_ref.at[tp, me],
            z_send.at[k - 1],
            z_recv.at[k - 1],
            {"sp": lax.rem(me + k, n)},
        )
        z_copies.append(copy)

    def along(owner, k, send, recv, device):
        block = out_ref.at[owner, sources[k]]
        return remote(block, block, send, recv, device)

    x_copies = [remote(own_ref, out_ref.at[tp, me], x_send.at[0], x_recv.at[0], {"tp": far})]
    c_copies = [remote(own_ref, out_ref.at[tp, me], c_send.at[0], c_recv.at[0], {"tp": near})]
    for k in range(1, n):
        x_copies.append(along(tp, k, x_send.at[k], x_recv.at[k], {"tp": far}))
        c_copies.append(along(tp, k, c_send.at[k], c_recv.at[k], {"tp": near}))
    f_copies = [along(far, k, c_send.at[n + k], c_recv.at[n + k], {"tp": near}) for k in range(n)]
    x_copies[0].start()
    for copy in z_copies:
        copy.start()
    c_copies[0].start()
    out_ref[tp, me] = own_ref[...]
    for k in range(1, n):
        z_copies[k - 1].wait_recv()
        x_copies[k].start()
        c_copies[k].start()
    for k in range(n):
        x_copies[k].wait_recv()
        f_copies[k].start()
    for copy in c_copies + f_copies:
        copy.wait_recv()
    for copy in z_copies + x_copies + c_copies + f_copies:
        copy.wait_send()


def gather_rows(own):
    n, wide = lax.axis_size("sp"), lax.axis_size("tp")
    if n > 8 or wide != 4:
        out = lax.all_gather(own, ("tp", "sp"), axis=0)
        return out.reshape((wide, n) + own.shape)
    dma = pltpu.SemaphoreType.DMA
    return pl.pallas_call(
        functools.partial(rows_kernel, n),
        out_shape=jax.ShapeDtypeStruct((wide, n) + own.shape, own.dtype),
        in_specs=[VMEM],
        out_specs=VMEM,
        scratch_shapes=[
            dma((n - 1,)),
            dma((n - 1,)),
            dma((n,)),
            dma((n,)),
            dma((2 * n,)),
            dma((2 * n,)),
        ],
        compiler_params=pltpu.CompilerParams(collective_id=2, has_side_effects=True),
        cost_estimate=pl.CostEstimate(flops=0, bytes_accessed=90_000_000, transcendentals=0),
        name="gather_rows",
    )(own)


def reduce_kernel(
    n, chunks, part_ref, base_ref, out_ref, got_c, sum_c, got_x, sum_x, got_z,
    c_send, c_recv, x_send, x_recv, z_send, z_recv,
):
    tp, near, far = partners()
    low, high = lax.rem(tp, 2), tp // 2
    shifts = range(1, n)
    me = lax.axis_index("sp") if n > 1 else 0
    greet([{"tp": near}, {"tp": far}] + [{"sp": lax.rem(me + k, n)} for k in shifts])
    width = part_ref.shape[-1] // chunks
    cols = [pl.ds(i * width, width) for i in range(chunks)]
    c_copies, x_copies, z_copies = [], [], []
    for i in range(chunks):
        copy = remote(
            part_ref.at[:, 1 - low, :, :, cols[i]],
            got_c.at[i],
            c_send.at[i],
            c_recv.at[i],
            {"tp": near},
        )
        copy.start()
        c_copies.append(copy)
    for i in range(chunks):
        c_copies[i].wait_recv()
        mine = part_ref[:, low, :, :, cols[i]].astype(jnp.float32)
        sum_c[i] = (mine + got_c[i].astype(jnp.float32)).astype(sum_c.dtype)
        copy = remote(
            sum_c.at[i, 1 - high], got_x.at[i], x_send.at[i], x_recv.at[i], {"tp": far}
        )
        copy.start()
        x_copies.append(copy)
    for i in range(chunks):
        x_copies[i].wait_recv()
        both = sum_c[i, high].astype(jnp.float32) + got_x[i].astype(jnp.float32)
        sum_x[i] = both.astype(sum_x.dtype)
        for k in shifts:
            peer = lax.rem(me + k, n)
            copy = remote(
                sum_x.at[i, peer],
                got_z.at[i, k - 1],
                z_send.at[i, k - 1],
                z_recv.at[i, k - 1],
                {"sp": peer},
            )
            copy.start()
            z_copies.append(copy)
    for i in range(chunks):
        total = sum_x[i, me].astype(jnp.float32)
        for k in shifts:
            z_copies[i * (n - 1) + k - 1].wait_recv()
            total = total + got_z[i, k - 1].astype(jnp.float32)
        out_ref[:, cols[i]] = (base_ref[:, cols[i]] + total).astype(out_ref.dtype)
    for copy in c_copies + x_copies + z_copies:
        copy.wait_send()


def reduce_rows(part, base, dtype, over_sp):
    wide, n = part.shape[:2]
    if n > 8 or wide != 4 or part.size > 8_000_000:
        axes = ("tp", "sp") if over_sp else "tp"
        flat = part.reshape(-1, part.shape[-1])
        total = lax.psum_scatter(flat, axes, scatter_dimension=0, tiled=True)
        return (base + total.astype(jnp.float32)).astype(dtype)
    rows, columns = part.shape[2:]
    chunks = 4 if columns % 512 == 0 else 1
    width = columns // chunks
    dma = pltpu.SemaphoreType.DMA
    zs = max(n - 1, 1)
    return pl.pallas_call(
        functools.partial(reduce_kernel, n, chunks),
        out_shape=jax.ShapeDtypeStruct((rows, columns), dtype),
        in_specs=[VMEM, VMEM],
        out_specs=VMEM,
        scratch_shapes=[
            pltpu.VMEM((chunks, 2, n, rows, width), part.dtype),
            pltpu.VMEM((chunks, 2, n, rows, width), part.dtype),
            pltpu.VMEM((chunks, n, rows, width), part.dtype),
            pltpu.VMEM((chunks, n, rows, width), part.dtype),
            pltpu.VMEM((chunks, zs, rows, width), part.dtype),
            dma((chunks,)),
            dma((chunks,)),
            dma((chunks,)),
            dma((chunks,)),
            dma((chunks, zs)),
            dma((chunks, zs)),
        ],
        compiler_params=pltpu.CompilerParams(
            collective_id=3 if over_sp else 4, has_side_effects=True
        ),
        cost_estimate=pl.CostEstimate(flops=0, bytes_accessed=60_000_000, transcendentals=0),
        name="reduce_all" if over_sp else "reduce_tp",
    )(part.reshape(2, 2, n, rows, columns), base)


def rotate(block, positions, heads):
    columns = block.shape[-1]
    width = columns // heads
    half = width // 2
    at = jnp.arange(columns, dtype=jnp.int32)
    freqs = ROPE_BASE ** (-(at % half).astype(jnp.float32) * 2.0 / width)
    angles = positions.astype(jnp.float32)[:, None] * freqs[None, :]
    source = jnp.where(at % width < half, at + half, at - half)
    sign = jnp.where(at % width < half, -1.0, 1.0)
    turn = jnp.where(at[:, None] == source[None, :], sign[None, :], 0.0).astype(jnp.bfloat16)
    flat = block.reshape(-1, columns)
    other = jnp.dot(flat, turn, preferred_element_type=jnp.float32).reshape(block.shape)
    turned = block.astype(jnp.float32) * jnp.cos(angles) + other * jnp.sin(angles)
    return turned.astype(jnp.bfloat16)


def depthwise(current, taps, docs):
    shown = current.astype(jnp.float32)
    total = taps[2] * shown
    for back in (1, 2):
        moved = jnp.pad(shown, ((0, 0), (back, 0), (0, 0)))[:, : shown.shape[1]]
        moved_docs = jnp.pad(docs, ((0, 0), (back, 0)), constant_values=-1)[:, : docs.shape[1]]
        total = total + jnp.where((moved_docs == docs)[..., None], taps[2 - back] * moved, 0.0)
    return total


def cyclic(array, axis, by):
    length = lax.axis_size(axis)
    return lax.ppermute(array, axis, [(i, (i + by) % length) for i in range(length)])


def exchange(piece, whole):
    count = lax.axis_size("sp")
    copies = lax.axis_size("grp")
    me = lax.axis_index("sp")
    mine = lax.axis_index("grp")
    if count > 8:
        pieces = jnp.stack([whole(dest) for dest in range(count)], axis=0)
        return lax.all_to_all(pieces, "sp", 0, 0)
    parts = []
    for shift in range(1, count):
        part = piece(lax.rem(me + shift, count), mine)
        parts.append(cyclic(part, "sp", shift))
    got = [jnp.stack(parts, axis=0)]
    for turn in range(1, copies):
        got.append(cyclic(got[0], "grp", turn))
    got = jnp.stack(got, axis=1)
    held = whole(me)
    held = jnp.broadcast_to(held[None], (1,) + held.shape)
    order = [lax.rem(mine - share + copies, copies) for share in range(copies)]
    out = []
    for source in range(count):
        shift = lax.rem(me - source + count, count)
        there = lax.max(shift - 1, 0)
        shares = [
            lax.dynamic_slice(got, (there, at) + (0,) * (got.ndim - 2), (1, 1) + got.shape[2:])[0]
            for at in order
        ]
        out.append(jnp.where(shift == 0, held, jnp.concatenate(shares, axis=0)[None]))
    return jnp.concatenate(out, axis=0)


def online_step(state, queries, keys, vals, allowed, scale):
    peak, total, accum = state
    scores = (
        jnp.einsum("sqhgd,skhd->shgqk", queries, keys, preferred_element_type=jnp.float32) * scale
    )
    mask = allowed[:, None, None]
    scores = jnp.where(mask, scores, NEG_BIG)
    new_peak = jnp.maximum(peak, jnp.max(scores, axis=-1))
    expd = jnp.where(mask, jnp.exp(scores - new_peak[..., None]), 0.0)
    fade = jnp.exp(peak - new_peak)
    new_total = total * fade + jnp.sum(expd, axis=-1)
    update = jnp.einsum(
        "shgqk,skhd->shgqd", expd.astype(jnp.bfloat16), vals, preferred_element_type=jnp.float32
    )
    return (new_peak, new_total, accum * fade[..., None] + update)


HBM = pl.BlockSpec(memory_space=pltpu.HBM)
SMEM = pl.BlockSpec(memory_space=pltpu.SMEM)
LANES = 128


def rounded(array):
    return array.astype(jnp.bfloat16)


def wide(array):
    return array.astype(jnp.float32)


def dot(left, right):
    return jnp.dot(left, right, preferred_element_type=jnp.float32)


class Phases:
    def __init__(self):
        self.open = None

    def __call__(self, name):
        if self.open is not None:
            self.open.__exit__(None, None, None)
        self.open = jax.named_scope(name) if name else None
        if name:
            self.open.__enter__()


def layer_kernel(
    n, per, tiles, scale,
    k_one, k_two, vals_own, doc_ids, lam, head_gain, join, q_one_hbm, q_two_hbm, norm_gain_hbm,
    taps_gate_hbm, taps_value_hbm, cosine_hbm, sine_hbm, turn_hbm, spread_hbm, resid_hbm, out_hbm, gate_hbm, value_hbm, down_hbm,
    out,
    q_one, q_two, norm_gain, taps_gate, taps_value, cosine, sine, turn, spread, resid,
    kv_all, docs_all, docs_row, out_w, heads, part_one, got_one, sum_one, got_far, mid,
    rows_all, up_w, down_w, hidden, part_two, got_two, sum_far, got_x, sum_z, own_z, got_z, got_in, held_z,
    d_send, d_recv, k_send, k_recv, o_sem, w_send, w_recv, y_send,
    c1_send, c1_recv, x1_send, x1_recv,
    az_send, az_recv, ax_send, ax_recv, ac_send, ac_recv,
    c2_recv, x2_recv, z2_recv,
):
    phase = Phases()
    z, g = lax.axis_index("sp"), lax.axis_index("grp")
    tp, near, far = partners()
    low, high = lax.rem(tp, 2), tp // 2
    diag = (1 - high) * 2 + 1 - low
    other = {"grp": 1 - g}
    spare = per * n - tiles
    seqs, rows = q_one.shape[:2]
    depth, columns = gate_hbm.shape[0], down_hbm.shape[1]
    features, total = resid.shape[1], n * rows
    loads = [
        pltpu.make_async_copy(there, here, sems.at[z, at])
        for sems, pairs in (
            (
                y_send,
                (
                    (q_one_hbm, q_one), (q_two_hbm, q_two), (cosine_hbm, cosine),
                    (sine_hbm, sine), (turn_hbm, turn),
                ),
            ),
            (
                w_send,
                (
                    (spread_hbm, spread), (resid_hbm, resid), (norm_gain_hbm, norm_gain),
                    (taps_gate_hbm, taps_gate), (taps_value_hbm, taps_value),
                ),
            ),
        )
        for at, (there, here) in enumerate(pairs)
    ]
    for load in loads:
        load.start()
    peers = [lax.rem(z + k, n) for k in range(1, n)]
    phase("greet")
    greet([{"sp": peer} for peer in peers] + [{"tp": near}, {"tp": far}, other])

    def rows_at(block):
        return pl.ds(pl.multiple_of(block * rows, rows), rows)

    phase("send_kv")
    def doc_copy(k, source, peer):
        part = docs_all.at[source]
        return remote(part, part, d_send.at[k], d_recv.at[source], {"sp": peer})

    def key_copy(block, p):
        half = seqs // 2
        part = kv_all.at[p * half : (p + 1) * half, rows_at(block)]
        peer = lax.rem(z + 1, n)
        return remote(part, part, k_send.at[block, p], k_recv.at[block, p], {"sp": peer})

    for seq in range(seqs):
        paired = dot(k_one[seq], join[0]) + dot(k_two[seq], join[1])
        kv_all[seq, rows_at(z), :LANES] = rounded(paired)
        kv_all[seq, rows_at(z), LANES:] = vals_own[seq]

    @pl.when(z < n - 1)
    def _():
        for p in (0, 1):
            key_copy(z, p).start()

    slot = lax.broadcasted_iota(jnp.int32, (rows, total), 1)
    spot = lax.broadcasted_iota(jnp.int32, (rows, total), 0) + z * rows
    place = jnp.where(slot == spot, 1.0, 0.0).astype(jnp.bfloat16)
    padded = jnp.concatenate([wide(doc_ids[...]), jnp.zeros((8 - seqs, rows), jnp.float32)], axis=0)
    docs_all[z] = dot(rounded(padded), place)
    for k, peer in enumerate(peers):
        doc_copy(k, z, peer).start()

    out_copy = pltpu.make_async_copy(out_hbm, out_w, o_sem)
    out_copy.start()

    def tile_of(block, k):
        return per * block + k - low * spare

    def valid(block, k):
        tile = tile_of(block, k)
        return (tile >= 0) & (tile < tiles)

    def weight_from(m, tile):
        at = pl.ds(pl.multiple_of(jnp.clip(tile, 0, tiles - 1) * LANES, LANES), LANES)
        if m >= 2:
            first = jnp.clip(tile, 0, tiles - 1) * LANES + (m - 2) * (LANES // 2)
            half = pl.ds(pl.multiple_of(first, LANES // 2), LANES // 2)
            return down_hbm.at[half, :]
        return (gate_hbm, value_hbm)[m].at[:, at]

    def weight_to(m, source, k):
        if m >= 2:
            across = pl.ds(pl.multiple_of(source * columns, columns), columns)
            return down_w.at[pl.ds(k * LANES + (m - 2) * (LANES // 2), LANES // 2), across]
        along = pl.ds(pl.multiple_of(source * depth, depth), depth)
        return up_w.at[along, pl.ds((2 * k + m) * LANES, LANES)]

    def over_z(m, k, source, dest):
        return lax.rem(k + m + source + dest, 2) == g

    def z_copy(m, k, peer):
        return remote(
            weight_from(m, tile_of(peer, k)), weight_to(m, z, k),
            w_send.at[peer, (4 * k + m) // 2], w_recv.at[z, 4 * k + m], {"sp": peer},
        )

    def y_copy(m, k, source):
        block = weight_to(m, source, k)
        at = 4 * k + m
        return remote(block, block, y_send.at[source, at // 2], w_recv.at[source, at], other)

    def own_copy(m, k):
        return pltpu.make_async_copy(
            weight_from(m, tile_of(z, k)), weight_to(m, z, k), w_recv.at[z, 4 * k + m]
        )

    def at_distance(d):
        return ((lax.rem(z - d + n, n), z - d >= 0), (lax.rem(z + d, n), z + d < n))

    def when_sent(d, items, act, ways=(0, 1)):
        for way in ways:
            peer, there = at_distance(d)[way]
            for k, m in items:

                @pl.when(there & valid(peer, k) & over_z(m, k, z, peer))
                def _():
                    act(z_copy(m, k, peer))

    def when_hopped(d, items, act, sides=(0, 1)):
        for k, m in items:
            for source, there in [at_distance(d)[side] for side in sides]:

                @pl.when(there & valid(z, k) & over_z(m, k, source, z))
                def _():
                    act(y_copy(m, k, source))

    def send(d, items, ways=(0, 1)):
        when_sent(d, items, lambda copy: copy.start(), ways)

    def relay(d, items, sides=(0, 1)):
        def act(copy):
            copy.wait_recv()
            copy.start()

        when_hopped(d, items, act, sides)

    ups = [(k, m) for k in range(per) for m in (0, 1)]
    downs = [(k, m) for k in range(per) for m in (2, 3)]
    early, middle, late = ups[: 2 * per - 2], ups[2 * per - 2 : 2 * per - 1], ups[2 * per - 1 :]

    def settle(m, k):
        for source in peers:

            @pl.when(valid(z, k) & jnp.logical_not(over_z(m, k, source, z)))
            def _():
                y_copy(m, k, source).wait_recv()

        @pl.when(valid(z, k))
        def _():
            own_copy(m, k).wait()

    phase("send_up")
    for d in range(1, n):
        send(d, early + middle, (0,))
    for step in range(1, n):
        block = z - step

        @pl.when(block >= 0)
        def _():
            for p in (0, 1):
                key_copy(block, p).wait_recv()

                @pl.when(z < n - 1)
                def _():
                    key_copy(block, p).start()

    for d in range(1, n):
        send(d, early, (1,))
    for k in range(per):

        @pl.when(valid(z, k))
        def _():
            for m in range(4):
                own_copy(m, k).start()

        @pl.when(jnp.logical_not(valid(z, k)))
        def _():
            pair = pl.ds(2 * k * LANES, 2 * LANES)
            up_w[:, pair] = jnp.zeros((up_w.shape[0], 2 * LANES), up_w.dtype)
            one = pl.ds(k * LANES, LANES)
            down_w[one, :] = jnp.zeros((LANES, down_w.shape[1]), down_w.dtype)

    for block in range(1, n):

        @pl.when(block > z)
        def _():
            blank = jnp.zeros((kv_all.shape[0], rows, kv_all.shape[2]), kv_all.dtype)
            kv_all[:, pl.ds(block * rows, rows)] = blank

    phase("wait_kv")
    for k, source in enumerate(peers):
        doc_copy(k, source, source).wait_recv()
    all_docs = functools.reduce(lambda a, b: a + b, [docs_all[i] for i in range(n)])
    for seq in range(seqs):
        docs_row[seq] = jnp.broadcast_to(all_docs[seq : seq + 1], (8, total))
    gain = jnp.concatenate([head_gain[...], head_gain[...]], axis=1)

    def iota(height, width, axis):
        return lax.broadcasted_iota(jnp.int32, (height, width), axis)

    def attend(seq, carry):
        doc_row = docs_row[seq][0:1]
        at_query = iota(rows, total, 0) + z * rows
        at_key = iota(rows, total, 1)
        doc_query = jnp.sum(jnp.where(at_key == at_query, doc_row, 0.0), axis=1, keepdims=True)
        allowed = (at_key <= at_query) & (doc_row == doc_query)
        bias = jnp.where(allowed, 0.0, NEG_BIG)
        bias = jnp.concatenate([bias] * 4, axis=0)
        q_cos, q_sin = cosine[rows_at(z)], sine[rows_at(z)]
        packed = kv_all[seq]
        spun = dot(packed[:, :LANES], spread[...])
        vals = wide(packed[:, LANES:])
        swapped = pltpu.roll(vals, LANES // 2, 1)
        lane = iota(total, LANES, 1)
        queries, keys = [], []
        width = cosine.shape[1]
        for index, source in enumerate((q_one, q_two)):
            block = source[seq]
            turned = wide(block) * q_cos + dot(block, turn[...]) * q_sin
            queries.append(rounded(turned))
            start = 2 * index * width
            straight = spun[:, start : start + width]
            crossed = spun[:, start + width : start + 2 * width]
            keys.append(rounded(straight * cosine[...] + crossed * sine[...]))
        q_lane = iota(rows, LANES, 1) // (LANES // 4)
        row4 = iota(4 * rows, 1, 0) // rows
        half_lane = iota(2 * rows, LANES, 1) < LANES // 2
        for c in range(2):
            across = slice(c * LANES, (c + 1) * LANES)
            pair = (vals, swapped) if c == 0 else (swapped, vals)
            both = rounded(jnp.where(lane < LANES // 2, pair[0], pair[1]))
            found = []
            for query, key in zip(queries, keys):
                local = wide(query[:, across])
                stack = jnp.concatenate(
                    [rounded(jnp.where(q_lane == j, local, 0.0)) for j in (0, 2, 1, 3)], axis=0
                )
                scores = lax.dot_general(
                    stack, key[:, across], (((1,), (1,)), ((), ())),
                    preferred_element_type=jnp.float32,
                )
                scores = scores * scale + bias
                expd = jnp.exp(scores - jnp.max(scores, axis=1, keepdims=True))
                summed = jnp.sum(expd, axis=1, keepdims=True)
                found.append(dot(rounded(expd), both) / summed)
            weights = jnp.where(
                row4 == 0, lam[4 * c],
                jnp.where(
                    row4 == 1, lam[4 * c + 2],
                    jnp.where(row4 == 2, lam[4 * c + 1], lam[4 * c + 3]),
                ),
            )
            mixed = found[0] - weights * found[1]
            meansq = jnp.sum(mixed * mixed, axis=1, keepdims=True) * (1.0 / LANES)
            normed = mixed * lax.rsqrt(meansq + NORM_EPS) * gain
            merged = rounded(jnp.where(half_lane, normed[: 2 * rows], normed[2 * rows :]))
            base = 2 * c * LANES
            heads[seq, :, base : base + LANES] = merged[:rows]
            heads[seq, :, base + LANES : base + 2 * LANES] = merged[rows:]
        return carry

    for load in loads:
        load.wait()
    phase("attend")
    lax.fori_loop(0, seqs, attend, 0)

    phase("proj")
    out_copy.wait()
    halves = got_one.shape[0]
    width = features // halves

    def c1_copy(i):
        cols = pl.ds(i * width, width)
        return remote(
            part_one.at[:, 1 - low, :, cols], got_one.at[i], c1_send.at[i], c1_recv.at[i], {"tp": near}
        )

    def x1_copy(i):
        return remote(sum_one.at[i], got_far.at[i], x1_send.at[i], x1_recv.at[i], {"tp": far})

    flat = heads[...].reshape(4 * rows, heads.shape[2])
    for i in range(halves):
        cols = pl.ds(i * width, width)
        made = rounded(dot(flat, out_w[:, cols]))
        part_one[:, :, :, cols] = made.reshape(2, 2, rows, width)
        c1_copy(i).start()
    phase("wait_c1")
    for i in range(halves):
        cols = pl.ds(i * width, width)
        c1_copy(i).wait_recv()
        sum_one[i] = rounded(wide(part_one[1 - high, low, :, cols]) + wide(got_one[i, 1 - high]))
        x1_copy(i).start()
        kept = wide(part_one[high, low, :, cols]) + wide(got_one[i, high])
        mid[:, cols] = wide(resid[:, cols]) + kept
    phase("relay_u1")
    relay(1, early)
    phase("wait_x1")
    for i in range(halves):
        cols = pl.ds(i * width, width)
        x1_copy(i).wait_recv()
        mid[:, cols] = mid[:, cols] + wide(got_far[i])
    phase("norm")
    held = mid[...]
    meansq = jnp.mean(held * held, axis=1, keepdims=True)
    rows_all[tp, rows_at(z)] = rounded(held * lax.rsqrt(meansq + NORM_EPS) * norm_gain[...])

    cuts = 2
    part_rows = rows // cuts

    def piece_of(owner, block, p):
        first = pl.multiple_of(block * rows + p * part_rows, part_rows)
        return rows_all.at[owner, pl.ds(first, part_rows)]

    def x_copy(owner, block, p):
        part = piece_of(owner, block, p)
        return remote(part, part, ax_send.at[block, p], ax_recv.at[block, p], {"tp": far})

    def c_copy(owner, hop, block):
        part = rows_all.at[owner, rows_at(block)]
        sems = (ac_send.at[hop, block], ac_recv.at[hop, block])
        return remote(part, part, *sems, {"tp": near})

    def chain_copy(way, block, p):
        part = piece_of(tp, block, p)
        peer = lax.rem(z + (1 if way == 0 else n - 1), n)
        return remote(part, part, az_send.at[way, block, p], az_recv.at[block, p], {"sp": peer})

    def pass_on(block, p):
        @pl.when((z >= block) & (z < n - 1))
        def _():
            chain_copy(0, block, p).start()

        @pl.when((z <= block) & (z > 0))
        def _():
            chain_copy(1, block, p).start()

        x_copy(tp, block, p).start()
        if p == cuts - 1:
            c_copy(tp, 0, block).start()

    def chain(step):
        for p in range(cuts):
            for block in (z - step, z + step):

                @pl.when((block >= 0) & (block < n))
                def _():
                    chain_copy(0, block, p).wait_recv()
                    pass_on(block, p)

    phase("ag_start")
    for p in range(cuts):
        pass_on(z, p)

    phase("relay_u2")
    for d in range(2, n):
        relay(d, early)
    for d in range(1, n):
        relay(d, middle, (1,))
    for step in range(1, n):
        phase(f"ag_z{step}")
        chain(step)
        ends = (z == 0) | (z == n - 1)
        for at, items in ((2, (late, middle + late)), (2, (downs, downs))):

            @pl.when((ends & (step == at)) | (jnp.logical_not(ends) & (step == 1)))
            def _():
                for d in range(1, n):
                    for way in (0, 1):
                        send(d, items[way], (way,))

    phase("relay_u3")
    for d in range(1, n):
        relay(d, middle, (0,))
        relay(d, late)
    phase("relay_d3")
    relay(1, downs)
    relay(2, downs)
    phase("settle_up")
    for k, m in ups:
        settle(m, k)

    def cross():
        for step in range(n):
            for p in range(cuts):
                for block in (z - step, z + step) if step else (z,):

                    @pl.when((block >= 0) & (block < n))
                    def _():
                        x_copy(far, block, p).wait_recv()
                        if p == cuts - 1:
                            c_copy(far, 1, block).start()

    def lift(i, carry):
        seq = lax.rem(high + i // 2, 2) * 2 + lax.rem(low + i, 2)
        for turn_at, (owner, hop) in ((1, (near, 0)), (3, (diag, 1))):

            @pl.when(i == turn_at)
            def _():
                for block in range(n):
                    c_copy(owner, hop, block).wait_recv()

        @pl.when(i == 0)
        def _():
            for d in range(3, n):
                relay(d, downs)

        @pl.when(i == 2)
        def _():
            cross()

        doc_row = docs_row[seq][0:1]
        at_row, at_col = iota(total, total, 0), iota(total, total, 1)
        doc_col = jnp.sum(jnp.where(at_row == at_col, doc_row, 0.0), axis=1, keepdims=True)
        same = jnp.where(doc_row == doc_col, 1.0, 0.0)
        back_one, back_two = [
            jnp.sum(jnp.where(at_col == at_row - back, same, 0.0), axis=1, keepdims=True)
            for back in (1, 2)
        ]

        def depthwise_of(current, taps):
            shown = wide(rounded(current))
            return (
                taps[2:3] * shown
                + taps[1:2] * (pltpu.roll(shown, 1, 0) * back_one)
                + taps[0:1] * (pltpu.roll(shown, 2, 0) * back_two)
            )

        for k in range(per):
            made = dot(rows_all[seq], up_w[:, 2 * k * LANES : (2 * k + 2) * LANES])
            tile = jnp.clip(tile_of(z, k), 0, tiles - 1)
            at = pl.ds(pl.multiple_of(tile * LANES, LANES), LANES)
            conv_g = depthwise_of(made[:, :LANES], taps_gate[:, at])
            conv_v = depthwise_of(made[:, LANES:], taps_value[:, at])
            unit = conv_g / (1.0 + jnp.exp(-conv_g)) * conv_v
            hidden[seq, :, k * LANES : (k + 1) * LANES] = rounded(unit)
        return carry

    phase("lift")
    lax.fori_loop(0, rows_all.shape[0], lift, 0)
    phase("settle_d")
    for k, m in downs:
        settle(m, k)

    def c2_copy(i, seq, block):
        there = rows_at(block)
        sems = (ac_send.at[i, block], c2_recv.at[i, block])
        return remote(part_two.at[seq, there], got_two.at[i, there], *sems, {"tp": near})

    chunk = 512 if features % 512 == 0 else features
    upper = z // (n // 2)
    mate = n // 2 - 1 - z + upper * n
    gate = (z == n // 2 - 1) | (z == n // 2)
    across = [upper * j + (1 - upper) * (n - 1 - j) for j in range(n // 2)]
    order = across + [mate, z]
    stops = [(j, p) for j in range(len(order)) for p in range(cuts)]

    def slot(p):
        return pl.ds(p * part_rows, part_rows)

    def piece_rows(block, p):
        return pl.ds(pl.multiple_of(block * rows + p * part_rows, part_rows), part_rows)

    def x2_copy(block, p):
        sems = (ax_send.at[block, p], x2_recv.at[block, p])
        return remote(sum_far.at[block, slot(p)], got_x.at[block, slot(p)], *sems, {"tp": far})

    def mate_copy(p):
        sems = (k_send.at[2, p], z2_recv.at[2, p])
        return remote(sum_z.at[2, slot(p)], got_z.at[0, slot(p)], *sems, {"sp": mate})

    def inner_copy(j, p):
        sems = (k_send.at[j, p], z2_recv.at[j, p])
        return remote(sum_z.at[j, slot(p)], got_in.at[j, slot(p)], *sems, {"sp": mate})

    def outer_copy(j, p):
        sems = (k_send.at[j, p], z2_recv.at[3, p])
        return remote(sum_z.at[j, slot(p)], got_z.at[1, slot(p)], *sems, {"sp": across[j]})

    def combine(j, p):
        @pl.when(gate)
        def _():
            inner_copy(j, p).wait_recv()
            sum_z[j, slot(p)] = rounded(held_z[j, slot(p)] + wide(got_in[j, slot(p)]))
            outer_copy(j, p).start()

    def lower(i, carry):
        seq = lax.rem(high + 1 - i // 2, 2) * 2 + lax.rem(low + 1 - lax.rem(i, 2), 2)
        for c in range(features // chunk):
            cols = slice(c * chunk, (c + 1) * chunk)
            part_two[seq, :, cols] = rounded(dot(hidden[seq], down_w[:, cols]))

        @pl.when(lax.rem(i, 2) == 0)
        def _():
            for block in order:
                c2_copy(i // 2, seq, block).start()

        @pl.when(i == 1)
        def _():
            for block in order:
                c2_copy(0, diag, block).wait_recv()
                for p in range(cuts):
                    there = piece_rows(block, p)
                    both = wide(part_two[far, there]) + wide(got_two[0, there])
                    sum_far[block, slot(p)] = rounded(both)
                    x2_copy(block, p).start()

        return carry

    for block in range(n):

        @pl.when((z >= block) & (z < n - 1))
        def _():
            for p in (0, 1):
                key_copy(block, p).wait_send()

        for p in range(cuts):
            x_copy(tp, block, p).wait_send()
        c_copy(tp, 0, block).wait_send()
        c_copy(far, 1, block).wait_send()
    phase("lower")
    lax.fori_loop(0, rows_all.shape[0], lower, 0)
    phase("x2")
    lag = 1
    for t, (j, p) in enumerate(stops):
        block = order[j]
        if p == 0:
            c2_copy(1, near, block).wait_recv()
        there = piece_rows(block, p)
        x2_copy(block, p).wait_recv()
        both = wide(part_two[tp, there]) + wide(got_two[1, there]) + wide(got_x[block, slot(p)])
        if j < len(across):

            @pl.when(gate)
            def _():
                held_z[j, slot(p)] = both

            @pl.when(jnp.logical_not(gate))
            def _():
                sum_z[j, slot(p)] = rounded(both)
                inner_copy(j, p).start()

        elif j == len(across):
            sum_z[j, slot(p)] = rounded(both)
            mate_copy(p).start()
        else:
            own_z[slot(p)] = mid[slot(p)] + both
        if t >= lag and stops[t - lag][0] < len(across):
            combine(*stops[t - lag])
    phase("z2")
    for p in range(cuts):
        mate_copy(p).wait_recv()
        outer_copy(0, p).wait_recv()
        answer = own_z[slot(p)] + wide(got_z[0, slot(p)]) + wide(got_z[1, slot(p)])
        out[slot(p)] = answer.astype(out.dtype)

    phase("drain")
    for k, peer in enumerate(peers):
        doc_copy(k, z, peer).wait_send()
    for p in range(cuts):
        mate_copy(p).wait_send()
        for j in range(len(across)):
            inner_copy(j, p).wait_send()
    for d in range(1, n):
        when_sent(d, ups + downs, lambda copy: copy.wait_send())
        when_hopped(d, ups + downs, lambda copy: copy.wait_send())
    for i in range(halves):
        c1_copy(i).wait_send()
        x1_copy(i).wait_send()
    for block in range(n):

        @pl.when((z >= block) & (z < n - 1))
        def _():
            for p in range(cuts):
                chain_copy(0, block, p).wait_send()

        @pl.when((z <= block) & (z > 0))
        def _():
            for p in range(cuts):
                chain_copy(1, block, p).wait_send()

        for p in range(cuts):
            x2_copy(block, p).wait_send()
        c2_copy(0, diag, block).wait_send()
        c2_copy(1, near, block).wait_send()
    phase(None)


def rope_tables(total, width, copies):
    half = width // 2
    freqs = np.float32(ROPE_BASE) ** (-np.arange(half, dtype=np.float32) * np.float32(2.0) / np.float32(width))
    angles = np.arange(total, dtype=np.float32)[:, None] * freqs.astype(np.float32)[None, :]
    tile = lambda table: np.tile(table.astype(np.float32), (1, 2 * copies))
    return tile(np.cos(angles)), tile(np.sin(angles))


def turn_matrix(width):
    half = width // 2
    at = np.arange(width)
    source = np.where(at < half, at + half, at - half)
    sign = np.where(at < half, -1.0, 1.0)
    return np.where(at[:, None] == source[None, :], sign[None, :], 0.0)


def spread_matrix(width, group, kv_local):
    straight = np.kron(np.eye(kv_local), np.tile(np.eye(width), (1, group)))
    crossed = np.kron(np.eye(kv_local), np.tile(turn_matrix(width), (1, group)))
    both = np.concatenate([straight, crossed], axis=1)
    return np.kron(np.eye(2), both)


def kernel_fits(resid_in, query_one, key_one, value, lam, gate_weight):
    heads = lam.shape[0]
    width = query_one.shape[2] // heads
    kv_local = key_one.shape[2] // width
    group = heads // kv_local
    seqs, rows = query_one.shape[:2]
    return (
        lax.axis_size("tp") == 4
        and lax.axis_size("grp") == 2
        and lax.axis_size("sp") == 4
        and kv_local == 2
        and group == 4
        and group * width == LANES
        and value.shape[2] == LANES
        and seqs == 4
        and resid_in.shape[0] == 1
        and rows % 16 == 0
        and rows * lax.axis_size("sp") <= 256
        and gate_weight.shape[0] <= 512
        and gate_weight.shape[1] % LANES == 0
        and gate_weight.shape[1] <= 1536
        and resid_in.shape[2] <= 2048
    )


def whole_layer(
    resid_in, query_one, key_one, query_two, key_two, value, lam, head_gain, doc_ids,
    out_weight, norm_gain, gate_weight, value_weight, conv_gate, conv_value, down_weight,
):
    n = lax.axis_size("sp")
    seqs, rows = query_one.shape[:2]
    heads = lam.shape[0]
    width = query_one.shape[2] // heads
    kv_local = key_one.shape[2] // width
    group = heads // kv_local
    features, total = resid_in.shape[2], n * rows
    depth, columns = gate_weight.shape[0], down_weight.shape[1]
    tiles = gate_weight.shape[1] // LANES
    per = -(-tiles // n)
    cosine, sine = rope_tables(total, width, heads)
    turn = np.kron(np.eye(heads), turn_matrix(width))
    spread = spread_matrix(width, group, kv_local)
    key_width = kv_local * width
    join = np.stack([np.eye(key_width, LANES), np.eye(key_width, LANES, LANES - key_width)])
    halves = 2
    bf16, f32 = jnp.bfloat16, jnp.float32
    dma = pltpu.SemaphoreType.DMA
    vmem = pltpu.VMEM
    scratch = [
        vmem(query_one.shape, bf16),
        vmem(query_two.shape, bf16),
        vmem((1, features), f32),
        vmem(conv_gate.shape, f32),
        vmem(conv_value.shape, f32),
        vmem(cosine.shape, f32),
        vmem(sine.shape, f32),
        vmem(turn.shape, bf16),
        vmem(spread.shape, bf16),
        vmem((rows, features), bf16),
        vmem((seqs, total, 2 * LANES), bf16),
        vmem((n, 8, total), f32),
        vmem((seqs, 8, total), f32),
        vmem(out_weight.shape, bf16),
        vmem((seqs, rows, out_weight.shape[0]), bf16),
        vmem((2, 2, rows, features), bf16),
        vmem((halves, 2, rows, features // halves), bf16),
        vmem((halves, rows, features // halves), bf16),
        vmem((halves, rows, features // halves), bf16),
        vmem((rows, features), f32),
        vmem((seqs, total, features), bf16),
        vmem((n * depth, 2 * per * LANES), bf16),
        vmem((per * LANES, n * columns), bf16),
        vmem((seqs, total, per * LANES), bf16),
        vmem((seqs, total, features), bf16),
        vmem((2, total, features), bf16),
        vmem((n, rows, features), bf16),
        vmem((n, rows, features), bf16),
        vmem((n - 1, rows, features), bf16),
        vmem((rows, features), f32),
        vmem((2, rows, features), bf16),
        vmem((2, rows, features), bf16),
        vmem((2, rows, features), f32),
        dma((n,)), dma((n,)), dma((n, 2)), dma((n, 2)), dma,
        dma((n, 2 * per)), dma((n, 4 * per)), dma((n, 2 * per)),
        dma((halves,)), dma((halves,)), dma((halves,)), dma((halves,)),
        dma((2, n, 2)), dma((n, 2)), dma((n, 2)), dma((n, 2)), dma((2, n)), dma((2, n)),
        dma((2, n)), dma((n, 2)), dma((n, 2)),
    ]
    out = pl.pallas_call(
        functools.partial(layer_kernel, n, per, tiles, width ** (-0.5)),
        out_shape=jax.ShapeDtypeStruct((rows, features), resid_in.dtype),
        in_specs=[VMEM] * 4 + [SMEM] + [VMEM] * 2 + [HBM] * 14,
        out_specs=VMEM,
        scratch_shapes=scratch,
        compiler_params=pltpu.CompilerParams(
            collective_id=5, has_side_effects=True, vmem_limit_bytes=60 * 2**20
        ),
        name="whole_layer",
    )(
        key_one, key_two, value, doc_ids, lam, head_gain[None], jnp.asarray(join, bf16),
        query_one, query_two, norm_gain[None], conv_gate, conv_value,
        jnp.asarray(cosine), jnp.asarray(sine), jnp.asarray(turn, bf16),
        jnp.asarray(spread, bf16), resid_in.reshape(rows, features),
        out_weight, gate_weight, value_weight, down_weight,
    )
    return out.reshape(resid_in.shape)


def per_device_apart(
    resid_in,
    query_one,
    key_one,
    query_two,
    key_two,
    value,
    lam,
    head_gain,
    doc_ids,
    out_weight,
    norm_gain,
    gate_weight,
    value_weight,
    conv_gate,
    conv_value,
    down_weight,
):
    n_sp = lax.axis_size("sp")
    me = lax.axis_index("sp")
    depth, width = gate_weight.shape
    share = width // n_sp
    copies = lax.axis_size("grp")

    def cut(weight, row, column, size):
        return lax.dynamic_slice(weight, (row, column), size)

    def up_piece(dest, part):
        size = (depth // copies, share)
        row, column = part * size[0], dest * share
        return jnp.stack([cut(gate_weight, row, column, size), cut(value_weight, row, column, size)])

    def up_whole(dest):
        return jnp.stack([up_piece(dest, part) for part in range(copies)])

    def down_piece(dest, part):
        size = (share // copies, down_weight.shape[1])
        return cut(down_weight, dest * share + part * size[0], 0, size)

    def down_whole(dest):
        return jnp.stack([down_piece(dest, part) for part in range(copies)])

    up_all = exchange(up_piece, up_whole)
    down_all = exchange(down_piece, down_whole)
    gate_all = up_all[:, :, 0].reshape(-1, share)
    value_all = up_all[:, :, 1].reshape(-1, share)
    down_full = jnp.transpose(down_all, (1, 2, 0, 3)).reshape(share, -1)
    seqs = query_one.shape[0]
    rows = query_one.shape[1]
    heads = lam.shape[0]
    key_width = query_one.shape[2] // heads
    kv_local = key_one.shape[2] // key_width
    group = heads // kv_local
    head_width = value.shape[2] // kv_local
    scale = key_width ** (-0.5)
    positions = lax.axis_index("sp") * rows + jnp.arange(rows, dtype=jnp.int32)
    q_first = rotate(query_one, positions, heads).reshape(seqs, rows, kv_local, group, key_width)
    q_second = rotate(query_two, positions, heads).reshape(seqs, rows, kv_local, group, key_width)
    k_first = rotate(key_one, positions, kv_local).reshape(seqs, rows, kv_local * key_width)
    k_second = rotate(key_two, positions, kv_local).reshape(seqs, rows, kv_local * key_width)
    start_state = (
        jnp.full((seqs, kv_local, group, rows), NEG_BIG, jnp.float32),
        jnp.zeros((seqs, kv_local, group, rows), jnp.float32),
        jnp.zeros((seqs, kv_local, group, rows, head_width), jnp.float32),
    )
    packed = jnp.concatenate(
        [k_first, k_second, value, doc_ids.astype(jnp.bfloat16)[..., None]], axis=-1
    )
    packed = gather_sp(packed)
    key_cols = k_first.shape[2]
    keys_one = packed[..., :key_cols]
    keys_two = packed[..., key_cols : 2 * key_cols]
    vals = packed[..., 2 * key_cols : -1]
    docs = packed[..., -1].astype(jnp.int32)
    count = keys_one.shape[1]
    step_len = math.gcd(count, 512)

    def inner(state, index):
        offset = index * step_len
        ka = lax.dynamic_slice_in_dim(keys_one, offset, step_len, 1).reshape(
            seqs, step_len, kv_local, key_width
        )
        kb = lax.dynamic_slice_in_dim(keys_two, offset, step_len, 1).reshape(
            seqs, step_len, kv_local, key_width
        )
        va = lax.dynamic_slice_in_dim(vals, offset, step_len, 1).reshape(
            seqs, step_len, kv_local, head_width
        )
        dpiece = lax.dynamic_slice_in_dim(docs, offset, step_len, 1)
        key_pos = offset + jnp.arange(step_len, dtype=jnp.int32)
        allowed = (key_pos[None, None, :] <= positions[None, :, None]) & (
            dpiece[:, None, :] == doc_ids[:, :, None]
        )
        first = online_step(state[0], q_first, ka, va, allowed, scale)
        second = online_step(state[1], q_second, kb, va, allowed, scale)
        return ((first, second), None)

    def run(state):
        return lax.scan(inner, state, jnp.arange(count // step_len))[0]

    first, second = lax.cond(
        jnp.int32(0) <= positions[rows - 1], run, lambda state: state, (start_state, start_state)
    )
    weights = lam.reshape(kv_local, group)[None, :, :, None, None]
    mixed = first[2] / first[1][..., None] - weights * (second[2] / second[1][..., None])
    meansq = jnp.mean(mixed * mixed, axis=-1, keepdims=True)
    normed_heads = mixed * lax.rsqrt(meansq + NORM_EPS) * head_gain
    heads_out = jnp.transpose(normed_heads, (0, 3, 1, 2, 4)).reshape(
        seqs * rows, heads * head_width
    )
    heads_out = heads_out.astype(jnp.bfloat16)
    own = resid_in.shape[0]
    features = resid_in.shape[2]
    proj = jnp.dot(heads_out, out_weight, preferred_element_type=jnp.float32).astype(jnp.bfloat16)
    mid = reduce_rows(
        proj.reshape(-1, 1, own * rows, features),
        resid_in.astype(jnp.float32).reshape(own * rows, features),
        jnp.float32,
        False,
    )
    meansq_mid = jnp.mean(mid * mid, axis=-1, keepdims=True)
    normed = (mid * lax.rsqrt(meansq_mid + NORM_EPS) * norm_gain).astype(jnp.bfloat16)
    gathered = gather_rows(normed).reshape(-1, n_sp, own, rows, features)
    full_rows = jnp.transpose(gathered, (0, 2, 1, 3, 4)).reshape(-1, features)
    total_rows = n_sp * rows
    start = me * share
    taps_gate = lax.dynamic_slice_in_dim(conv_gate, start, share, 1)
    taps_value = lax.dynamic_slice_in_dim(conv_value, start, share, 1)
    up_gate = jnp.dot(full_rows, gate_all, preferred_element_type=jnp.float32)
    up_value = jnp.dot(full_rows, value_all, preferred_element_type=jnp.float32)
    up_gate = up_gate.astype(jnp.bfloat16).reshape(seqs, total_rows, share)
    up_value = up_value.astype(jnp.bfloat16).reshape(seqs, total_rows, share)
    conv_g = depthwise(up_gate, taps_gate, docs)
    conv_v = depthwise(up_value, taps_value, docs)
    hidden = (jax.nn.silu(conv_g) * conv_v).astype(jnp.bfloat16)
    hidden = hidden.reshape(-1, own, n_sp, rows, share)
    hidden = jnp.transpose(hidden, (0, 2, 1, 3, 4)).reshape(-1, share)
    partial_down = jnp.dot(hidden, down_full, preferred_element_type=jnp.float32)
    partial_down = partial_down.astype(jnp.bfloat16).reshape(-1, n_sp, own * rows, features)
    return reduce_rows(partial_down, mid, jnp.bfloat16, True).reshape(resid_in.shape)


def per_device(*args):
    resid_in, query_one, key_one, value, lam, gate_weight = [args[i] for i in (0, 1, 2, 5, 6, 11)]
    if kernel_fits(resid_in, query_one, key_one, value, lam, gate_weight):
        return whole_layer(*args)
    return per_device_apart(*args)


def solution(mesh):
    placed = (
        P(("grp", "tp"), "sp", None),
        P("grp", "sp", "tp"),
        P("grp", "sp", "tp"),
        P("grp", "sp", "tp"),
        P("grp", "sp", "tp"),
        P("grp", "sp", "tp"),
        P("tp"),
        P(),
        P("grp", "sp"),
        P("tp", None),
        P(),
        P("sp", "tp"),
        P("sp", "tp"),
        P(None, "tp"),
        P(None, "tp"),
        P("tp", "sp"),
    )
    return jax.shard_map(
        per_device,
        mesh=mesh,
        in_specs=placed,
        out_specs=P(("grp", "tp"), "sp", None),
        check_vma=False,
    )
```

```python
import functools
import math

import jax
import jax.numpy as jnp
import numpy as np
from jax import lax
from jax.experimental import pallas as pl
from jax.experimental.pallas import tpu as pltpu
from jax.sharding import PartitionSpec as P

NEG_BIG = -1e30
NORM_EPS = 1e-06
ROPE_BASE = 500000.0


MESH = pl.DeviceIdType.MESH
VMEM = pl.BlockSpec(memory_space=pltpu.VMEM)


def greet(devices):
    barrier = pltpu.get_barrier_semaphore()
    for device in devices:
        pl.semaphore_signal(barrier, inc=1, device_id=device, device_id_type=MESH)
    pl.semaphore_wait(barrier, len(devices))


def remote(src, dst, send_sem, recv_sem, device):
    return pltpu.make_async_remote_copy(
        src_ref=src,
        dst_ref=dst,
        send_sem=send_sem,
        recv_sem=recv_sem,
        device_id=device,
        device_id_type=MESH,
    )


def partners():
    at = lax.axis_index("tp")
    return at, at + 1 - 2 * lax.rem(at, 2), lax.rem(at + 2, 4)


def spread_kernel(n, own_ref, out_ref, send_sem, recv_sem):
    me = lax.axis_index("sp")
    peers = [lax.rem(me + shift, n) for shift in range(1, n)]
    greet([{"sp": peer} for peer in peers])
    copies = []
    for k, peer in enumerate(peers):
        copy = remote(
            own_ref, out_ref.at[:, me], send_sem.at[k], recv_sem.at[k], {"sp": peer}
        )
        copy.start()
        copies.append(copy)
    out_ref[:, me] = own_ref[...]
    for copy in copies:
        copy.wait_recv()
    for copy in copies:
        copy.wait_send()


def gather_sp(own):
    n = lax.axis_size("sp")
    if n > 8:
        return lax.all_gather(own, "sp", axis=1, tiled=True)
    outer, rows, width = own.shape
    out = pl.pallas_call(
        functools.partial(spread_kernel, n),
        out_shape=jax.ShapeDtypeStruct((outer, n, rows, width), own.dtype),
        in_specs=[VMEM],
        out_specs=VMEM,
        scratch_shapes=[pltpu.SemaphoreType.DMA((n - 1,)), pltpu.SemaphoreType.DMA((n - 1,))],
        compiler_params=pltpu.CompilerParams(collective_id=1, has_side_effects=True),
        cost_estimate=pl.CostEstimate(flops=0, bytes_accessed=30_000_000, transcendentals=0),
        name="gather_sp",
    )(own)
    return out.reshape(outer, n * rows, width)


def rows_kernel(n, own_ref, out_ref, z_send, z_recv, x_send, x_recv, c_send, c_recv):
    me = lax.axis_index("sp")
    tp, near, far = partners()
    greet([{"tp": near}, {"tp": far}] + [{"sp": lax.rem(me + k, n)} for k in range(1, n)])
    sources = [lax.rem(me - k + n, n) for k in range(n)]
    z_copies = []
    for k in range(1, n):
        copy = remote(
            own_ref,
            out_ref.at[tp, me],
            z_send.at[k - 1],
            z_recv.at[k - 1],
            {"sp": lax.rem(me + k, n)},
        )
        z_copies.append(copy)

    def along(owner, k, send, recv, device):
        block = out_ref.at[owner, sources[k]]
        return remote(block, block, send, recv, device)

    x_copies = [remote(own_ref, out_ref.at[tp, me], x_send.at[0], x_recv.at[0], {"tp": far})]
    c_copies = [remote(own_ref, out_ref.at[tp, me], c_send.at[0], c_recv.at[0], {"tp": near})]
    for k in range(1, n):
        x_copies.append(along(tp, k, x_send.at[k], x_recv.at[k], {"tp": far}))
        c_copies.append(along(tp, k, c_send.at[k], c_recv.at[k], {"tp": near}))
    f_copies = [along(far, k, c_send.at[n + k], c_recv.at[n + k], {"tp": near}) for k in range(n)]
    x_copies[0].start()
    for copy in z_copies:
        copy.start()
    c_copies[0].start()
    out_ref[tp, me] = own_ref[...]
    for k in range(1, n):
        z_copies[k - 1].wait_recv()
        x_copies[k].start()
        c_copies[k].start()
    for k in range(n):
        x_copies[k].wait_recv()
        f_copies[k].start()
    for copy in c_copies + f_copies:
        copy.wait_recv()
    for copy in z_copies + x_copies + c_copies + f_copies:
        copy.wait_send()


def gather_rows(own):
    n, wide = lax.axis_size("sp"), lax.axis_size("tp")
    if n > 8 or wide != 4:
        out = lax.all_gather(own, ("tp", "sp"), axis=0)
        return out.reshape((wide, n) + own.shape)
    dma = pltpu.SemaphoreType.DMA
    return pl.pallas_call(
        functools.partial(rows_kernel, n),
        out_shape=jax.ShapeDtypeStruct((wide, n) + own.shape, own.dtype),
        in_specs=[VMEM],
        out_specs=VMEM,
        scratch_shapes=[
            dma((n - 1,)),
            dma((n - 1,)),
            dma((n,)),
            dma((n,)),
            dma((2 * n,)),
            dma((2 * n,)),
        ],
        compiler_params=pltpu.CompilerParams(collective_id=2, has_side_effects=True),
        cost_estimate=pl.CostEstimate(flops=0, bytes_accessed=90_000_000, transcendentals=0),
        name="gather_rows",
    )(own)


def reduce_kernel(
    n, chunks, part_ref, base_ref, out_ref, got_c, sum_c, got_x, sum_x, got_z,
    c_send, c_recv, x_send, x_recv, z_send, z_recv,
):
    tp, near, far = partners()
    low, high = lax.rem(tp, 2), tp // 2
    shifts = range(1, n)
    me = lax.axis_index("sp") if n > 1 else 0
    greet([{"tp": near}, {"tp": far}] + [{"sp": lax.rem(me + k, n)} for k in shifts])
    width = part_ref.shape[-1] // chunks
    cols = [pl.ds(i * width, width) for i in range(chunks)]
    c_copies, x_copies, z_copies = [], [], []
    for i in range(chunks):
        copy = remote(
            part_ref.at[:, 1 - low, :, :, cols[i]],
            got_c.at[i],
            c_send.at[i],
            c_recv.at[i],
            {"tp": near},
        )
        copy.start()
        c_copies.append(copy)
    for i in range(chunks):
        c_copies[i].wait_recv()
        mine = part_ref[:, low, :, :, cols[i]].astype(jnp.float32)
        sum_c[i] = (mine + got_c[i].astype(jnp.float32)).astype(sum_c.dtype)
        copy = remote(
            sum_c.at[i, 1 - high], got_x.at[i], x_send.at[i], x_recv.at[i], {"tp": far}
        )
        copy.start()
        x_copies.append(copy)
    for i in range(chunks):
        x_copies[i].wait_recv()
        both = sum_c[i, high].astype(jnp.float32) + got_x[i].astype(jnp.float32)
        sum_x[i] = both.astype(sum_x.dtype)
        for k in shifts:
            peer = lax.rem(me + k, n)
            copy = remote(
                sum_x.at[i, peer],
                got_z.at[i, k - 1],
                z_send.at[i, k - 1],
                z_recv.at[i, k - 1],
                {"sp": peer},
            )
            copy.start()
            z_copies.append(copy)
    for i in range(chunks):
        total = sum_x[i, me].astype(jnp.float32)
        for k in shifts:
            z_copies[i * (n - 1) + k - 1].wait_recv()
            total = total + got_z[i, k - 1].astype(jnp.float32)
        out_ref[:, cols[i]] = (base_ref[:, cols[i]] + total).astype(out_ref.dtype)
    for copy in c_copies + x_copies + z_copies:
        copy.wait_send()


def reduce_rows(part, base, dtype, over_sp):
    wide, n = part.shape[:2]
    if n > 8 or wide != 4 or part.size > 8_000_000:
        axes = ("tp", "sp") if over_sp else "tp"
        flat = part.reshape(-1, part.shape[-1])
        total = lax.psum_scatter(flat, axes, scatter_dimension=0, tiled=True)
        return (base + total.astype(jnp.float32)).astype(dtype)
    rows, columns = part.shape[2:]
    chunks = 4 if columns % 512 == 0 else 1
    width = columns // chunks
    dma = pltpu.SemaphoreType.DMA
    zs = max(n - 1, 1)
    return pl.pallas_call(
        functools.partial(reduce_kernel, n, chunks),
        out_shape=jax.ShapeDtypeStruct((rows, columns), dtype),
        in_specs=[VMEM, VMEM],
        out_specs=VMEM,
        scratch_shapes=[
            pltpu.VMEM((chunks, 2, n, rows, width), part.dtype),
            pltpu.VMEM((chunks, 2, n, rows, width), part.dtype),
            pltpu.VMEM((chunks, n, rows, width), part.dtype),
            pltpu.VMEM((chunks, n, rows, width), part.dtype),
            pltpu.VMEM((chunks, zs, rows, width), part.dtype),
            dma((chunks,)),
            dma((chunks,)),
            dma((chunks,)),
            dma((chunks,)),
            dma((chunks, zs)),
            dma((chunks, zs)),
        ],
        compiler_params=pltpu.CompilerParams(
            collective_id=3 if over_sp else 4, has_side_effects=True
        ),
        cost_estimate=pl.CostEstimate(flops=0, bytes_accessed=60_000_000, transcendentals=0),
        name="reduce_all" if over_sp else "reduce_tp",
    )(part.reshape(2, 2, n, rows, columns), base)


def rotate(block, positions, heads):
    columns = block.shape[-1]
    width = columns // heads
    half = width // 2
    at = jnp.arange(columns, dtype=jnp.int32)
    freqs = ROPE_BASE ** (-(at % half).astype(jnp.float32) * 2.0 / width)
    angles = positions.astype(jnp.float32)[:, None] * freqs[None, :]
    source = jnp.where(at % width < half, at + half, at - half)
    sign = jnp.where(at % width < half, -1.0, 1.0)
    turn = jnp.where(at[:, None] == source[None, :], sign[None, :], 0.0).astype(jnp.bfloat16)
    flat = block.reshape(-1, columns)
    other = jnp.dot(flat, turn, preferred_element_type=jnp.float32).reshape(block.shape)
    turned = block.astype(jnp.float32) * jnp.cos(angles) + other * jnp.sin(angles)
    return turned.astype(jnp.bfloat16)


def depthwise(current, taps, docs):
    shown = current.astype(jnp.float32)
    total = taps[2] * shown
    for back in (1, 2):
        moved = jnp.pad(shown, ((0, 0), (back, 0), (0, 0)))[:, : shown.shape[1]]
        moved_docs = jnp.pad(docs, ((0, 0), (back, 0)), constant_values=-1)[:, : docs.shape[1]]
        total = total + jnp.where((moved_docs == docs)[..., None], taps[2 - back] * moved, 0.0)
    return total


def cyclic(array, axis, by):
    length = lax.axis_size(axis)
    return lax.ppermute(array, axis, [(i, (i + by) % length) for i in range(length)])


def exchange(piece, whole):
    count = lax.axis_size("sp")
    copies = lax.axis_size("grp")
    me = lax.axis_index("sp")
    mine = lax.axis_index("grp")
    if count > 8:
        pieces = jnp.stack([whole(dest) for dest in range(count)], axis=0)
        return lax.all_to_all(pieces, "sp", 0, 0)
    parts = []
    for shift in range(1, count):
        part = piece(lax.rem(me + shift, count), mine)
        parts.append(cyclic(part, "sp", shift))
    got = [jnp.stack(parts, axis=0)]
    for turn in range(1, copies):
        got.append(cyclic(got[0], "grp", turn))
    got = jnp.stack(got, axis=1)
    held = whole(me)
    held = jnp.broadcast_to(held[None], (1,) + held.shape)
    order = [lax.rem(mine - share + copies, copies) for share in range(copies)]
    out = []
    for source in range(count):
        shift = lax.rem(me - source + count, count)
        there = lax.max(shift - 1, 0)
        shares = [
            lax.dynamic_slice(got, (there, at) + (0,) * (got.ndim - 2), (1, 1) + got.shape[2:])[0]
            for at in order
        ]
        out.append(jnp.where(shift == 0, held, jnp.concatenate(shares, axis=0)[None]))
    return jnp.concatenate(out, axis=0)


def online_step(state, queries, keys, vals, allowed, scale):
    peak, total, accum = state
    scores = (
        jnp.einsum("sqhgd,skhd->shgqk", queries, keys, preferred_element_type=jnp.float32) * scale
    )
    mask = allowed[:, None, None]
    scores = jnp.where(mask, scores, NEG_BIG)
    new_peak = jnp.maximum(peak, jnp.max(scores, axis=-1))
    expd = jnp.where(mask, jnp.exp(scores - new_peak[..., None]), 0.0)
    fade = jnp.exp(peak - new_peak)
    new_total = total * fade + jnp.sum(expd, axis=-1)
    update = jnp.einsum(
        "shgqk,skhd->shgqd", expd.astype(jnp.bfloat16), vals, preferred_element_type=jnp.float32
    )
    return (new_peak, new_total, accum * fade[..., None] + update)


HBM = pl.BlockSpec(memory_space=pltpu.HBM)
SMEM = pl.BlockSpec(memory_space=pltpu.SMEM)
LANES = 128


def rounded(array):
    return array.astype(jnp.bfloat16)


def wide(array):
    return array.astype(jnp.float32)


def dot(left, right):
    return jnp.dot(left, right, preferred_element_type=jnp.float32)


class Phases:
    def __init__(self):
        self.open = None

    def __call__(self, name):
        if self.open is not None:
            self.open.__exit__(None, None, None)
        self.open = jax.named_scope(name) if name else None
        if name:
            self.open.__enter__()


def layer_kernel(
    n, per, tiles, scale,
    k_one, k_two, vals_own, doc_ids, lam, head_gain, join, q_one_hbm, q_two_hbm, norm_gain_hbm,
    taps_gate_hbm, taps_value_hbm, cosine_hbm, sine_hbm, turn_hbm, spread_hbm, resid_hbm, out_hbm, gate_hbm, value_hbm, down_hbm,
    out,
    q_one, q_two, norm_gain, taps_gate, taps_value, cosine, sine, turn, spread, resid,
    kv_all, docs_all, docs_row, out_w, heads, part_one, got_one, sum_one, got_far, mid,
    rows_all, up_w, down_w, hidden, part_two, got_two, sum_far, got_x, sum_z, own_z, got_z, got_in, held_z,
    d_send, d_recv, k_send, k_recv, o_sem, w_send, w_recv, y_send,
    c1_send, c1_recv, x1_send, x1_recv,
    az_send, az_recv, ax_send, ax_recv, ac_send, ac_recv,
    c2_recv, x2_recv, z2_recv,
):
    phase = Phases()
    z, g = lax.axis_index("sp"), lax.axis_index("grp")
    tp, near, far = partners()
    low, high = lax.rem(tp, 2), tp // 2
    diag = (1 - high) * 2 + 1 - low
    other = {"grp": 1 - g}
    spare = per * n - tiles
    seqs, rows = q_one.shape[:2]
    depth, columns = gate_hbm.shape[0], down_hbm.shape[1]
    features, total = resid.shape[1], n * rows
    loads = [
        pltpu.make_async_copy(there, here, sems.at[z, at])
        for sems, pairs in (
            (
                y_send,
                (
                    (q_one_hbm, q_one), (q_two_hbm, q_two), (cosine_hbm, cosine),
                    (sine_hbm, sine), (turn_hbm, turn),
                ),
            ),
            (
                w_send,
                (
                    (spread_hbm, spread), (resid_hbm, resid), (norm_gain_hbm, norm_gain),
                    (taps_gate_hbm, taps_gate), (taps_value_hbm, taps_value),
                ),
            ),
        )
        for at, (there, here) in enumerate(pairs)
    ]
    for load in loads:
        load.start()
    peers = [lax.rem(z + k, n) for k in range(1, n)]
    phase("greet")
    greet([{"sp": peer} for peer in peers] + [{"tp": near}, {"tp": far}, other])

    def rows_at(block):
        return pl.ds(pl.multiple_of(block * rows, rows), rows)

    phase("send_kv")
    def doc_copy(k, source, peer):
        part = docs_all.at[source]
        return remote(part, part, d_send.at[k], d_recv.at[source], {"sp": peer})

    def key_copy(block, p):
        half = seqs // 2
        part = kv_all.at[p * half : (p + 1) * half, rows_at(block)]
        peer = lax.rem(z + 1, n)
        return remote(part, part, k_send.at[block, p], k_recv.at[block, p], {"sp": peer})

    for seq in range(seqs):
        paired = dot(k_one[seq], join[0]) + dot(k_two[seq], join[1])
        kv_all[seq, rows_at(z), :LANES] = rounded(paired)
        kv_all[seq, rows_at(z), LANES:] = vals_own[seq]

    @pl.when(z < n - 1)
    def _():
        for p in (0, 1):
            key_copy(z, p).start()

    slot = lax.broadcasted_iota(jnp.int32, (rows, total), 1)
    spot = lax.broadcasted_iota(jnp.int32, (rows, total), 0) + z * rows
    place = jnp.where(slot == spot, 1.0, 0.0).astype(jnp.bfloat16)
    padded = jnp.concatenate([wide(doc_ids[...]), jnp.zeros((8 - seqs, rows), jnp.float32)], axis=0)
    docs_all[z] = dot(rounded(padded), place)
    for k, peer in enumerate(peers):
        doc_copy(k, z, peer).start()

    out_copy = pltpu.make_async_copy(out_hbm, out_w, o_sem)
    out_copy.start()

    def tile_of(block, k):
        return per * block + k - low * spare

    def valid(block, k):
        tile = tile_of(block, k)
        return (tile >= 0) & (tile < tiles)

    def weight_from(m, tile):
        at = pl.ds(pl.multiple_of(jnp.clip(tile, 0, tiles - 1) * LANES, LANES), LANES)
        if m >= 2:
            first = jnp.clip(tile, 0, tiles - 1) * LANES + (m - 2) * (LANES // 2)
            half = pl.ds(pl.multiple_of(first, LANES // 2), LANES // 2)
            return down_hbm.at[half, :]
        return (gate_hbm, value_hbm)[m].at[:, at]

    def weight_to(m, source, k):
        if m >= 2:
            across = pl.ds(pl.multiple_of(source * columns, columns), columns)
            return down_w.at[pl.ds(k * LANES + (m - 2) * (LANES // 2), LANES // 2), across]
        along = pl.ds(pl.multiple_of(source * depth, depth), depth)
        return up_w.at[along, pl.ds((2 * k + m) * LANES, LANES)]

    def over_z(m, k, source, dest):
        return lax.rem(k + m + source + dest, 2) == g

    def z_copy(m, k, peer):
        return remote(
            weight_from(m, tile_of(peer, k)), weight_to(m, z, k),
            w_send.at[peer, (4 * k + m) // 2], w_recv.at[z, 4 * k + m], {"sp": peer},
        )

    def y_copy(m, k, source):
        block = weight_to(m, source, k)
        at = 4 * k + m
        return remote(block, block, y_send.at[source, at // 2], w_recv.at[source, at], other)

    def own_copy(m, k):
        return pltpu.make_async_copy(
            weight_from(m, tile_of(z, k)), weight_to(m, z, k), w_recv.at[z, 4 * k + m]
        )

    def at_distance(d):
        return ((lax.rem(z - d + n, n), z - d >= 0), (lax.rem(z + d, n), z + d < n))

    def when_sent(d, items, act, ways=(0, 1)):
        for way in ways:
            peer, there = at_distance(d)[way]
            for k, m in items:

                @pl.when(there & valid(peer, k) & over_z(m, k, z, peer))
                def _():
                    act(z_copy(m, k, peer))

    def when_hopped(d, items, act, sides=(0, 1)):
        for k, m in items:
            for source, there in [at_distance(d)[side] for side in sides]:

                @pl.when(there & valid(z, k) & over_z(m, k, source, z))
                def _():
                    act(y_copy(m, k, source))

    def send(d, items, ways=(0, 1)):
        when_sent(d, items, lambda copy: copy.start(), ways)

    def relay(d, items, sides=(0, 1)):
        def act(copy):
            copy.wait_recv()
            copy.start()

        when_hopped(d, items, act, sides)

    ups = [(k, m) for k in range(per) for m in (0, 1)]
    downs = [(k, m) for k in range(per) for m in (2, 3)]
    early, middle, late = ups[: 2 * per - 2], ups[2 * per - 2 : 2 * per - 1], ups[2 * per - 1 :]

    def settle(m, k):
        for source in peers:

            @pl.when(valid(z, k) & jnp.logical_not(over_z(m, k, source, z)))
            def _():
                y_copy(m, k, source).wait_recv()

        @pl.when(valid(z, k))
        def _():
            own_copy(m, k).wait()

    phase("send_up")
    for d in range(1, n):
        send(d, early + middle, (0,))
    for step in range(1, n):
        block = z - step

        @pl.when(block >= 0)
        def _():
            for p in (0, 1):
                key_copy(block, p).wait_recv()

                @pl.when(z < n - 1)
                def _():
                    key_copy(block, p).start()

    for d in range(1, n):
        send(d, early, (1,))
    for k in range(per):

        @pl.when(valid(z, k))
        def _():
            for m in range(4):
                own_copy(m, k).start()

        @pl.when(jnp.logical_not(valid(z, k)))
        def _():
            pair = pl.ds(2 * k * LANES, 2 * LANES)
            up_w[:, pair] = jnp.zeros((up_w.shape[0], 2 * LANES), up_w.dtype)
            one = pl.ds(k * LANES, LANES)
            down_w[one, :] = jnp.zeros((LANES, down_w.shape[1]), down_w.dtype)

    for block in range(1, n):

        @pl.when(block > z)
        def _():
            blank = jnp.zeros((kv_all.shape[0], rows, kv_all.shape[2]), kv_all.dtype)
            kv_all[:, pl.ds(block * rows, rows)] = blank

    phase("wait_kv")
    for k, source in enumerate(peers):
        doc_copy(k, source, source).wait_recv()
    all_docs = functools.reduce(lambda a, b: a + b, [docs_all[i] for i in range(n)])
    for seq in range(seqs):
        docs_row[seq] = jnp.broadcast_to(all_docs[seq : seq + 1], (8, total))
    gain = jnp.concatenate([head_gain[...], head_gain[...]], axis=1)

    def iota(height, width, axis):
        return lax.broadcasted_iota(jnp.int32, (height, width), axis)

    def attend(seq, carry):
        doc_row = docs_row[seq][0:1]
        at_query = iota(rows, total, 0) + z * rows
        at_key = iota(rows, total, 1)
        doc_query = jnp.sum(jnp.where(at_key == at_query, doc_row, 0.0), axis=1, keepdims=True)
        allowed = (at_key <= at_query) & (doc_row == doc_query)
        bias = jnp.where(allowed, 0.0, NEG_BIG)
        bias = jnp.concatenate([bias] * 4, axis=0)
        q_cos, q_sin = cosine[rows_at(z)], sine[rows_at(z)]
        packed = kv_all[seq]
        spun = dot(packed[:, :LANES], spread[...])
        vals = wide(packed[:, LANES:])
        swapped = pltpu.roll(vals, LANES // 2, 1)
        lane = iota(total, LANES, 1)
        queries, keys = [], []
        width = cosine.shape[1]
        for index, source in enumerate((q_one, q_two)):
            block = source[seq]
            turned = wide(block) * q_cos + dot(block, turn[...]) * q_sin
            queries.append(rounded(turned))
            start = 2 * index * width
            straight = spun[:, start : start + width]
            crossed = spun[:, start + width : start + 2 * width]
            keys.append(rounded(straight * cosine[...] + crossed * sine[...]))
        q_lane = iota(rows, LANES, 1) // (LANES // 4)
        row4 = iota(4 * rows, 1, 0) // rows
        half_lane = iota(2 * rows, LANES, 1) < LANES // 2
        for c in range(2):
            across = slice(c * LANES, (c + 1) * LANES)
            pair = (vals, swapped) if c == 0 else (swapped, vals)
            both = rounded(jnp.where(lane < LANES // 2, pair[0], pair[1]))
            found = []
            for query, key in zip(queries, keys):
                local = wide(query[:, across])
                stack = jnp.concatenate(
                    [rounded(jnp.where(q_lane == j, local, 0.0)) for j in (0, 2, 1, 3)], axis=0
                )
                scores = lax.dot_general(
                    stack, key[:, across], (((1,), (1,)), ((), ())),
                    preferred_element_type=jnp.float32,
                )
                scores = scores * scale + bias
                expd = jnp.exp(scores - jnp.max(scores, axis=1, keepdims=True))
                summed = jnp.sum(expd, axis=1, keepdims=True)
                found.append(dot(rounded(expd), both) / summed)
            weights = jnp.where(
                row4 == 0, lam[4 * c],
                jnp.where(
                    row4 == 1, lam[4 * c + 2],
                    jnp.where(row4 == 2, lam[4 * c + 1], lam[4 * c + 3]),
                ),
            )
            mixed = found[0] - weights * found[1]
            meansq = jnp.sum(mixed * mixed, axis=1, keepdims=True) * (1.0 / LANES)
            normed = mixed * lax.rsqrt(meansq + NORM_EPS) * gain
            merged = rounded(jnp.where(half_lane, normed[: 2 * rows], normed[2 * rows :]))
            base = 2 * c * LANES
            heads[seq, :, base : base + LANES] = merged[:rows]
            heads[seq, :, base + LANES : base + 2 * LANES] = merged[rows:]
        return carry

    for load in loads:
        load.wait()
    phase("attend")
    lax.fori_loop(0, seqs, attend, 0)

    phase("proj")
    out_copy.wait()
    halves = got_one.shape[0]
    width = features // halves

    def c1_copy(i):
        cols = pl.ds(i * width, width)
        return remote(
            part_one.at[:, 1 - low, :, cols], got_one.at[i], c1_send.at[i], c1_recv.at[i], {"tp": near}
        )

    def x1_copy(i):
        return remote(sum_one.at[i], got_far.at[i], x1_send.at[i], x1_recv.at[i], {"tp": far})

    flat = heads[...].reshape(4 * rows, heads.shape[2])
    for i in range(halves):
        cols = pl.ds(i * width, width)
        made = rounded(dot(flat, out_w[:, cols]))
        part_one[:, :, :, cols] = made.reshape(2, 2, rows, width)
        c1_copy(i).start()
    phase("wait_c1")
    for i in range(halves):
        cols = pl.ds(i * width, width)
        c1_copy(i).wait_recv()
        sum_one[i] = rounded(wide(part_one[1 - high, low, :, cols]) + wide(got_one[i, 1 - high]))
        x1_copy(i).start()
        kept = wide(part_one[high, low, :, cols]) + wide(got_one[i, high])
        mid[:, cols] = wide(resid[:, cols]) + kept
    phase("relay_u1")
    relay(1, early)
    phase("wait_x1")
    for i in range(halves):
        cols = pl.ds(i * width, width)
        x1_copy(i).wait_recv()
        mid[:, cols] = mid[:, cols] + wide(got_far[i])
    phase("norm")
    held = mid[...]
    meansq = jnp.mean(held * held, axis=1, keepdims=True)
    rows_all[tp, rows_at(z)] = rounded(held * lax.rsqrt(meansq + NORM_EPS) * norm_gain[...])

    cuts = 2
    part_rows = rows // cuts

    def piece_of(owner, block, p):
        first = pl.multiple_of(block * rows + p * part_rows, part_rows)
        return rows_all.at[owner, pl.ds(first, part_rows)]

    def x_copy(owner, block, p):
        part = piece_of(owner, block, p)
        return remote(part, part, ax_send.at[block, p], ax_recv.at[block, p], {"tp": far})

    def c_copy(owner, hop, block):
        part = rows_all.at[owner, rows_at(block)]
        sems = (ac_send.at[hop, block], ac_recv.at[hop, block])
        return remote(part, part, *sems, {"tp": near})

    def chain_copy(way, block, p):
        part = piece_of(tp, block, p)
        peer = lax.rem(z + (1 if way == 0 else n - 1), n)
        return remote(part, part, az_send.at[way, block, p], az_recv.at[block, p], {"sp": peer})

    def pass_on(block, p):
        @pl.when((z >= block) & (z < n - 1))
        def _():
            chain_copy(0, block, p).start()

        @pl.when((z <= block) & (z > 0))
        def _():
            chain_copy(1, block, p).start()

        x_copy(tp, block, p).start()
        if p == cuts - 1:
            c_copy(tp, 0, block).start()

    def chain(step):
        for p in range(cuts):
            for block in (z - step, z + step):

                @pl.when((block >= 0) & (block < n))
                def _():
                    chain_copy(0, block, p).wait_recv()
                    pass_on(block, p)

    phase("ag_start")
    for p in range(cuts):
        pass_on(z, p)

    phase("relay_u2")
    for d in range(2, n):
        relay(d, early)
    for d in range(1, n):
        relay(d, middle, (1,))
    for step in range(1, n):
        phase(f"ag_z{step}")
        chain(step)
        ends = (z == 0) | (z == n - 1)
        for at, items in ((2, (late, middle + late)), (2, (downs, downs))):

            @pl.when((ends & (step == at)) | (jnp.logical_not(ends) & (step == 1)))
            def _():
                for d in range(1, n):
                    for way in (0, 1):
                        send(d, items[way], (way,))

    phase("relay_u3")
    for d in range(1, n):
        relay(d, late, (1,))
        relay(d, middle + late, (0,))
    phase("relay_d3")
    relay(1, downs)
    relay(2, downs)
    phase("settle_up")
    for k, m in ups:
        settle(m, k)

    def cross():
        for step in range(n):
            for p in range(cuts):
                for block in (z - step, z + step) if step else (z,):

                    @pl.when((block >= 0) & (block < n))
                    def _():
                        x_copy(far, block, p).wait_recv()
                        if p == cuts - 1:
                            c_copy(far, 1, block).start()

    def lift(i, carry):
        seq = lax.rem(high + i // 2, 2) * 2 + lax.rem(low + i, 2)
        for turn_at, (owner, hop) in ((1, (near, 0)), (3, (diag, 1))):

            @pl.when(i == turn_at)
            def _():
                for block in range(n):
                    c_copy(owner, hop, block).wait_recv()

        @pl.when(i == 0)
        def _():
            for d in range(3, n):
                relay(d, downs)

        @pl.when(i == 1)
        def _():
            cross()

        doc_row = docs_row[seq][0:1]
        at_row, at_col = iota(total, total, 0), iota(total, total, 1)
        doc_col = jnp.sum(jnp.where(at_row == at_col, doc_row, 0.0), axis=1, keepdims=True)
        same = jnp.where(doc_row == doc_col, 1.0, 0.0)
        back_one, back_two = [
            jnp.sum(jnp.where(at_col == at_row - back, same, 0.0), axis=1, keepdims=True)
            for back in (1, 2)
        ]

        def depthwise_of(current, taps):
            shown = wide(rounded(current))
            return (
                taps[2:3] * shown
                + taps[1:2] * (pltpu.roll(shown, 1, 0) * back_one)
                + taps[0:1] * (pltpu.roll(shown, 2, 0) * back_two)
            )

        for k in range(per):
            made = dot(rows_all[seq], up_w[:, 2 * k * LANES : (2 * k + 2) * LANES])
            tile = jnp.clip(tile_of(z, k), 0, tiles - 1)
            at = pl.ds(pl.multiple_of(tile * LANES, LANES), LANES)
            conv_g = depthwise_of(made[:, :LANES], taps_gate[:, at])
            conv_v = depthwise_of(made[:, LANES:], taps_value[:, at])
            unit = conv_g / (1.0 + jnp.exp(-conv_g)) * conv_v
            hidden[seq, :, k * LANES : (k + 1) * LANES] = rounded(unit)
        return carry

    phase("lift")
    lax.fori_loop(0, rows_all.shape[0], lift, 0)
    phase("settle_d")
    for k, m in downs:
        settle(m, k)

    def c2_copy(i, seq, block):
        there = rows_at(block)
        sems = (ac_send.at[i, block], c2_recv.at[i, block])
        return remote(part_two.at[seq, there], got_two.at[i, there], *sems, {"tp": near})

    chunk = 512 if features % 512 == 0 else features
    upper = z // (n // 2)
    mate = n // 2 - 1 - z + upper * n
    gate = (z == n // 2 - 1) | (z == n // 2)
    across = [upper * j + (1 - upper) * (n - 1 - j) for j in range(n // 2)]
    order = across + [mate, z]
    stops = [(j, p) for j in range(len(order)) for p in range(cuts)]

    def slot(p):
        return pl.ds(p * part_rows, part_rows)

    def piece_rows(block, p):
        return pl.ds(pl.multiple_of(block * rows + p * part_rows, part_rows), part_rows)

    def x2_copy(block, p):
        sems = (ax_send.at[block, p], x2_recv.at[block, p])
        return remote(sum_far.at[block, slot(p)], got_x.at[block, slot(p)], *sems, {"tp": far})

    def mate_copy(p):
        sems = (k_send.at[2, p], z2_recv.at[2, p])
        return remote(sum_z.at[2, slot(p)], got_z.at[0, slot(p)], *sems, {"sp": mate})

    def inner_copy(j, p):
        sems = (k_send.at[j, p], z2_recv.at[j, p])
        return remote(sum_z.at[j, slot(p)], got_in.at[j, slot(p)], *sems, {"sp": mate})

    def outer_copy(j, p):
        sems = (k_send.at[j, p], z2_recv.at[3, p])
        return remote(sum_z.at[j, slot(p)], got_z.at[1, slot(p)], *sems, {"sp": across[j]})

    def combine(j, p):
        @pl.when(gate)
        def _():
            inner_copy(j, p).wait_recv()
            sum_z[j, slot(p)] = rounded(held_z[j, slot(p)] + wide(got_in[j, slot(p)]))
            outer_copy(j, p).start()

    def lower(i, carry):
        seq = lax.rem(high + 1 - i // 2, 2) * 2 + lax.rem(low + 1 - lax.rem(i, 2), 2)
        for c in range(features // chunk):
            cols = slice(c * chunk, (c + 1) * chunk)
            part_two[seq, :, cols] = rounded(dot(hidden[seq], down_w[:, cols]))

        @pl.when(lax.rem(i, 2) == 0)
        def _():
            for block in order:
                c2_copy(i // 2, seq, block).start()

        @pl.when(i == 1)
        def _():
            for block in order:
                c2_copy(0, diag, block).wait_recv()
                for p in range(cuts):
                    there = piece_rows(block, p)
                    both = wide(part_two[far, there]) + wide(got_two[0, there])
                    sum_far[block, slot(p)] = rounded(both)
                    x2_copy(block, p).start()

        return carry

    for block in range(n):

        @pl.when((z >= block) & (z < n - 1))
        def _():
            for p in (0, 1):
                key_copy(block, p).wait_send()

        for p in range(cuts):
            x_copy(tp, block, p).wait_send()
        c_copy(tp, 0, block).wait_send()
        c_copy(far, 1, block).wait_send()
    phase("lower")
    lax.fori_loop(0, rows_all.shape[0], lower, 0)
    phase("x2")
    lag = 1
    for t, (j, p) in enumerate(stops):
        block = order[j]
        if p == 0:
            c2_copy(1, near, block).wait_recv()
        there = piece_rows(block, p)
        x2_copy(block, p).wait_recv()
        both = wide(part_two[tp, there]) + wide(got_two[1, there]) + wide(got_x[block, slot(p)])
        if j < len(across):

            @pl.when(gate)
            def _():
                held_z[j, slot(p)] = both

            @pl.when(jnp.logical_not(gate))
            def _():
                sum_z[j, slot(p)] = rounded(both)
                inner_copy(j, p).start()

        elif j == len(across):
            sum_z[j, slot(p)] = rounded(both)
            mate_copy(p).start()
        else:
            own_z[slot(p)] = mid[slot(p)] + both
        if t >= lag and stops[t - lag][0] < len(across):
            combine(*stops[t - lag])
    phase("z2")
    for p in range(cuts):
        mate_copy(p).wait_recv()
        outer_copy(0, p).wait_recv()
        answer = own_z[slot(p)] + wide(got_z[0, slot(p)]) + wide(got_z[1, slot(p)])
        out[slot(p)] = answer.astype(out.dtype)

    phase("drain")
    for k, peer in enumerate(peers):
        doc_copy(k, z, peer).wait_send()
    for p in range(cuts):
        mate_copy(p).wait_send()
        for j in range(len(across)):
            inner_copy(j, p).wait_send()
    for d in range(1, n):
        when_sent(d, ups + downs, lambda copy: copy.wait_send())
        when_hopped(d, ups + downs, lambda copy: copy.wait_send())
    for i in range(halves):
        c1_copy(i).wait_send()
        x1_copy(i).wait_send()
    for block in range(n):

        @pl.when((z >= block) & (z < n - 1))
        def _():
            for p in range(cuts):
                chain_copy(0, block, p).wait_send()

        @pl.when((z <= block) & (z > 0))
        def _():
            for p in range(cuts):
                chain_copy(1, block, p).wait_send()

        for p in range(cuts):
            x2_copy(block, p).wait_send()
        c2_copy(0, diag, block).wait_send()
        c2_copy(1, near, block).wait_send()
    phase(None)


def rope_tables(total, width, copies):
    half = width // 2
    freqs = np.float32(ROPE_BASE) ** (-np.arange(half, dtype=np.float32) * np.float32(2.0) / np.float32(width))
    angles = np.arange(total, dtype=np.float32)[:, None] * freqs.astype(np.float32)[None, :]
    tile = lambda table: np.tile(table.astype(np.float32), (1, 2 * copies))
    return tile(np.cos(angles)), tile(np.sin(angles))


def turn_matrix(width):
    half = width // 2
    at = np.arange(width)
    source = np.where(at < half, at + half, at - half)
    sign = np.where(at < half, -1.0, 1.0)
    return np.where(at[:, None] == source[None, :], sign[None, :], 0.0)


def spread_matrix(width, group, kv_local):
    straight = np.kron(np.eye(kv_local), np.tile(np.eye(width), (1, group)))
    crossed = np.kron(np.eye(kv_local), np.tile(turn_matrix(width), (1, group)))
    both = np.concatenate([straight, crossed], axis=1)
    return np.kron(np.eye(2), both)


def kernel_fits(resid_in, query_one, key_one, value, lam, gate_weight):
    heads = lam.shape[0]
    width = query_one.shape[2] // heads
    kv_local = key_one.shape[2] // width
    group = heads // kv_local
    seqs, rows = query_one.shape[:2]
    return (
        lax.axis_size("tp") == 4
        and lax.axis_size("grp") == 2
        and lax.axis_size("sp") == 4
        and kv_local == 2
        and group == 4
        and group * width == LANES
        and value.shape[2] == LANES
        and seqs == 4
        and resid_in.shape[0] == 1
        and rows % 16 == 0
        and rows * lax.axis_size("sp") <= 256
        and gate_weight.shape[0] <= 512
        and gate_weight.shape[1] % LANES == 0
        and gate_weight.shape[1] <= 1536
        and resid_in.shape[2] <= 2048
    )


def whole_layer(
    resid_in, query_one, key_one, query_two, key_two, value, lam, head_gain, doc_ids,
    out_weight, norm_gain, gate_weight, value_weight, conv_gate, conv_value, down_weight,
):
    n = lax.axis_size("sp")
    seqs, rows = query_one.shape[:2]
    heads = lam.shape[0]
    width = query_one.shape[2] // heads
    kv_local = key_one.shape[2] // width
    group = heads // kv_local
    features, total = resid_in.shape[2], n * rows
    depth, columns = gate_weight.shape[0], down_weight.shape[1]
    tiles = gate_weight.shape[1] // LANES
    per = -(-tiles // n)
    cosine, sine = rope_tables(total, width, heads)
    turn = np.kron(np.eye(heads), turn_matrix(width))
    spread = spread_matrix(width, group, kv_local)
    key_width = kv_local * width
    join = np.stack([np.eye(key_width, LANES), np.eye(key_width, LANES, LANES - key_width)])
    halves = 2
    bf16, f32 = jnp.bfloat16, jnp.float32
    dma = pltpu.SemaphoreType.DMA
    vmem = pltpu.VMEM
    scratch = [
        vmem(query_one.shape, bf16),
        vmem(query_two.shape, bf16),
        vmem((1, features), f32),
        vmem(conv_gate.shape, f32),
        vmem(conv_value.shape, f32),
        vmem(cosine.shape, f32),
        vmem(sine.shape, f32),
        vmem(turn.shape, bf16),
        vmem(spread.shape, bf16),
        vmem((rows, features), bf16),
        vmem((seqs, total, 2 * LANES), bf16),
        vmem((n, 8, total), f32),
        vmem((seqs, 8, total), f32),
        vmem(out_weight.shape, bf16),
        vmem((seqs, rows, out_weight.shape[0]), bf16),
        vmem((2, 2, rows, features), bf16),
        vmem((halves, 2, rows, features // halves), bf16),
        vmem((halves, rows, features // halves), bf16),
        vmem((halves, rows, features // halves), bf16),
        vmem((rows, features), f32),
        vmem((seqs, total, features), bf16),
        vmem((n * depth, 2 * per * LANES), bf16),
        vmem((per * LANES, n * columns), bf16),
        vmem((seqs, total, per * LANES), bf16),
        vmem((seqs, total, features), bf16),
        vmem((2, total, features), bf16),
        vmem((n, rows, features), bf16),
        vmem((n, rows, features), bf16),
        vmem((n - 1, rows, features), bf16),
        vmem((rows, features), f32),
        vmem((2, rows, features), bf16),
        vmem((2, rows, features), bf16),
        vmem((2, rows, features), f32),
        dma((n,)), dma((n,)), dma((n, 2)), dma((n, 2)), dma,
        dma((n, 2 * per)), dma((n, 4 * per)), dma((n, 2 * per)),
        dma((halves,)), dma((halves,)), dma((halves,)), dma((halves,)),
        dma((2, n, 2)), dma((n, 2)), dma((n, 2)), dma((n, 2)), dma((2, n)), dma((2, n)),
        dma((2, n)), dma((n, 2)), dma((n, 2)),
    ]
    out = pl.pallas_call(
        functools.partial(layer_kernel, n, per, tiles, width ** (-0.5)),
        out_shape=jax.ShapeDtypeStruct((rows, features), resid_in.dtype),
        in_specs=[VMEM] * 4 + [SMEM] + [VMEM] * 2 + [HBM] * 14,
        out_specs=VMEM,
        scratch_shapes=scratch,
        compiler_params=pltpu.CompilerParams(
            collective_id=5, has_side_effects=True, vmem_limit_bytes=60 * 2**20
        ),
        name="whole_layer",
    )(
        key_one, key_two, value, doc_ids, lam, head_gain[None], jnp.asarray(join, bf16),
        query_one, query_two, norm_gain[None], conv_gate, conv_value,
        jnp.asarray(cosine), jnp.asarray(sine), jnp.asarray(turn, bf16),
        jnp.asarray(spread, bf16), resid_in.reshape(rows, features),
        out_weight, gate_weight, value_weight, down_weight,
    )
    return out.reshape(resid_in.shape)


def per_device_apart(
    resid_in,
    query_one,
    key_one,
    query_two,
    key_two,
    value,
    lam,
    head_gain,
    doc_ids,
    out_weight,
    norm_gain,
    gate_weight,
    value_weight,
    conv_gate,
    conv_value,
    down_weight,
):
    n_sp = lax.axis_size("sp")
    me = lax.axis_index("sp")
    depth, width = gate_weight.shape
    share = width // n_sp
    copies = lax.axis_size("grp")

    def cut(weight, row, column, size):
        return lax.dynamic_slice(weight, (row, column), size)

    def up_piece(dest, part):
        size = (depth // copies, share)
        row, column = part * size[0], dest * share
        return jnp.stack([cut(gate_weight, row, column, size), cut(value_weight, row, column, size)])

    def up_whole(dest):
        return jnp.stack([up_piece(dest, part) for part in range(copies)])

    def down_piece(dest, part):
        size = (share // copies, down_weight.shape[1])
        return cut(down_weight, dest * share + part * size[0], 0, size)

    def down_whole(dest):
        return jnp.stack([down_piece(dest, part) for part in range(copies)])

    up_all = exchange(up_piece, up_whole)
    down_all = exchange(down_piece, down_whole)
    gate_all = up_all[:, :, 0].reshape(-1, share)
    value_all = up_all[:, :, 1].reshape(-1, share)
    down_full = jnp.transpose(down_all, (1, 2, 0, 3)).reshape(share, -1)
    seqs = query_one.shape[0]
    rows = query_one.shape[1]
    heads = lam.shape[0]
    key_width = query_one.shape[2] // heads
    kv_local = key_one.shape[2] // key_width
    group = heads // kv_local
    head_width = value.shape[2] // kv_local
    scale = key_width ** (-0.5)
    positions = lax.axis_index("sp") * rows + jnp.arange(rows, dtype=jnp.int32)
    q_first = rotate(query_one, positions, heads).reshape(seqs, rows, kv_local, group, key_width)
    q_second = rotate(query_two, positions, heads).reshape(seqs, rows, kv_local, group, key_width)
    k_first = rotate(key_one, positions, kv_local).reshape(seqs, rows, kv_local * key_width)
    k_second = rotate(key_two, positions, kv_local).reshape(seqs, rows, kv_local * key_width)
    start_state = (
        jnp.full((seqs, kv_local, group, rows), NEG_BIG, jnp.float32),
        jnp.zeros((seqs, kv_local, group, rows), jnp.float32),
        jnp.zeros((seqs, kv_local, group, rows, head_width), jnp.float32),
    )
    packed = jnp.concatenate(
        [k_first, k_second, value, doc_ids.astype(jnp.bfloat16)[..., None]], axis=-1
    )
    packed = gather_sp(packed)
    key_cols = k_first.shape[2]
    keys_one = packed[..., :key_cols]
    keys_two = packed[..., key_cols : 2 * key_cols]
    vals = packed[..., 2 * key_cols : -1]
    docs = packed[..., -1].astype(jnp.int32)
    count = keys_one.shape[1]
    step_len = math.gcd(count, 512)

    def inner(state, index):
        offset = index * step_len
        ka = lax.dynamic_slice_in_dim(keys_one, offset, step_len, 1).reshape(
            seqs, step_len, kv_local, key_width
        )
        kb = lax.dynamic_slice_in_dim(keys_two, offset, step_len, 1).reshape(
            seqs, step_len, kv_local, key_width
        )
        va = lax.dynamic_slice_in_dim(vals, offset, step_len, 1).reshape(
            seqs, step_len, kv_local, head_width
        )
        dpiece = lax.dynamic_slice_in_dim(docs, offset, step_len, 1)
        key_pos = offset + jnp.arange(step_len, dtype=jnp.int32)
        allowed = (key_pos[None, None, :] <= positions[None, :, None]) & (
            dpiece[:, None, :] == doc_ids[:, :, None]
        )
        first = online_step(state[0], q_first, ka, va, allowed, scale)
        second = online_step(state[1], q_second, kb, va, allowed, scale)
        return ((first, second), None)

    def run(state):
        return lax.scan(inner, state, jnp.arange(count // step_len))[0]

    first, second = lax.cond(
        jnp.int32(0) <= positions[rows - 1], run, lambda state: state, (start_state, start_state)
    )
    weights = lam.reshape(kv_local, group)[None, :, :, None, None]
    mixed = first[2] / first[1][..., None] - weights * (second[2] / second[1][..., None])
    meansq = jnp.mean(mixed * mixed, axis=-1, keepdims=True)
    normed_heads = mixed * lax.rsqrt(meansq + NORM_EPS) * head_gain
    heads_out = jnp.transpose(normed_heads, (0, 3, 1, 2, 4)).reshape(
        seqs * rows, heads * head_width
    )
    heads_out = heads_out.astype(jnp.bfloat16)
    own = resid_in.shape[0]
    features = resid_in.shape[2]
    proj = jnp.dot(heads_out, out_weight, preferred_element_type=jnp.float32).astype(jnp.bfloat16)
    mid = reduce_rows(
        proj.reshape(-1, 1, own * rows, features),
        resid_in.astype(jnp.float32).reshape(own * rows, features),
        jnp.float32,
        False,
    )
    meansq_mid = jnp.mean(mid * mid, axis=-1, keepdims=True)
    normed = (mid * lax.rsqrt(meansq_mid + NORM_EPS) * norm_gain).astype(jnp.bfloat16)
    gathered = gather_rows(normed).reshape(-1, n_sp, own, rows, features)
    full_rows = jnp.transpose(gathered, (0, 2, 1, 3, 4)).reshape(-1, features)
    total_rows = n_sp * rows
    start = me * share
    taps_gate = lax.dynamic_slice_in_dim(conv_gate, start, share, 1)
    taps_value = lax.dynamic_slice_in_dim(conv_value, start, share, 1)
    up_gate = jnp.dot(full_rows, gate_all, preferred_element_type=jnp.float32)
    up_value = jnp.dot(full_rows, value_all, preferred_element_type=jnp.float32)
    up_gate = up_gate.astype(jnp.bfloat16).reshape(seqs, total_rows, share)
    up_value = up_value.astype(jnp.bfloat16).reshape(seqs, total_rows, share)
    conv_g = depthwise(up_gate, taps_gate, docs)
    conv_v = depthwise(up_value, taps_value, docs)
    hidden = (jax.nn.silu(conv_g) * conv_v).astype(jnp.bfloat16)
    hidden = hidden.reshape(-1, own, n_sp, rows, share)
    hidden = jnp.transpose(hidden, (0, 2, 1, 3, 4)).reshape(-1, share)
    partial_down = jnp.dot(hidden, down_full, preferred_element_type=jnp.float32)
    partial_down = partial_down.astype(jnp.bfloat16).reshape(-1, n_sp, own * rows, features)
    return reduce_rows(partial_down, mid, jnp.bfloat16, True).reshape(resid_in.shape)


def per_device(*args):
    resid_in, query_one, key_one, value, lam, gate_weight = [args[i] for i in (0, 1, 2, 5, 6, 11)]
    if kernel_fits(resid_in, query_one, key_one, value, lam, gate_weight):
        return whole_layer(*args)
    return per_device_apart(*args)


def solution(mesh):
    placed = (
        P(("grp", "tp"), "sp", None),
        P("grp", "sp", "tp"),
        P("grp", "sp", "tp"),
        P("grp", "sp", "tp"),
        P("grp", "sp", "tp"),
        P("grp", "sp", "tp"),
        P("tp"),
        P(),
        P("grp", "sp"),
        P("tp", None),
        P(),
        P("sp", "tp"),
        P("sp", "tp"),
        P(None, "tp"),
        P(None, "tp"),
        P("tp", "sp"),
    )
    return jax.shard_map(
        per_device,
        mesh=mesh,
        in_specs=placed,
        out_specs=P(("grp", "tp"), "sp", None),
        check_vma=False,
    )
```
